32 devices in a mesh: ep: 16 (over z, y, x), tp: 2 (over core).
Axes of the slice: x: 2, y: 2, z: 4, core: 2. Of those that a mesh axis runs over, the one named last changes fastest.
Arguments:
- tokens: bfloat16 [4096, 2048], P(('ep', 'tp')), may hold values from -6 to 6
- norm_gain: float32 [2048], replicated, may hold values from 0.25 to 4
- routes: int32 [4096, 2], P(('ep', 'tp')), may hold values from 0 to 15, all different within a row; in each aligned block of 128 rows (0 to 127, 128 to 255, ...) at most 22 rows name the same one
- route_weights: float32 [4096, 2], P(('ep', 'tp')), may hold values from 0.1 to 1
- w_gate: bfloat16 [16, 2048, 1024], P('ep', None, 'tp'), may hold values from -0.125 to 0.125
- w_up: bfloat16 [16, 2048, 1024], P('ep', None, 'tp'), may hold values from -0.125 to 0.125
- w_down: bfloat16 [16, 1024, 2048], P('ep', 'tp'), may hold values from -0.1875 to 0.1875
- dense_in: bfloat16 [2048, 256], P('ep'), may hold values from -0.125 to 0.125
- dense_out: bfloat16 [2048, 256], P('ep'), may hold values from -0.375 to 0.375
- dense_gate: float32 [2048], replicated, may hold values from -6 to 6
Outputs:
- mixed: bfloat16 [4096, 2048], P(('ep', 'tp'))
The draws below stay inside these ranges and needn't reach their ends.
Inputs may be any that keep to these rules, and one draw needn't show every extreme that they name: `routes`: each row names 2 different experts. Among the 128 rows of one device no expert is named more than 22 times; every draw has a device and an expert with exactly 22.
All inputs are finite; a program needn't handle non-finite values.
Results may differ from the reference program's by a relative error of at most 0.0074.
Values may be sent and summed in bfloat16 or wider, within the bound.
A program may use at most 128 MiB of HBM per device.

```python
import math
import jax
import jax.numpy as jnp
import numpy as np
from jax import lax

D = 2048
FF = 1024
DH = 256
TOP_K = 2
TOK_DEV = 128
EXPERTS = 16
TOKENS = 4096
CAP = 22
N_TP = 2


def draw_norm_gain(key, part):
    return 1.0 + 0.18 * jnp.clip(jax.random.normal(key, (D,), jnp.float32), -4.0, 4.0)


def shard_levels(key, shape, pieces, low, largest):
    factor_of = 1.0
    for axis_at, blocks in pieces:
        steps = jax.random.uniform(jax.random.fold_in(jax.random.fold_in(key, 6), axis_at), (blocks,), jnp.float32, low / len(pieces), largest / len(pieces))
        factor_of = factor_of * jnp.repeat(jnp.exp(steps), shape[axis_at] // blocks).reshape((-1,) + (1,) * (len(shape) - 1 - axis_at))
    return factor_of


def assign_block(own_key, own, number, rows, amount, top, bound, slope):
    order = jax.random.permutation(own_key, amount)
    packed, common = portions_of(amount, rows * top, bound, slope, True), portions_of(amount, rows * top, bound, slope, False)
    places = jnp.arange(amount)

    def named(lengths, turn):
        used = int((lengths > 0).sum())
        fixed = max(1, used // 4)
        passed = fixed + (places - fixed + turn * (used - fixed)) % max(1, amount - fixed)
        return jnp.zeros((amount,), jnp.int32).at[order[jnp.where(places < fixed, places, passed)]].set(jnp.asarray(lengths, jnp.int32))

    lengths = jnp.where(number % 4 == 0, named(packed, number // 4), named(common, number - number // 4 - 1))
    mixed = jax.random.permutation(jax.random.fold_in(own, 3), amount)
    donor, sink = mixed[0:amount // 2 * 2:2], mixed[1:amount // 2 * 2:2]
    margin = jnp.minimum(lengths[donor] - 1, bound - lengths[sink]) // 2
    margin = jnp.where((donor == order[0]) | (sink == order[0]) | (lengths[sink] == 0), 0, jnp.maximum(margin, 0))
    passed = jax.random.randint(jax.random.fold_in(own, 4), (amount // 2,), 0, 1 << 20) % (margin + 1)
    lengths = lengths.at[donor].add(-passed).at[sink].add(passed)
    items = jnp.searchsorted(jnp.cumsum(lengths), jnp.arange(rows * top), side="right").astype(jnp.int32)
    table = items.reshape(top, rows).T
    table = table[jax.random.permutation(jax.random.fold_in(own, 1), rows)]
    turn = jax.random.randint(jax.random.fold_in(own, 2), (rows, 1), 0, top)
    return jnp.take_along_axis(table, (jnp.arange(top)[None, :] + turn) % top, axis=1)


def portions_of(amount, total, reach, skew, full):
    loads = [(1 << 20) // math.isqrt(standing ** skew) + 1 for standing in range(1, amount + 1)]
    largest = reach if full else min(reach, max(-(-total // amount), total * loads[0] // sum(loads)))
    least = 1 if total - largest >= amount - 1 else 0
    given, spare = [largest] + [least] * (amount - 1), total - largest - least * (amount - 1)
    while spare > 0:
        free = [i for i in range(1, amount) if given[i] < largest] or [i for i in range(1, amount) if given[i] < reach]
        mass, left = sum([loads[i] for i in free]), spare
        for i in free:
            addition = min(reach - given[i], max(1, left * loads[i] // mass), spare)
            given[i] = given[i] + addition
            spare = spare - addition
    return np.array(given)


def noise(rng, dims, width, reach, split=(), kind=jnp.bfloat16):
    array = jax.random.normal(rng, dims, jnp.float32) * width
    if len(split) > 0:
        array = shard_levels(rng, dims, split, -0.22, 0.18) * array
    return jnp.clip(array, min=-reach, max=reach).astype(kind)


def setup_inputs(seed: int = 0) -> dict:
    key_of = jax.random.split(jax.random.key(seed), 11)
    tokens = noise(key_of[0], (TOKENS, D), 1.0, 6.0, ((0, 32),))
    norm_gain = draw_norm_gain(jax.random.fold_in(key_of[10], 71), 0)
    routes_keys = jax.random.split(jax.random.fold_in(key_of[2], 1), TOKENS // TOK_DEV)
    routes_turns = jax.random.permutation(jax.random.fold_in(key_of[2], 3), TOKENS // TOK_DEV)
    routes = jax.vmap(lambda own, number: assign_block(jax.random.fold_in(key_of[2], 2), own, number, TOK_DEV, EXPERTS, TOP_K, CAP, 2))(routes_keys, routes_turns).reshape((TOKENS, TOP_K))
    route_weights = jnp.clip(0.1 + 0.9 * jax.random.uniform(key_of[3], (TOKENS, TOP_K), jnp.float32) ** shard_levels(key_of[3], (TOKENS, TOP_K), ((0, 32),), -0.2, 0.2), 0.1, 1.0)
    w_gate = noise(key_of[4], (EXPERTS, D, FF), D ** -0.5, 0.125, ((0, 16), (2, 2)))
    w_up = noise(key_of[5], (EXPERTS, D, FF), D ** -0.5, 0.125, ((0, 16), (2, 2)))
    w_down = noise(key_of[6], (EXPERTS, FF, D), FF ** -0.5, 0.1875, ((0, 16), (1, 2)))
    dense_in = noise(key_of[7], (D, DH), D ** -0.5, 0.125, ((0, 16),))
    dense_out = noise(key_of[8], (D, DH), DH ** -0.5, 0.375, ((0, 16),))
    dense_gate = noise(key_of[9], (D,), 1.5, 6.0, (), jnp.float32)
    return dict(tokens=tokens, norm_gain=norm_gain, routes=routes, route_weights=route_weights, w_gate=w_gate, w_up=w_up, w_down=w_down, dense_in=dense_in, dense_out=dense_out, dense_gate=dense_gate)


CLAMP_LIMIT = 7.0
SLOPE_ALPHA = 1.702
NORM_EPS = 1e-06

def rms_normed(tokens, norm_gain):
    widened = tokens.astype(jnp.float32)
    inv_scale = lax.rsqrt(lax.optimization_barrier(jnp.mean(widened * widened, axis=1, keepdims=True)) + NORM_EPS)
    return (widened * inv_scale * norm_gain).astype(jnp.bfloat16)

def clamped_unit(gate_pre, up_pre):
    gate_clip = jnp.minimum(gate_pre, CLAMP_LIMIT)
    up_clip = jnp.clip(up_pre, -CLAMP_LIMIT, CLAMP_LIMIT)
    return ((up_clip + 1.0) * gate_clip * jax.nn.sigmoid(SLOPE_ALPHA * gate_clip)).astype(jnp.bfloat16)

def reference(tokens, norm_gain, routes, route_weights, w_gate, w_up, w_down, dense_in, dense_out, dense_gate):
    normed = rms_normed(tokens, norm_gain)
    sources = TOKENS // TOK_DEV
    entries = TOK_DEV * TOP_K
    block_routes = routes.reshape(sources, entries)
    onehot = (block_routes[:, :, None] == jnp.arange(EXPERTS, dtype=jnp.int32)[None, None, :]).astype(jnp.int32)
    slot_index = lax.optimization_barrier(jnp.sum((jnp.cumsum(onehot, axis=1) - onehot) * onehot, axis=2))
    source_ids = jnp.arange(sources, dtype=jnp.int32)[:, None]
    position = (block_routes * (sources * CAP) + source_ids * CAP + slot_index).reshape(-1).astype(jnp.int32)
    entry_ids = jnp.arange(TOKENS * TOP_K, dtype=jnp.int32)
    slot_table = jnp.full((EXPERTS * sources * CAP,), -1, jnp.int32).at[position].set(entry_ids)
    slot_table = slot_table.reshape(EXPERTS, sources * CAP)
    half_width = FF // N_TP

    def one_expert(expert_args):
        entry_index, gate_w, up_w, down_w = expert_args
        is_valid = entry_index >= 0
        token_of = jnp.where(is_valid, entry_index, 0) // TOP_K
        gathered_rows = jnp.where(is_valid[:, None], normed[token_of], jnp.zeros((), jnp.bfloat16))
        gate_pre = jnp.dot(gathered_rows, gate_w, preferred_element_type=jnp.float32)
        up_pre = jnp.dot(gathered_rows, up_w, preferred_element_type=jnp.float32)
        hidden = clamped_unit(gate_pre, up_pre)
        summed = jnp.zeros((gathered_rows.shape[0], D), jnp.float32)
        for half_index in range(N_TP):
            low = half_index * half_width
            partial_value = jnp.dot(hidden[:, low:low + half_width], down_w[low:low + half_width], preferred_element_type=jnp.float32).astype(jnp.bfloat16)
            summed = summed + lax.optimization_barrier(partial_value).astype(jnp.float32)
        return summed.astype(jnp.bfloat16)
    results = lax.map(one_expert, (slot_table, w_gate, w_up, w_down))
    flat_results = results.reshape(EXPERTS * sources * CAP, D)
    picked = flat_results[position].astype(jnp.float32).reshape(TOKENS, TOP_K, D)
    weighted = lax.optimization_barrier(jnp.sum(picked * route_weights[:, :, None], axis=1))
    dense_hidden = jax.nn.silu(jnp.dot(normed, dense_in, preferred_element_type=jnp.float32)).astype(jnp.bfloat16)
    branch = lax.dot_general(dense_hidden, dense_out, (((1,), (1,)), ((), ())), preferred_element_type=jnp.float32)
    return (weighted + jax.nn.sigmoid(dense_gate) * branch).astype(jnp.bfloat16)
```

```python
import functools
import math

import jax
import jax.numpy as jnp
from jax import lax
from jax.experimental import pallas as pl
from jax.experimental.pallas import tpu as pltpu
from jax.sharding import PartitionSpec as P

CLAMP_LIMIT = 7.0
SLOPE_ALPHA = 1.702
NORM_EPS = 1e-06
MESH = pl.DeviceIdType.MESH
F32 = jnp.float32
BF16 = jnp.bfloat16


def clamped_unit(gate_pre, up_pre):
    gate_clip = jnp.minimum(gate_pre, CLAMP_LIMIT)
    up_clip = jnp.clip(up_pre, -CLAMP_LIMIT, CLAMP_LIMIT)
    return ((up_clip + 1.0) * gate_clip * jax.nn.sigmoid(SLOPE_ALPHA * gate_clip)).astype(BF16)


def layer_kernel(
    sizes,
    routes_t_ref,
    routes_ref,
    weights_ref,
    tokens_ref,
    gain_ref,
    dgate_ref,
    din_ref,
    dout_ref,
    wg_ref,
    wu_ref,
    wd_ref,
    out_ref,
    normed,
    keys,
    stacked,
    places,
    xs,
    totals,
    unpack_ref,
    pack_ref,
    buf,
    recv,
    outb,
    ret,
    wgs,
    wus,
    wds,
    hid,
    dn,
    acc,
    send1,
    recv1,
    send2,
    recv2,
    w_local,
    w_send,
    w_recv,
    ds1,
    dr1,
    ds2,
    dr2,
    ds3,
    dr3,
):
    n, n1, n2, cap, blocks = sizes
    rows, width = tokens_ref.shape
    half = wg_ref.shape[1]
    tall, tile = blocks * cap, width // blocks
    group_rows, packed_rows = n2 * cap, n2 * blocks * cap
    me = lax.axis_index("ep")
    core = lax.axis_index("tp")
    plane, spot = me // n2, me % n2
    peer = 1 - core

    barrier = pltpu.get_barrier_semaphore()

    def greet(i, carry):
        pl.semaphore_signal(
            barrier, inc=1, device_id={"ep": (me + i) % n}, device_id_type=MESH
        )
        return carry

    lax.fori_loop(1, n, greet, 0)
    pl.semaphore_signal(barrier, inc=1, device_id={"tp": peer}, device_id_type=MESH)

    weight_pairs = ((wg_ref, wgs), (wu_ref, wus), (wd_ref, wds))
    for i, (src, dst) in enumerate(weight_pairs):
        pltpu.make_async_copy(src, dst.at[0], w_local.at[i]).start()

    @pl.when(core == 0)
    def _():
        dn[0, plane, spot] = din_ref[...]

    @pl.when(core == 1)
    def _():
        dn[1, plane, spot] = dout_ref[...]

    widened = tokens_ref[...].astype(F32)
    inv_scale = lax.rsqrt(jnp.mean(widened * widened, axis=1, keepdims=True) + NORM_EPS)
    normed[...] = (widened * inv_scale * gain_ref[...]).astype(BF16)
    for j in range(blocks):
        stacked[j * rows : (j + 1) * rows, :] = normed[:, j * tile : (j + 1) * tile]

    expert_ids = lax.broadcasted_iota(jnp.int32, (n, rows), 0)
    chosen = (routes_t_ref[0:1, :] == expert_ids) | (routes_t_ref[1:2, :] == expert_ids)
    earlier = (
        lax.broadcasted_iota(jnp.int32, (rows, rows), 0)
        < lax.broadcasted_iota(jnp.int32, (rows, rows), 1)
    )
    counted = jnp.dot(
        jnp.where(chosen, 1.0, 0.0).astype(BF16),
        jnp.where(earlier, 1.0, 0.0).astype(BF16),
        preferred_element_type=F32,
    )
    for j in range(blocks):
        found = jnp.where(chosen, counted.astype(jnp.int32) + j * cap, -1)
        for z in range(n1):
            keys[z, :, j * rows : (j + 1) * rows] = found[z * n2 : (z + 1) * n2]
    experts_across = lax.broadcasted_iota(jnp.int32, (rows, n), 1)
    takes = [routes_ref[:, k : k + 1] == experts_across for k in range(2)]
    before = (
        lax.broadcasted_iota(jnp.int32, (rows, rows), 0)
        > lax.broadcasted_iota(jnp.int32, (rows, rows), 1)
    )
    counts = jnp.dot(
        jnp.where(before, 1.0, 0.0).astype(BF16),
        jnp.where(takes[0] | takes[1], 1.0, 0.0).astype(BF16),
        preferred_element_type=F32,
    )
    for k in range(2):
        slot = jnp.sum(jnp.where(takes[k], counts, 0.0), axis=1, keepdims=True)
        places[:, k : k + 1] = routes_ref[:, k : k + 1] * tall + slot.astype(jnp.int32)

    pl.semaphore_wait(barrier, n)

    def weight_copy(i):
        src, dst = weight_pairs[i]
        return pltpu.make_async_remote_copy(
            src_ref=src,
            dst_ref=dst.at[1],
            send_sem=w_send.at[i],
            recv_sem=w_recv.at[i],
            device_id={"tp": peer},
            device_id_type=MESH,
        )

    def dense_copy1(bit, block):
        other = plane + bit - 2 * bit * ((plane // bit) % 2)
        return pltpu.make_async_remote_copy(
            src_ref=dn.at[core, block, spot],
            dst_ref=dn.at[core, block, spot],
            send_sem=ds1.at[block],
            recv_sem=dr1.at[block],
            device_id={"ep": other * n2 + spot},
            device_id_type=MESH,
        )

    bits = [1 << b for b in reversed(range(n1.bit_length() - 1))]

    def dense_held(bit, where):
        return [where % (2 * bit) + m * 2 * bit for m in range(n1 // (2 * bit))]

    def dense_start(bit):
        for block in dense_held(bit, plane):
            dense_copy1(bit, block).start()

    def dense_finish(bit):
        for block in dense_held(bit, plane + bit - 2 * bit * ((plane // bit) % 2)):
            dense_copy1(bit, block).wait_recv()
        for block in dense_held(bit, plane):
            dense_copy1(bit, block).wait_send()

    def dense_copy2(other, slot):
        return pltpu.make_async_remote_copy(
            src_ref=dn.at[core, :, slot],
            dst_ref=dn.at[core, :, slot],
            send_sem=ds2.at[other],
            recv_sem=dr2.at[slot],
            device_id={"ep": plane * n2 + other},
            device_id_type=MESH,
        )

    def dense_copy3(which):
        return pltpu.make_async_remote_copy(
            src_ref=dn.at[which],
            dst_ref=dn.at[which],
            send_sem=ds3,
            recv_sem=dr3,
            device_id={"tp": peer},
            device_id_type=MESH,
        )

    def each(count, act):
        def step(i, carry):
            act(i)
            return carry

        lax.fori_loop(0, count, step, 0)

    dense_start(bits[0])
    for i in range(3):
        weight_copy(i).start()

    def dispatch(dst, slot):
        return pltpu.make_async_remote_copy(
            src_ref=buf.at[dst],
            dst_ref=recv.at[slot],
            send_sem=send1.at[dst],
            recv_sem=recv1.at[slot],
            device_id={"ep": dst},
            device_id_type=MESH,
        )

    def give_back(dst, slot):
        return pltpu.make_async_remote_copy(
            src_ref=outb.at[dst],
            dst_ref=ret.at[slot],
            send_sem=send2.at[dst],
            recv_sem=recv2.at[slot],
            device_id={"ep": dst},
            device_id_type=MESH,
        )

    def partner_plane(x):
        return sum(((plane // b) % 2 + (x // b) % 2) % 2 * b for b in bits)

    def turn(i):
        return partner_plane(i % 2 * (n1 // 2) + i // 2)

    def send_group(i):
        group = partner_plane((i + n1 // 2) % n1)
        first = group * n2
        wanted = keys[group]
        picks = wanted[:, None, :] == lax.broadcasted_iota(
            jnp.int32, (n2, tall, blocks * rows), 1
        )
        picks = jnp.where(picks, 1.0, 0.0).reshape(packed_rows, blocks * rows).astype(BF16)
        found = jnp.dot(picks, stacked[...], preferred_element_type=F32)
        buf[pl.ds(first, n2)] = found.reshape(n2, tall, tile).astype(BF16)

        def start(j):
            dst = first + (spot + 1 + j) % n2

            @pl.when(dst != me)
            def _():
                dispatch(dst, me).start()

            @pl.when(dst == me)
            def _():
                recv[me] = buf[me]

        each(n2, start)

    each(n1, send_group)


    for i, (src, dst) in enumerate(weight_pairs):
        pltpu.make_async_copy(src, dst.at[0], w_local.at[i]).wait()
    for i in range(3):
        weight_copy(i).wait()

    piece = min(256, half)
    upright = lax.broadcasted_iota(jnp.int32, (packed_rows, packed_rows), 0)
    across = lax.broadcasted_iota(jnp.int32, (packed_rows, packed_rows), 1)

    def packed_place(r):
        return (r // cap) % n2 * tall + r // group_rows * cap + r % cap

    unpack = jnp.where(packed_place(upright) == across, 1.0, 0.0).astype(BF16)
    pack = jnp.where(packed_place(across) == upright, 1.0, 0.0).astype(BF16)
    unpack_ref[...] = unpack
    pack_ref[...] = pack

    def run_group(i):
        group = turn(i)
        first = group * n2

        def arrive(j):
            src = first + j

            @pl.when(src != me)
            def _():
                dispatch(src, src).wait_recv()

        each(n2, arrive)
        came = recv[pl.ds(first, n2)].astype(F32).reshape(packed_rows, tile).astype(BF16)
        apart = jnp.dot(unpack_ref[...], came, preferred_element_type=F32)
        for j in range(blocks):
            xs[:, j * tile : (j + 1) * tile] = apart[
                j * group_rows : (j + 1) * group_rows
            ].astype(BF16)
        x = xs[...]
        for part in range(2):
            for low in range(0, half, piece):
                gate_pre = jnp.dot(
                    x, wgs[part, :, low : low + piece], preferred_element_type=F32
                )
                up_pre = jnp.dot(x, wus[part, :, low : low + piece], preferred_element_type=F32)
                hid[part, :, low : low + piece] = clamped_unit(gate_pre, up_pre)
        for j in range(blocks):
            total = jnp.zeros((group_rows, tile), F32)
            for part in range(2):
                partial = jnp.dot(
                    hid[part],
                    wds[part, :, j * tile : (j + 1) * tile],
                    preferred_element_type=F32,
                )
                total = total + partial.astype(BF16).astype(F32)
            totals[j * group_rows : (j + 1) * group_rows, :] = total
        joined = jnp.dot(pack_ref[...], totals[...].astype(BF16), preferred_element_type=F32)
        outb[pl.ds(first, n2)] = joined.reshape(n2, tall, tile).astype(BF16)

        def start(j):
            dst = first + (spot + 1 + j) % n2

            @pl.when(dst != me)
            def _():
                give_back(dst, me).start()

            @pl.when(dst == me)
            def _():
                ret[me] = outb[me]

        each(n2, start)

    def run_turn(i):
        run_group(i)
        for b, bit in enumerate(bits):

            @pl.when(i == b)
            def _():
                dense_finish(bit)
                if b + 1 < len(bits):
                    dense_start(bits[b + 1])
                else:
                    each(n2 - 1, lambda j: dense_copy2((spot + 1 + j) % n2, spot).start())

    each(n1, run_turn)
    each(n2 - 1, lambda i: dense_copy2((spot + 1 + i) % n2, (spot + 1 + i) % n2).wait_recv())
    dense_copy3(core).start()
    dense_copy3(core).wait_send()
    dense_copy3(peer).wait_recv()
    depth = din_ref.shape[1]
    dense_pre = jnp.dot(
        normed[...], dn[0].reshape(width, depth), preferred_element_type=F32
    )
    dense_hidden = jax.nn.silu(dense_pre).astype(BF16)
    step = width // n1
    for z in range(n1):
        branch = lax.dot_general(
            dense_hidden,
            dn[1, z].reshape(step, depth),
            (((1,), (1,)), ((), ())),
            preferred_element_type=F32,
        )
        acc[:, z * step : (z + 1) * step] = (
            jax.nn.sigmoid(dgate_ref[:, z * step : (z + 1) * step]) * branch
        )

    def combine_group(i):
        group = turn(i)
        first = group * n2

        def arrive(j):
            src = first + j

            @pl.when(src != me)
            def _():
                give_back(src, src).wait_recv()

        each(n2, arrive)
        back = ret[pl.ds(first, n2)].astype(F32).reshape(packed_rows, tile).astype(BF16)
        lanes = lax.broadcasted_iota(jnp.int32, (rows, packed_rows), 1) + first * tall
        wanted = jnp.concatenate(
            [
                jnp.where(places[:, k : k + 1] + j * cap == lanes, 1.0, 0.0).astype(BF16)
                for k in range(2)
                for j in range(blocks)
            ],
            axis=0,
        )
        picked = jnp.dot(wanted, back, preferred_element_type=F32)
        for j in range(blocks):
            total = acc[:, j * tile : (j + 1) * tile]
            for k in range(2):
                at = (k * blocks + j) * rows
                total = total + picked[at : at + rows] * weights_ref[:, k : k + 1]
            acc[:, j * tile : (j + 1) * tile] = total

    each(n1, combine_group)
    out_ref[...] = acc[...].astype(BF16)

    def drain(i):
        other = (me + 1 + i) % n
        dispatch(other, me).wait_send()
        give_back(other, me).wait_send()

    each(n - 1, drain)
    each(n2 - 1, lambda i: dense_copy2((spot + 1 + i) % n2, spot).wait_send())


LANES = 128


def gateway_kernel(
    sizes,
    routes_ref,
    weights_ref,
    tokens_ref,
    gain_ref,
    dgate_ref,
    din_ref,
    dout_ref,
    wg_ref,
    wu_ref,
    wd_ref,
    out_ref,
    routes_of,
    weights_of,
    dense,
    picks,
    wanted,
    columns,
    buf,
    recv,
    xs,
    hid,
    unpack_ref,
    pack_ref,
    outb,
    ret,
    accs,
    pout,
    fin,
    wgs,
    wus,
    wds,
    dn,
    w_local,
    w_send,
    w_recv,
    meta_send,
    meta_recv,
    dense_send,
    dense_recv,
    send1,
    recv1,
    send2,
    recv2,
    fin_send,
    fin_recv,
    dn_send,
    dn_recv,
):
    n, n1, n2, cap, blocks = sizes
    rows, width = tokens_ref.shape
    half = wg_ref.shape[1]
    tall = blocks * cap
    chunk = blocks * LANES
    chunks = width // chunk
    near = n // 2
    group_rows, packed_rows = n2 * cap, n2 * tall
    me = lax.axis_index("ep")
    core = lax.axis_index("tp")
    peer = 1 - core
    plane, spot = me // n2, me % n2
    side = plane // 2
    mine = me % near
    base = side * near
    is_gate = (plane + 1) // 2 % 2
    sibling = plane + 1 - 2 * (plane % 2)
    gate_plane = 1 + side
    far_gate = 2 - side
    gates_end = (plane + 2) % 4
    on_gate = is_gate == 1
    on_end = is_gate == 0

    def at(where):
        return {"ep": where}

    def each(count, act):
        def step(i, carry):
            act(i)
            return carry

        lax.fori_loop(0, count, step, 0)

    def remote(src, dst, send_sem, recv_sem, device):
        return pltpu.make_async_remote_copy(
            src_ref=src,
            dst_ref=dst,
            send_sem=send_sem,
            recv_sem=recv_sem,
            device_id=device,
            device_id_type=MESH,
        )

    barrier = pltpu.get_barrier_semaphore()

    def greet(device):
        pl.semaphore_signal(barrier, inc=1, device_id=device, device_id_type=MESH)

    each(near - 1, lambda i: greet(at(base + (mine + 1 + i) % near)))
    greet({"tp": peer})
    greet(at(far_gate * n2 + spot))

    @pl.when(on_gate)
    def _():
        greet(at(gates_end * n2 + spot))

    weight_pairs = ((wg_ref, wgs), (wu_ref, wus), (wd_ref, wds))
    for i, (src, dst) in enumerate(weight_pairs):
        pltpu.make_async_copy(src, dst.at[0], w_local.at[i]).start()

    @pl.when(core == 0)
    def _():
        dn[0, plane, spot] = din_ref[...]

    @pl.when(core == 1)
    def _():
        dn[1, plane, spot] = dout_ref[...]

    widened = tokens_ref[...].astype(F32)
    inv_scale = lax.rsqrt(jnp.mean(widened * widened, axis=1, keepdims=True) + NORM_EPS)
    normed = (widened * inv_scale * gain_ref[...]).astype(BF16)
    for c in range(chunks):
        for j in range(blocks):
            low = c * chunk + j * LANES
            dense[0, c, j * rows : (j + 1) * rows, :] = normed[:, low : low + LANES]
    routes_of[0] = routes_ref[...]
    weights_of[0] = weights_ref[...]

    def prepare(kind):
        experts = lax.broadcasted_iota(jnp.int32, (near, rows), 0) + base
        first, second = routes_of[kind, 0:1, :], routes_of[kind, 1:2, :]
        takes = (first == experts, second == experts)
        chosen = takes[0] | takes[1]
        earlier = (
            lax.broadcasted_iota(jnp.int32, (rows, rows), 0)
            < lax.broadcasted_iota(jnp.int32, (rows, rows), 1)
        )
        counted = jnp.dot(
            jnp.where(chosen, 1.0, 0.0).astype(BF16),
            jnp.where(earlier, 1.0, 0.0).astype(BF16),
            preferred_element_type=F32,
        )
        slots = counted.astype(jnp.int32)
        keys = jnp.concatenate(
            [jnp.where(chosen, slots + j * cap, -1) for j in range(blocks)], axis=1
        )
        hits = keys[:, None, :] == lax.broadcasted_iota(
            jnp.int32, (near, tall, blocks * rows), 1
        )
        picks[kind] = (
            jnp.where(hits, 1.0, 0.0).reshape(near * tall, blocks * rows).astype(BF16)
        )
        local = lax.broadcasted_iota(jnp.int32, (near, rows), 0) * tall
        places = [
            jnp.sum(
                jnp.where(take, counted + local.astype(F32) + n * tall, 0.0),
                axis=0,
                keepdims=True,
            )
            - n * tall
            for take in takes
        ]
        stack = jnp.concatenate(
            places + [weights_of[kind], jnp.zeros((4, rows), F32)], axis=0
        )
        turned = jnp.transpose(stack)
        columns[kind] = turned
        lanes = lax.broadcasted_iota(jnp.int32, (rows, near * tall), 1)
        for k in range(2):
            place = turned[:, k : k + 1].astype(jnp.int32)
            for j in range(blocks):
                top = (k * blocks + j) * rows
                wanted[kind, top : top + rows, :] = jnp.where(
                    place + j * cap == lanes, 1.0, 0.0
                ).astype(BF16)

    prepare(0)

    def packed_place(r):
        return (r // cap) % n2 * tall + r // group_rows * cap + r % cap

    upright = lax.broadcasted_iota(jnp.int32, (packed_rows, packed_rows), 0)
    across = lax.broadcasted_iota(jnp.int32, (packed_rows, packed_rows), 1)
    unpack_ref[...] = jnp.where(packed_place(upright) == across, 1.0, 0.0).astype(BF16)
    pack_ref[...] = jnp.where(packed_place(across) == upright, 1.0, 0.0).astype(BF16)
    for kind in range(3):
        accs[kind] = jnp.zeros((rows, width), F32)

    pl.semaphore_wait(barrier, 9 + is_gate + (near - 8))

    def meta_copies():
        slot = 2 - is_gate
        device = at(far_gate * n2 + spot)
        return (
            remote(routes_ref, routes_of.at[slot], meta_send.at[0], meta_recv.at[0, slot], device),
            remote(weights_ref, weights_of.at[slot], meta_send.at[1], meta_recv.at[1, slot], device),
        )

    def dense_copy(c):
        slot = 2 - is_gate
        return remote(
            dense.at[0, c],
            dense.at[slot, c],
            dense_send.at[c],
            dense_recv.at[slot, c],
            at(far_gate * n2 + spot),
        )

    def dense_start():
        for copy in meta_copies():
            copy.start()
        each(chunks, lambda c: dense_copy(c).start())

    def meta_wait(slot):
        device = at(far_gate * n2 + spot)
        remote(
            routes_ref, routes_of.at[slot], meta_send.at[0], meta_recv.at[0, slot], device
        ).wait_recv()
        remote(
            weights_ref, weights_of.at[slot], meta_send.at[1], meta_recv.at[1, slot], device
        ).wait_recv()

    def dense_wait(slot, c):
        remote(
            dense.at[0, c],
            dense.at[slot, c],
            dense_send.at[c],
            dense_recv.at[slot, c],
            at(far_gate * n2 + spot),
        ).wait_recv()

    def dn_up():
        block = dn.at[core, plane, spot]
        return remote(block, block, dn_send.at[0], dn_recv.at[0], at(sibling * n2 + spot))

    def dn_up_wait():
        block = dn.at[core, sibling, spot]
        remote(block, block, dn_send.at[0], dn_recv.at[0], at(sibling * n2 + spot)).wait_recv()

    def dn_cross(which):
        pair = dn.at[core, pl.ds(which * 2, 2), spot]
        return remote(pair, pair, dn_send.at[1], dn_recv.at[1], at(far_gate * n2 + spot))

    def dn_flat(part, other, slot):
        pair = dn.at[core, pl.ds(((side + part) % 2) * 2, 2), slot]
        return remote(
            pair,
            pair,
            dn_send.at[2 + part * n2 + other],
            dn_recv.at[2 + part * n2 + slot],
            at(plane * n2 + other),
        )

    def dn_swap(which):
        last = 2 + 2 * n2
        return remote(
            dn.at[which], dn.at[which], dn_send.at[last], dn_recv.at[last], {"tp": peer}
        )

    def weight_copy(i):
        src, dst = weight_pairs[i]
        return remote(src, dst.at[1], w_send.at[i], w_recv.at[i], {"tp": peer})

    def dispatch(kind, expert, c):
        late = (kind + 1) // 2
        group = (1 - late) * ((expert // n2 + plane) % 2) + late * (kind + 1)
        return remote(
            buf.at[kind, expert, c],
            recv.at[group, spot, c],
            send1.at[kind, expert, c],
            recv1.at[group, spot, c],
            at(base + expert),
        )

    def select(kind, c):
        found = jnp.dot(picks[kind], dense[kind, c], preferred_element_type=F32)
        buf[kind, :, c] = found.reshape(near, tall, LANES).astype(BF16)
        late = (kind + 1) // 2

        def start(i):
            expert = (mine + n2 + i) % near

            @pl.when(expert != mine)
            def _():
                dispatch(kind, expert, c).start()

            @pl.when(expert == mine)
            def _():
                recv[late * (kind + 1), spot, c] = buf[kind, mine, c]

        each(near, start)

    @pl.when(on_gate)
    def _():
        dense_start()

    @pl.when(on_end)
    def _():
        dn_up().start()

    for i in range(3):
        weight_copy(i).start()
    each(chunks, lambda c: select(0, c))

    @pl.when(on_end)
    def _():
        dense_start()

    @pl.when(on_gate)
    def _():
        dn_up_wait()
        dn_cross(side).start()
        each(n2 - 1, lambda i: dn_flat(0, (spot + 1 + i) % n2, spot).start())

    def hop(group):
        late, odd = group // 2, group % 2
        return (1 - late) * ((1 - odd) * plane + odd * sibling) + late * gate_plane

    def give_back(group, s, c):
        late, odd = group // 2, group % 2
        kind = late * (1 + odd)
        return remote(
            outb.at[group, s, c],
            ret.at[kind, mine, c],
            send2.at[group, s, c],
            recv2.at[kind, mine, c],
            at(hop(group) * n2 + s),
        )

    piece = min(256, half)

    def run_group(group):
        origin = hop(group) * n2
        kind = group // 2 * (1 + group % 2)
        for c in range(chunks):

            def arrive(s):
                @pl.when(origin + s != me)
                def _():
                    remote(
                        buf.at[0, 0, c],
                        recv.at[group, s, c],
                        send1.at[0, 0, c],
                        recv1.at[group, s, c],
                        at(origin + s),
                    ).wait_recv()

            each(n2, arrive)
            came = recv[group, :, c].reshape(packed_rows, LANES)
            apart = jnp.dot(unpack_ref[...], came, preferred_element_type=F32)
            for j in range(blocks):
                low = c * chunk + j * LANES
                xs[:, low : low + LANES] = apart[
                    j * group_rows : (j + 1) * group_rows
                ].astype(BF16)
        x = xs[...]
        for part in range(2):
            for low in range(0, half, piece):
                gate_pre = jnp.dot(
                    x, wgs[part, :, low : low + piece], preferred_element_type=F32
                )
                up_pre = jnp.dot(x, wus[part, :, low : low + piece], preferred_element_type=F32)
                hid[part, :, low : low + piece] = clamped_unit(gate_pre, up_pre)
        for c in range(chunks):
            total = jnp.dot(
                hid[0], wds[0, :, c * chunk : (c + 1) * chunk], preferred_element_type=F32
            ) + jnp.dot(
                hid[1], wds[1, :, c * chunk : (c + 1) * chunk], preferred_element_type=F32
            )
            stacked = jnp.concatenate(
                [total[:, j * LANES : (j + 1) * LANES] for j in range(blocks)], axis=0
            ).astype(BF16)
            joined = jnp.dot(pack_ref[...], stacked, preferred_element_type=F32)
            outb[group, :, c] = joined.reshape(n2, tall, LANES).astype(BF16)

            def start(i):
                s = (spot + 1 + i) % n2

                @pl.when(origin + s != me)
                def _():
                    give_back(group, s, c).start()

                @pl.when(origin + s == me)
                def _():
                    ret[kind, mine, c] = outb[group, s, c]

            each(n2, start)

    def gather(kind, c):
        def arrive(i):
            expert = (mine + 1 + i) % near
            remote(
                outb.at[0, 0, c],
                ret.at[kind, expert, c],
                send2.at[0, 0, c],
                recv2.at[kind, expert, c],
                at(base + expert),
            ).wait_recv()

        each(near - 1, arrive)
        back = ret[kind, :, c].reshape(near * tall, LANES)
        picked = jnp.dot(wanted[kind], back, preferred_element_type=F32)
        totals = []
        for j in range(blocks):
            total = jnp.zeros((rows, LANES), F32)
            for k in range(2):
                top = (k * blocks + j) * rows
                total = total + picked[top : top + rows] * columns[kind, :, 2 + k : 3 + k]
            totals.append(total)
        return jnp.concatenate(totals, axis=1)

    def fin_copy(kind, c):
        where = (kind - 1) * gates_end + (2 - kind) * far_gate
        return remote(
            pout.at[kind, c],
            fin.at[c],
            fin_send.at[kind, c],
            fin_recv.at[c],
            at(where * n2 + spot),
        )

    def combine(kind, c):
        span = pl.ds(pl.multiple_of(c * chunk, chunk), chunk)
        pout[kind, c] = (accs[kind, :, span] + gather(kind, c)).astype(BF16)
        fin_copy(kind, c).start()

    def run_turn(i):
        kind = 1 + i // 2
        part = chunks // 2

        @pl.when(on_gate)
        def _():
            @pl.when(i % 2 == 0)
            def _():
                meta_wait(kind)
                prepare(kind)

            def take(m):
                c = i % 2 * part + m
                dense_wait(kind, c)
                select(kind, c)

            each(part, take)

            @pl.when(i == 3)
            def _():
                dn_cross(1 - side).wait_recv()
                each(n2 - 1, lambda m: dn_flat(1, (spot + 1 + m) % n2, spot).start())
                each(part, lambda c: combine(1, c))

        @pl.when(i == 0)
        def _():
            for w, (src, dst) in enumerate(weight_pairs):
                pltpu.make_async_copy(src, dst.at[0], w_local.at[w]).wait()
            for w in range(3):
                weight_copy(w).wait()

        run_group(i)

    each(n1, run_turn)

    @pl.when(on_gate)
    def _():
        part = chunks // 2
        each(chunks - part, lambda c: combine(1, part + c))
        for p in range(2):
            each(
                n2 - 1,
                lambda m: dn_flat(p, (spot + 1 + m) % n2, (spot + 1 + m) % n2).wait_recv(),
            )
        dn_swap(core).start()
        dn_swap(peer).wait_recv()
        depth = din_ref.shape[1]
        for kind in (2, 0):
            x = jnp.concatenate(
                [
                    dense[kind, c, j * rows : (j + 1) * rows, :]
                    for c in range(chunks)
                    for j in range(blocks)
                ],
                axis=1,
            )
            pre = jnp.dot(x, dn[0].reshape(width, depth), preferred_element_type=F32)
            dense_hidden = jax.nn.silu(pre).astype(BF16)
            step = width // n1
            for z in range(n1):
                branch = lax.dot_general(
                    dense_hidden,
                    dn[1, z].reshape(step, depth),
                    (((1,), (1,)), ((), ())),
                    preferred_element_type=F32,
                )
                accs[kind, :, z * step : (z + 1) * step] = (
                    jax.nn.sigmoid(dgate_ref[:, z * step : (z + 1) * step]) * branch
                )
        each(chunks, lambda c: combine(2, c))

    def own(c):
        span = pl.ds(pl.multiple_of(c * chunk, chunk), chunk)
        accs[0, :, span] = accs[0, :, span] + gather(0, c)

    each(chunks, own)

    def finish(c):
        remote(
            pout.at[1, c],
            fin.at[c],
            fin_send.at[1, c],
            fin_recv.at[c],
            at(far_gate * n2 + spot),
        ).wait_recv()
        span = pl.ds(pl.multiple_of(c * chunk, chunk), chunk)
        out_ref[:, span] = (accs[0, :, span] + fin[c].astype(F32)).astype(BF16)

    each(chunks, finish)

    def drain_dispatch(kind):
        def go(i):
            each(chunks, lambda c: dispatch(kind, (mine + 1 + i) % near, c).wait_send())

        each(near - 1, go)

    drain_dispatch(0)
    for copy in meta_copies():
        copy.wait_send()
    each(chunks, lambda c: dense_copy(c).wait_send())

    def drain_back(group):
        def go(s):
            @pl.when(hop(group) * n2 + s != me)
            def _():
                each(chunks, lambda c: give_back(group, s, c).wait_send())

        each(n2, go)

    each(n1, drain_back)

    @pl.when(on_end)
    def _():
        dn_up().wait_send()

    @pl.when(on_gate)
    def _():
        for kind in (1, 2):
            drain_dispatch(kind)
            each(chunks, lambda c: fin_copy(kind, c).wait_send())
        dn_cross(side).wait_send()
        for p in range(2):
            each(n2 - 1, lambda m: dn_flat(p, (spot + 1 + m) % n2, spot).wait_send())
        dn_swap(core).wait_send()


def gateway_call(sizes, operands):
    n, n1, n2, cap, blocks = sizes
    tokens, dense_in, w_gate = operands[2], operands[5], operands[7]
    rows, width = tokens.shape
    half, depth = w_gate.shape[1], dense_in.shape[1]
    tall, near = blocks * cap, n // 2
    chunk = blocks * LANES
    chunks = width // chunk
    packed = n2 * tall
    vmem = pl.BlockSpec(memory_space=pltpu.VMEM)
    anywhere = pl.BlockSpec(memory_space=pl.ANY)
    dma = pltpu.SemaphoreType.DMA
    return pl.pallas_call(
        functools.partial(gateway_kernel, sizes),
        out_shape=jax.ShapeDtypeStruct((rows, width), BF16),
        in_specs=[vmem] * 7 + [anywhere] * 3,
        out_specs=vmem,
        scratch_shapes=[
            pltpu.VMEM((3, 2, rows), jnp.int32),
            pltpu.VMEM((3, 2, rows), F32),
            pltpu.VMEM((3, chunks, blocks * rows, LANES), BF16),
            pltpu.VMEM((3, near * tall, blocks * rows), BF16),
            pltpu.VMEM((3, 2 * blocks * rows, near * tall), BF16),
            pltpu.VMEM((3, rows, 8), F32),
            pltpu.VMEM((3, near, chunks, tall, LANES), BF16),
            pltpu.VMEM((n1, n2, chunks, tall, LANES), BF16),
            pltpu.VMEM((n2 * cap, width), BF16),
            pltpu.VMEM((2, n2 * cap, half), BF16),
            pltpu.VMEM((packed, packed), BF16),
            pltpu.VMEM((packed, packed), BF16),
            pltpu.VMEM((n1, n2, chunks, tall, LANES), BF16),
            pltpu.VMEM((3, near, chunks, tall, LANES), BF16),
            pltpu.VMEM((3, rows, width), F32),
            pltpu.VMEM((3, chunks, rows, chunk), BF16),
            pltpu.VMEM((chunks, rows, chunk), BF16),
            pltpu.VMEM((2, width, half), BF16),
            pltpu.VMEM((2, width, half), BF16),
            pltpu.VMEM((2, half, width), BF16),
            pltpu.VMEM((2, n1, n2, width // n, depth), BF16),
            dma((3,)),
            dma((3,)),
            dma((3,)),
            dma((2,)),
            dma((2, 3)),
            dma((chunks,)),
            dma((3, chunks)),
            dma((3, near, chunks)),
            dma((n1, n2, chunks)),
            dma((n1, n2, chunks)),
            dma((3, near, chunks)),
            dma((3, chunks)),
            dma((chunks,)),
            dma((3 + 2 * n2,)),
            dma((3 + 2 * n2,)),
        ],
        compiler_params=pltpu.CompilerParams(
            collective_id=0, has_side_effects=True, vmem_limit_bytes=60 * 1024 * 1024
        ),
    )(*operands)


def shards(
    tokens, norm_gain, routes, route_weights, w_gate, w_up, w_down, dense_in, dense_out, dense_gate
):
    rows, width = tokens.shape
    top_count = routes.shape[1]
    n = lax.axis_size("ep")
    capacity = (4 * rows * top_count + 3 * n - 1) // (3 * n)
    cap = capacity
    blocks = 8 // math.gcd(cap, 8)
    tall, tile = blocks * cap, width // blocks
    n2 = 1
    while n2 * n2 < n:
        n2 *= 2
    n1 = n // n2
    half = w_gate.shape[2]
    depth = dense_in.shape[1]
    if n1 == 4 and n2 == 4 and width % (2 * blocks * LANES) == 0 and width % n == 0:
        return gateway_call(
            (n, n1, n2, cap, blocks),
            (
                routes.T,
                route_weights.T,
                tokens,
                norm_gain.reshape(1, width),
                dense_gate.reshape(1, width),
                dense_in,
                dense_out,
                w_gate[0],
                w_up[0],
                w_down[0],
            ),
        )
    vmem = pl.BlockSpec(memory_space=pltpu.VMEM)
    anywhere = pl.BlockSpec(memory_space=pl.ANY)
    dma = pltpu.SemaphoreType.DMA
    slab = pltpu.VMEM((n, tall, tile), BF16)
    return pl.pallas_call(
        functools.partial(layer_kernel, (n, n1, n2, cap, blocks)),
        out_shape=jax.ShapeDtypeStruct((rows, width), BF16),
        in_specs=[vmem] * 8 + [anywhere] * 3,
        out_specs=vmem,
        scratch_shapes=[
            pltpu.VMEM((rows, width), BF16),
            pltpu.VMEM((n1, n2, blocks * rows), jnp.int32),
            pltpu.VMEM((blocks * rows, tile), BF16),
            pltpu.VMEM((rows, 2), jnp.int32),
            pltpu.VMEM((n2 * cap, width), BF16),
            pltpu.VMEM((n2 * tall, tile), F32),
            pltpu.VMEM((n2 * tall, n2 * tall), BF16),
            pltpu.VMEM((n2 * tall, n2 * tall), BF16),
            slab,
            slab,
            slab,
            slab,
            pltpu.VMEM((2, width, half), BF16),
            pltpu.VMEM((2, width, half), BF16),
            pltpu.VMEM((2, half, width), BF16),
            pltpu.VMEM((2, n2 * cap, half), BF16),
            pltpu.VMEM((2, n1, n2, width // n, depth), BF16),
            pltpu.VMEM((rows, width), F32),
            dma((n,)),
            dma((n,)),
            dma((n,)),
            dma((n,)),
            dma((3,)),
            dma((3,)),
            dma((3,)),
            dma((n1,)),
            dma((n1,)),
            dma((n2,)),
            dma((n2,)),
            dma,
            dma,
        ],
        compiler_params=pltpu.CompilerParams(
            collective_id=0, has_side_effects=True, vmem_limit_bytes=60 * 1024 * 1024
        ),
    )(
        routes.T,
        routes,
        route_weights,
        tokens,
        norm_gain.reshape(1, width),
        dense_gate.reshape(1, width),
        dense_in,
        dense_out,
        w_gate[0],
        w_up[0],
        w_down[0],
    )


def solution(mesh):
    placed = (
        P(("ep", "tp"), None),
        P(),
        P(("ep", "tp"), None),
        P(("ep", "tp"), None),
        P("ep", None, "tp"),
        P("ep", None, "tp"),
        P("ep", "tp", None),
        P("ep", None),
        P("ep", None),
        P(),
    )
    return jax.shard_map(
        shards, mesh=mesh, in_specs=placed, out_specs=P(("ep", "tp"), None), check_vma=False
    )
```

```python
import functools
import math

import jax
import jax.numpy as jnp
from jax import lax
from jax.experimental import pallas as pl
from jax.experimental.pallas import tpu as pltpu
from jax.sharding import PartitionSpec as P

CLAMP_LIMIT = 7.0
SLOPE_ALPHA = 1.702
NORM_EPS = 1e-06
MESH = pl.DeviceIdType.MESH
F32 = jnp.float32
BF16 = jnp.bfloat16


def clamped_unit(gate_pre, up_pre):
    gate_clip = jnp.minimum(gate_pre, CLAMP_LIMIT)
    up_clip = jnp.clip(up_pre, -CLAMP_LIMIT, CLAMP_LIMIT)
    return ((up_clip + 1.0) * gate_clip * jax.nn.sigmoid(SLOPE_ALPHA * gate_clip)).astype(BF16)


def layer_kernel(
    sizes,
    routes_t_ref,
    routes_ref,
    weights_ref,
    tokens_ref,
    gain_ref,
    dgate_ref,
    din_ref,
    dout_ref,
    wg_ref,
    wu_ref,
    wd_ref,
    out_ref,
    normed,
    keys,
    stacked,
    places,
    xs,
    totals,
    unpack_ref,
    pack_ref,
    buf,
    recv,
    outb,
    ret,
    wgs,
    wus,
    wds,
    hid,
    dn,
    acc,
    send1,
    recv1,
    send2,
    recv2,
    w_local,
    w_send,
    w_recv,
    ds1,
    dr1,
    ds2,
    dr2,
    ds3,
    dr3,
):
    n, n1, n2, cap, blocks = sizes
    rows, width = tokens_ref.shape
    half = wg_ref.shape[1]
    tall, tile = blocks * cap, width // blocks
    group_rows, packed_rows = n2 * cap, n2 * blocks * cap
    me = lax.axis_index("ep")
    core = lax.axis_index("tp")
    plane, spot = me // n2, me % n2
    peer = 1 - core

    barrier = pltpu.get_barrier_semaphore()

    def greet(i, carry):
        pl.semaphore_signal(
            barrier, inc=1, device_id={"ep": (me + i) % n}, device_id_type=MESH
        )
        return carry

    lax.fori_loop(1, n, greet, 0)
    pl.semaphore_signal(barrier, inc=1, device_id={"tp": peer}, device_id_type=MESH)

    weight_pairs = ((wg_ref, wgs), (wu_ref, wus), (wd_ref, wds))
    for i, (src, dst) in enumerate(weight_pairs):
        pltpu.make_async_copy(src, dst.at[0], w_local.at[i]).start()

    @pl.when(core == 0)
    def _():
        dn[0, plane, spot] = din_ref[...]

    @pl.when(core == 1)
    def _():
        dn[1, plane, spot] = dout_ref[...]

    widened = tokens_ref[...].astype(F32)
    inv_scale = lax.rsqrt(jnp.mean(widened * widened, axis=1, keepdims=True) + NORM_EPS)
    normed[...] = (widened * inv_scale * gain_ref[...]).astype(BF16)
    for j in range(blocks):
        stacked[j * rows : (j + 1) * rows, :] = normed[:, j * tile : (j + 1) * tile]

    expert_ids = lax.broadcasted_iota(jnp.int32, (n, rows), 0)
    chosen = (routes_t_ref[0:1, :] == expert_ids) | (routes_t_ref[1:2, :] == expert_ids)
    earlier = (
        lax.broadcasted_iota(jnp.int32, (rows, rows), 0)
        < lax.broadcasted_iota(jnp.int32, (rows, rows), 1)
    )
    counted = jnp.dot(
        jnp.where(chosen, 1.0, 0.0).astype(BF16),
        jnp.where(earlier, 1.0, 0.0).astype(BF16),
        preferred_element_type=F32,
    )
    for j in range(blocks):
        found = jnp.where(chosen, counted.astype(jnp.int32) + j * cap, -1)
        for z in range(n1):
            keys[z, :, j * rows : (j + 1) * rows] = found[z * n2 : (z + 1) * n2]
    experts_across = lax.broadcasted_iota(jnp.int32, (rows, n), 1)
    takes = [routes_ref[:, k : k + 1] == experts_across for k in range(2)]
    before = (
        lax.broadcasted_iota(jnp.int32, (rows, rows), 0)
        > lax.broadcasted_iota(jnp.int32, (rows, rows), 1)
    )
    counts = jnp.dot(
        jnp.where(before, 1.0, 0.0).astype(BF16),
        jnp.where(takes[0] | takes[1], 1.0, 0.0).astype(BF16),
        preferred_element_type=F32,
    )
    for k in range(2):
        slot = jnp.sum(jnp.where(takes[k], counts, 0.0), axis=1, keepdims=True)
        places[:, k : k + 1] = routes_ref[:, k : k + 1] * tall + slot.astype(jnp.int32)

    pl.semaphore_wait(barrier, n)

    def weight_copy(i):
        src, dst = weight_pairs[i]
        return pltpu.make_async_remote_copy(
            src_ref=src,
            dst_ref=dst.at[1],
            send_sem=w_send.at[i],
            recv_sem=w_recv.at[i],
            device_id={"tp": peer},
            device_id_type=MESH,
        )

    def dense_copy1(bit, block):
        other = plane + bit - 2 * bit * ((plane // bit) % 2)
        return pltpu.make_async_remote_copy(
            src_ref=dn.at[core, block, spot],
            dst_ref=dn.at[core, block, spot],
            send_sem=ds1.at[block],
            recv_sem=dr1.at[block],
            device_id={"ep": other * n2 + spot},
            device_id_type=MESH,
        )

    bits = [1 << b for b in reversed(range(n1.bit_length() - 1))]

    def dense_held(bit, where):
        return [where % (2 * bit) + m * 2 * bit for m in range(n1 // (2 * bit))]

    def dense_start(bit):
        for block in dense_held(bit, plane):
            dense_copy1(bit, block).start()

    def dense_finish(bit):
        for block in dense_held(bit, plane + bit - 2 * bit * ((plane // bit) % 2)):
            dense_copy1(bit, block).wait_recv()
        for block in dense_held(bit, plane):
            dense_copy1(bit, block).wait_send()

    def dense_copy2(other, slot):
        return pltpu.make_async_remote_copy(
            src_ref=dn.at[core, :, slot],
            dst_ref=dn.at[core, :, slot],
            send_sem=ds2.at[other],
            recv_sem=dr2.at[slot],
            device_id={"ep": plane * n2 + other},
            device_id_type=MESH,
        )

    def dense_copy3(which):
        return pltpu.make_async_remote_copy(
            src_ref=dn.at[which],
            dst_ref=dn.at[which],
            send_sem=ds3,
            recv_sem=dr3,
            device_id={"tp": peer},
            device_id_type=MESH,
        )

    def each(count, act):
        def step(i, carry):
            act(i)
            return carry

        lax.fori_loop(0, count, step, 0)

    dense_start(bits[0])
    for i in range(3):
        weight_copy(i).start()

    def dispatch(dst, slot):
        return pltpu.make_async_remote_copy(
            src_ref=buf.at[dst],
            dst_ref=recv.at[slot],
            send_sem=send1.at[dst],
            recv_sem=recv1.at[slot],
            device_id={"ep": dst},
            device_id_type=MESH,
        )

    def give_back(dst, slot):
        return pltpu.make_async_remote_copy(
            src_ref=outb.at[dst],
            dst_ref=ret.at[slot],
            send_sem=send2.at[dst],
            recv_sem=recv2.at[slot],
            device_id={"ep": dst},
            device_id_type=MESH,
        )

    def partner_plane(x):
        return sum(((plane // b) % 2 + (x // b) % 2) % 2 * b for b in bits)

    def turn(i):
        return partner_plane(i % 2 * (n1 // 2) + i // 2)

    def send_group(i):
        group = partner_plane((i + n1 // 2) % n1)
        first = group * n2
        wanted = keys[group]
        picks = wanted[:, None, :] == lax.broadcasted_iota(
            jnp.int32, (n2, tall, blocks * rows), 1
        )
        picks = jnp.where(picks, 1.0, 0.0).reshape(packed_rows, blocks * rows).astype(BF16)
        found = jnp.dot(picks, stacked[...], preferred_element_type=F32)
        buf[pl.ds(first, n2)] = found.reshape(n2, tall, tile).astype(BF16)

        def start(j):
            dst = first + (spot + 1 + j) % n2

            @pl.when(dst != me)
            def _():
                dispatch(dst, me).start()

            @pl.when(dst == me)
            def _():
                recv[me] = buf[me]

        each(n2, start)

    each(n1, send_group)


    for i, (src, dst) in enumerate(weight_pairs):
        pltpu.make_async_copy(src, dst.at[0], w_local.at[i]).wait()
    for i in range(3):
        weight_copy(i).wait()

    piece = min(256, half)
    upright = lax.broadcasted_iota(jnp.int32, (packed_rows, packed_rows), 0)
    across = lax.broadcasted_iota(jnp.int32, (packed_rows, packed_rows), 1)

    def packed_place(r):
        return (r // cap) % n2 * tall + r // group_rows * cap + r % cap

    unpack = jnp.where(packed_place(upright) == across, 1.0, 0.0).astype(BF16)
    pack = jnp.where(packed_place(across) == upright, 1.0, 0.0).astype(BF16)
    unpack_ref[...] = unpack
    pack_ref[...] = pack

    def run_group(i):
        group = turn(i)
        first = group * n2

        def arrive(j):
            src = first + j

            @pl.when(src != me)
            def _():
                dispatch(src, src).wait_recv()

        each(n2, arrive)
        came = recv[pl.ds(first, n2)].astype(F32).reshape(packed_rows, tile).astype(BF16)
        apart = jnp.dot(unpack_ref[...], came, preferred_element_type=F32)
        for j in range(blocks):
            xs[:, j * tile : (j + 1) * tile] = apart[
                j * group_rows : (j + 1) * group_rows
            ].astype(BF16)
        x = xs[...]
        for part in range(2):
            for low in range(0, half, piece):
                gate_pre = jnp.dot(
                    x, wgs[part, :, low : low + piece], preferred_element_type=F32
                )
                up_pre = jnp.dot(x, wus[part, :, low : low + piece], preferred_element_type=F32)
                hid[part, :, low : low + piece] = clamped_unit(gate_pre, up_pre)
        for j in range(blocks):
            total = jnp.zeros((group_rows, tile), F32)
            for part in range(2):
                partial = jnp.dot(
                    hid[part],
                    wds[part, :, j * tile : (j + 1) * tile],
                    preferred_element_type=F32,
                )
                total = total + partial.astype(BF16).astype(F32)
            totals[j * group_rows : (j + 1) * group_rows, :] = total
        joined = jnp.dot(pack_ref[...], totals[...].astype(BF16), preferred_element_type=F32)
        outb[pl.ds(first, n2)] = joined.reshape(n2, tall, tile).astype(BF16)

        def start(j):
            dst = first + (spot + 1 + j) % n2

            @pl.when(dst != me)
            def _():
                give_back(dst, me).start()

            @pl.when(dst == me)
            def _():
                ret[me] = outb[me]

        each(n2, start)

    def run_turn(i):
        run_group(i)
        for b, bit in enumerate(bits):

            @pl.when(i == b)
            def _():
                dense_finish(bit)
                if b + 1 < len(bits):
                    dense_start(bits[b + 1])
                else:
                    each(n2 - 1, lambda j: dense_copy2((spot + 1 + j) % n2, spot).start())

    each(n1, run_turn)
    each(n2 - 1, lambda i: dense_copy2((spot + 1 + i) % n2, (spot + 1 + i) % n2).wait_recv())
    dense_copy3(core).start()
    dense_copy3(core).wait_send()
    dense_copy3(peer).wait_recv()
    depth = din_ref.shape[1]
    dense_pre = jnp.dot(
        normed[...], dn[0].reshape(width, depth), preferred_element_type=F32
    )
    dense_hidden = jax.nn.silu(dense_pre).astype(BF16)
    step = width // n1
    for z in range(n1):
        branch = lax.dot_general(
            dense_hidden,
            dn[1, z].reshape(step, depth),
            (((1,), (1,)), ((), ())),
            preferred_element_type=F32,
        )
        acc[:, z * step : (z + 1) * step] = (
            jax.nn.sigmoid(dgate_ref[:, z * step : (z + 1) * step]) * branch
        )

    def combine_group(i):
        group = turn(i)
        first = group * n2

        def arrive(j):
            src = first + j

            @pl.when(src != me)
            def _():
                give_back(src, src).wait_recv()

        each(n2, arrive)
        back = ret[pl.ds(first, n2)].astype(F32).reshape(packed_rows, tile).astype(BF16)
        lanes = lax.broadcasted_iota(jnp.int32, (rows, packed_rows), 1) + first * tall
        wanted = jnp.concatenate(
            [
                jnp.where(places[:, k : k + 1] + j * cap == lanes, 1.0, 0.0).astype(BF16)
                for k in range(2)
                for j in range(blocks)
            ],
            axis=0,
        )
        picked = jnp.dot(wanted, back, preferred_element_type=F32)
        for j in range(blocks):
            total = acc[:, j * tile : (j + 1) * tile]
            for k in range(2):
                at = (k * blocks + j) * rows
                total = total + picked[at : at + rows] * weights_ref[:, k : k + 1]
            acc[:, j * tile : (j + 1) * tile] = total

    each(n1, combine_group)
    out_ref[...] = acc[...].astype(BF16)

    def drain(i):
        other = (me + 1 + i) % n
        dispatch(other, me).wait_send()
        give_back(other, me).wait_send()

    each(n - 1, drain)
    each(n2 - 1, lambda i: dense_copy2((spot + 1 + i) % n2, spot).wait_send())


LANES = 128


def gateway_kernel(
    sizes,
    routes_ref,
    weights_ref,
    tokens_ref,
    gain_ref,
    dgate_ref,
    din_ref,
    dout_ref,
    wg_ref,
    wu_ref,
    wd_ref,
    out_ref,
    routes_of,
    weights_of,
    dense,
    picks,
    wanted,
    columns,
    buf,
    recv,
    xs,
    hid,
    unpack_ref,
    pack_ref,
    outb,
    ret,
    relay,
    accs,
    pout,
    fin,
    wgs,
    wus,
    wds,
    dn,
    w_local,
    w_send,
    w_recv,
    meta_send,
    meta_recv,
    dense_send,
    dense_recv,
    send1,
    recv1,
    send2,
    recv2,
    fin_send,
    fin_recv,
    dn_send,
    dn_recv,
    relay_send,
    relay_recv,
    clear,
):
    n, n1, n2, cap, blocks = sizes
    rows, width = tokens_ref.shape
    half = wg_ref.shape[1]
    tall = blocks * cap
    chunk = blocks * LANES
    chunks = width // chunk
    near = n // 2
    group_rows, packed_rows = n2 * cap, n2 * tall
    me = lax.axis_index("ep")
    core = lax.axis_index("tp")
    peer = 1 - core
    plane, spot = me // n2, me % n2
    side = plane // 2
    mine = me % near
    base = side * near
    is_gate = (plane + 1) // 2 % 2
    sibling = plane + 1 - 2 * (plane % 2)
    gate_plane = 1 + side
    far_gate = 2 - side
    far_end = 3 - 3 * side
    on_gate = is_gate == 1
    on_end = is_gate == 0

    def at(where):
        return {"ep": where}

    def each(count, act):
        def step(i, carry):
            act(i)
            return carry

        lax.fori_loop(0, count, step, 0)

    def remote(src, dst, send_sem, recv_sem, device):
        return pltpu.make_async_remote_copy(
            src_ref=src,
            dst_ref=dst,
            send_sem=send_sem,
            recv_sem=recv_sem,
            device_id=device,
            device_id_type=MESH,
        )

    barrier = pltpu.get_barrier_semaphore()

    def greet(device):
        pl.semaphore_signal(barrier, inc=1, device_id=device, device_id_type=MESH)

    each(near - 1, lambda i: greet(at(base + (mine + 1 + i) % near)))
    greet({"tp": peer})
    greet(at(far_gate * n2 + spot))

    @pl.when(on_gate)
    def _():
        greet(at(far_end * n2 + spot))

    weight_pairs = ((wg_ref, wgs), (wu_ref, wus), (wd_ref, wds))
    for i, (src, dst) in enumerate(weight_pairs):
        pltpu.make_async_copy(src, dst.at[0], w_local.at[i]).start()

    @pl.when(core == 0)
    def _():
        dn[0, plane, spot] = din_ref[...]

    @pl.when(core == 1)
    def _():
        dn[1, plane, spot] = dout_ref[...]

    with jax.named_scope("norm"):
        widened = tokens_ref[...].astype(F32)
        inv_scale = lax.rsqrt(jnp.mean(widened * widened, axis=1, keepdims=True) + NORM_EPS)
        normed = (widened * inv_scale * gain_ref[...]).astype(BF16)
        for c in range(chunks):
            for j in range(blocks):
                low = c * chunk + j * LANES
                dense[0, c, j * rows : (j + 1) * rows, :] = normed[:, low : low + LANES]
    routes_of[0] = routes_ref[...]
    weights_of[0] = weights_ref[...]

    def prepare(kind):
        experts = lax.broadcasted_iota(jnp.int32, (near, rows), 0) + base
        first, second = routes_of[kind, 0:1, :], routes_of[kind, 1:2, :]
        takes = (first == experts, second == experts)
        chosen = takes[0] | takes[1]
        earlier = (
            lax.broadcasted_iota(jnp.int32, (rows, rows), 0)
            < lax.broadcasted_iota(jnp.int32, (rows, rows), 1)
        )
        counted = jnp.dot(
            jnp.where(chosen, 1.0, 0.0).astype(BF16),
            jnp.where(earlier, 1.0, 0.0).astype(BF16),
            preferred_element_type=F32,
        )
        slots = counted.astype(jnp.int32)
        keys = jnp.concatenate(
            [jnp.where(chosen, slots + j * cap, -1) for j in range(blocks)], axis=1
        )
        hits = keys[:, None, :] == lax.broadcasted_iota(
            jnp.int32, (near, tall, blocks * rows), 1
        )
        picks[kind] = (
            jnp.where(hits, 1.0, 0.0).reshape(near * tall, blocks * rows).astype(BF16)
        )
        local = lax.broadcasted_iota(jnp.int32, (near, rows), 0) * tall
        places = [
            jnp.sum(
                jnp.where(take, counted + local.astype(F32) + n * tall, 0.0),
                axis=0,
                keepdims=True,
            )
            - n * tall
            for take in takes
        ]
        stack = jnp.concatenate(
            places + [weights_of[kind], jnp.zeros((4, rows), F32)], axis=0
        )
        turned = jnp.transpose(stack)
        columns[kind] = turned
        lanes = lax.broadcasted_iota(jnp.int32, (rows, near * tall), 1)
        for k in range(2):
            place = turned[:, k : k + 1].astype(jnp.int32)
            for j in range(blocks):
                top = (k * blocks + j) * rows
                wanted[kind, top : top + rows, :] = jnp.where(
                    place + j * cap == lanes, 1.0, 0.0
                ).astype(BF16)

    with jax.named_scope("prepare0"):
        prepare(0)

    def packed_place(r):
        return (r // cap) % n2 * tall + r // group_rows * cap + r % cap

    upright = lax.broadcasted_iota(jnp.int32, (packed_rows, packed_rows), 0)
    across = lax.broadcasted_iota(jnp.int32, (packed_rows, packed_rows), 1)
    unpack_ref[...] = jnp.where(packed_place(upright) == across, 1.0, 0.0).astype(BF16)
    pack_ref[...] = jnp.where(packed_place(across) == upright, 1.0, 0.0).astype(BF16)

    def meta_copies():
        slot = 2 - is_gate
        device = at(far_gate * n2 + spot)
        return (
            remote(routes_ref, routes_of.at[slot], meta_send.at[0], meta_recv.at[0, slot - 1], device),
            remote(weights_ref, weights_of.at[slot], meta_send.at[1], meta_recv.at[1, slot - 1], device),
        )

    def meta_wait(slot):
        device = at(far_gate * n2 + spot)
        remote(
            routes_ref, routes_of.at[slot], meta_send.at[0], meta_recv.at[0, slot - 1], device
        ).wait_recv()
        remote(
            weights_ref, weights_of.at[slot], meta_send.at[1], meta_recv.at[1, slot - 1], device
        ).wait_recv()

    def dense_copy(slot, c):
        return remote(
            dense.at[0, c],
            dense.at[slot, c],
            dense_send,
            dense_recv.at[slot - 1, c],
            at(far_gate * n2 + spot),
        )

    def dense_start():
        for c in range(chunks):
            dense_copy(2 - is_gate, c).start()

    def dn_block(which, index, target):
        block = dn.at[core, which, spot]
        return remote(
            block, block, dn_send.at[index], dn_recv.at[index], at(target * n2 + spot)
        )

    def dn_near(which):
        return dn_block(which, 0, sibling)

    def dn_cross(which):
        return dn_block(which, 1, far_gate)

    def dn_far(which):
        return dn_block(which, 2, far_gate)

    def dn_down(order):
        return dn_block(far_end if order else far_gate, 3 + order, sibling)

    first_bit, second_bit = 1 + core, 2 - core
    first_spot = spot + first_bit - 2 * first_bit * (spot // first_bit % 2)
    second_spot = spot + second_bit - 2 * second_bit * (spot // second_bit % 2)

    def dn_step(step, slot):
        columns_of = dn.at[core, :, slot]
        return remote(
            columns_of,
            columns_of,
            dn_send.at[5 + step],
            dn_recv.at[5 + step],
            at(plane * n2 + (second_spot if step else first_spot)),
        )

    def dn_start(step):
        dn_step(step, spot).start()
        if step:
            dn_step(step, first_spot).start()

    def dn_bytes(step):
        return dn_step(step, pl.ds(0, 2) if step else 0)

    def dn_swap(which):
        last = 7
        return remote(
            dn.at[which], dn.at[which], dn_send.at[last], dn_recv.at[last], {"tp": peer}
        )

    def weight_copy(i):
        src, dst = weight_pairs[i]
        return remote(src, dst.at[1], w_send.at[i], w_recv.at[i], {"tp": peer})

    spots = [(spot + i) % n2 for i in range(n2)]
    inner = plane % 2 * n2
    outer = n2 - inner

    def dispatch(kind, away, i, c):
        expert = (outer if away else inner) + spots[i]
        group = kind + 1 if kind else away
        return remote(
            buf.at[kind, expert] if c is None else buf.at[kind, expert, c],
            recv.at[group, spot] if c is None else recv.at[group, spot, c],
            send1.at[kind * 2 + away],
            recv1.at[group * chunks + (c or 0)],
            at(base + expert),
        )

    def dispatched(kind, away):
        sent = buf.at[kind, pl.ds(0, n2 - 1 + away)]
        remote(sent, sent, send1.at[kind * 2 + away], recv1.at[0], at(base + outer)).wait_send()

    others = [(1, i) for i in range(n2)] + [(0, i) for i in range(1, n2)]

    def select_own():
        everything = jnp.concatenate([dense[0, c] for c in range(chunks)], axis=1)
        found = jnp.dot(picks[0], everything, preferred_element_type=F32).astype(BF16)
        for c in range(chunks):
            buf[0, :, c] = found[:, c * LANES : (c + 1) * LANES].reshape(near, tall, LANES)
        for away, i in others:
            dispatch(0, away, i, None).start()
        recv[0, spot] = buf[0, mine]

    def select(kind, c):
        with jax.named_scope("densewait"):
            dense_copy(kind, c).wait_recv()
        with jax.named_scope("select"):
            found = jnp.dot(picks[kind], dense[kind, c], preferred_element_type=F32)
            buf[kind, :, c] = found.reshape(near, tall, LANES).astype(BF16)
            for away, i in others:
                dispatch(kind, away, i, c).start()
            recv[kind + 1, spot, c] = buf[kind, mine, c]

    def hop(group):
        return (plane, sibling, gate_plane, gate_plane)[group]

    def give_back(group, i, c):
        s = spots[i]
        kind = max(group - 1, 0)
        return remote(
            outb.at[group, s] if c is None else outb.at[group, s, c],
            ret.at[kind, mine] if c is None else ret.at[kind, mine, c],
            send2.at[group],
            recv2.at[kind * chunks + (c or 0)],
            at(hop(group) * n2 + s),
        )

    def given_back(group, count):
        sent = outb.at[group, pl.ds(0, count)]
        remote(sent, sent, send2.at[group], recv2.at[0], at(base + outer)).wait_send()

    def arrived(group, c, count):
        part = recv.at[group, pl.ds(0, count)]
        if c is not None:
            part = recv.at[group, pl.ds(0, count), c]
        remote(
            part, part, send1.at[0], recv1.at[group * chunks + (c or 0)], at(base + outer)
        ).wait_recv()

    def by_role(act):
        @pl.when(on_end)
        def _():
            act(n2)

        @pl.when(on_gate)
        def _():
            act(n2 - 1)

    piece = min(256, half)

    def feed(x):
        for part in range(2):
            for low in range(0, half, piece):
                gate_pre = jnp.dot(
                    x, wgs[part, :, low : low + piece], preferred_element_type=F32
                )
                up_pre = jnp.dot(x, wus[part, :, low : low + piece], preferred_element_type=F32)
                hid[part, :, low : low + piece] = clamped_unit(gate_pre, up_pre)

    def down(c):
        return jnp.dot(
            hid[0], wds[0, :, c * chunk : (c + 1) * chunk], preferred_element_type=F32
        ) + jnp.dot(
            hid[1], wds[1, :, c * chunk : (c + 1) * chunk], preferred_element_type=F32
        )

    def stack_tiles(total):
        return jnp.concatenate(
            [total[:, j * LANES : (j + 1) * LANES] for j in range(blocks)], axis=0
        )

    def run_near(group):
        with jax.named_scope("neararrive"):
            arrived(group, None, n2 - 1 + group)
        with jax.named_scope("near"):
            came = jnp.concatenate(
                [recv[group, :, c].reshape(packed_rows, LANES) for c in range(chunks)], axis=1
            )
            apart = jnp.dot(unpack_ref[...], came, preferred_element_type=F32).astype(BF16)
            for c in range(chunks):
                for j in range(blocks):
                    low = c * chunk + j * LANES
                    xs[:, low : low + LANES] = apart[
                        j * group_rows : (j + 1) * group_rows, c * LANES : (c + 1) * LANES
                    ]
            feed(xs[...])
            stacked = jnp.concatenate(
                [stack_tiles(down(c)) for c in range(chunks)], axis=1
            ).astype(BF16)
            joined = jnp.dot(pack_ref[...], stacked, preferred_element_type=F32).astype(BF16)
            for c in range(chunks):
                outb[group, :, c] = joined[:, c * LANES : (c + 1) * LANES].reshape(
                    n2, tall, LANES
                )
            if group == 0:
                ret[0, mine] = outb[0, spot]

    def send_near(group, low, high):
        for i in range(low, high):
            give_back(group, i, None).start()

    def run_far(group):
        for c in range(chunks):
            with jax.named_scope("arrive"):
                by_role(lambda count: arrived(group, c, count))
            came = recv[group, :, c].reshape(packed_rows, LANES)
            apart = jnp.dot(unpack_ref[...], came, preferred_element_type=F32).astype(BF16)
            for j in range(blocks):
                low = c * chunk + j * LANES
                xs[:, low : low + LANES] = apart[j * group_rows : (j + 1) * group_rows]
        with jax.named_scope("feed"):
            feed(xs[...])
        for c in range(chunks):
            stacked = stack_tiles(down(c)).astype(BF16)
            joined = jnp.dot(pack_ref[...], stacked, preferred_element_type=F32)
            outb[group, :, c] = joined.reshape(n2, tall, LANES).astype(BF16)

            @pl.when(on_end)
            def _():
                for i in range(1, n2):
                    pass_on(group, i, c).start()
                relay[group - 2, spot, c] = outb[group, spot, c]

            @pl.when(on_gate)
            def _():
                for i in range(1, n2):
                    give_back(group, i, c).start()
                ret[group - 1, mine, c] = outb[group, spot, c]

    def pass_on(group, i, c):
        s = spots[i]
        return remote(
            outb.at[group, s, c],
            relay.at[group - 2, spot, c],
            send2.at[group],
            relay_recv.at[(group - 2) * chunks + c],
            at(plane * n2 + s),
        )

    def forward(group, c):
        return remote(
            relay.at[group - 2, :, c],
            ret.at[group - 1, pl.ds(inner, n2), c],
            relay_send.at[group - 2],
            recv2.at[(group - 1) * chunks + c],
            at(sibling * n2 + spot),
        )

    def run_relay(group):
        with jax.named_scope("relay"):
            for c in range(chunks):
                part = relay.at[group - 2, pl.ds(0, n2 - 1), c]
                remote(
                    part,
                    part,
                    relay_send.at[0],
                    relay_recv.at[(group - 2) * chunks + c],
                    at(base + outer),
                ).wait_recv()
                forward(group, c).start()

    def returned(kind, c):
        part = ret.at[kind, pl.ds(0, near - 1)]
        if c is not None:
            part = ret.at[kind, pl.ds(0, near - 1), c]
        remote(
            part, part, send2.at[0], recv2.at[kind * chunks + (c or 0)], at(base + outer)
        ).wait_recv()

    def weigh(kind, picked):
        totals = []
        for j in range(blocks):
            total = jnp.zeros((rows, picked.shape[1]), F32)
            for k in range(2):
                top = (k * blocks + j) * rows
                total = total + picked[top : top + rows] * columns[kind, :, 2 + k : 3 + k]
            totals.append(total)
        return totals

    def fin_copy(kind, c):
        where = far_end if kind == 2 else far_gate
        return remote(
            pout.at[kind - 1, c],
            fin.at[c],
            fin_send.at[kind - 1],
            fin_recv.at[c],
            at(where * n2 + spot),
        )

    def combine(kind, c):
        with jax.named_scope("gatherwait"):
            returned(kind, c)
        with jax.named_scope("combine"):
            back = ret[kind, :, c].reshape(near * tall, LANES)
            picked = jnp.dot(wanted[kind], back, preferred_element_type=F32)
            total = jnp.concatenate(weigh(kind, picked), axis=1)
            pout[kind - 1, c] = total.astype(BF16)
            fin_copy(kind, c).start()

    def dense_branch():
        depth = din_ref.shape[1]
        x = jnp.concatenate(
            [
                dense[0, c, j * rows : (j + 1) * rows, :]
                for c in range(chunks)
                for j in range(blocks)
            ],
            axis=1,
        )
        pre = jnp.dot(x, dn[0].reshape(width, depth), preferred_element_type=F32)
        dense_hidden = jax.nn.silu(pre).astype(BF16)
        step = width // n1
        for z in range(n1):
            branch = lax.dot_general(
                dense_hidden,
                dn[1, z].reshape(step, depth),
                (((1,), (1,)), ((), ())),
                preferred_element_type=F32,
            )
            accs[:, z * step : (z + 1) * step] = (
                jax.nn.sigmoid(dgate_ref[:, z * step : (z + 1) * step]) * branch
            )

    def own():
        with jax.named_scope("ownwait"):
            returned(0, None)
        back = jnp.concatenate(
            [ret[0, :, c].reshape(near * tall, LANES) for c in range(chunks)], axis=1
        )
        picked = jnp.dot(wanted[0], back, preferred_element_type=F32)
        totals = weigh(0, picked)
        for c in range(chunks):
            for j in range(blocks):
                low = c * chunk + j * LANES
                accs[:, low : low + LANES] = (
                    accs[:, low : low + LANES] + totals[j][:, c * LANES : (c + 1) * LANES]
                )

    with jax.named_scope("barrier"):
        pl.semaphore_wait(barrier, near + 1 + is_gate)
    for copy in meta_copies():
        copy.start()

    @pl.when(on_gate)
    def _():
        dn_cross(plane).start()

    dense_start()
    dn_near(plane).start()

    @pl.when(on_end)
    def _():
        dn_far(plane).start()

    for i in range(3):
        weight_copy(i).start()
    with jax.named_scope("selectown"):
        select_own()

    def weights_wait():
        with jax.named_scope("weightwait"):
            for i, (src, dst) in enumerate(weight_pairs):
                pltpu.make_async_copy(src, dst.at[0], w_local.at[i]).wait()
            for i in range(3):
                weight_copy(i).wait()

    def prepare_for(kind):
        with jax.named_scope("prepare"):
            meta_wait(kind)
            prepare(kind)

    part = chunks // 2

    def step_wait():
        with jax.named_scope("stepwait"):
            dn_bytes(0).wait_recv()

    @pl.when(on_gate)
    def _():
        prepare_for(2)
        for c in range(part):
            select(2, c)
        weights_wait()
        run_near(0)
        for c in range(part, chunks):
            select(2, c)
        prepare_for(1)
        select(1, 0)
        with jax.named_scope("upwait"):
            dn_cross(far_gate).wait_recv()
        dn_down(0).start()
        select(1, 1)
        with jax.named_scope("upwait"):
            dn_far(far_end).wait_recv()
            dn_near(sibling).wait_recv()
        dn_down(1).start()
        dn_start(0)

    @pl.when(on_end)
    def _():
        weights_wait()
        run_near(0)
        send_near(0, 1, n2)
        run_near(1)

    with jax.named_scope("farC"):
        run_far(3)

    @pl.when(on_end)
    def _():
        run_relay(3)
        send_near(1, 0, part)
        with jax.named_scope("upwait"):
            dn_near(sibling).wait_recv()
            for order in range(2):
                dn_down(order).wait_recv()
        dn_start(0)

    @pl.when(on_gate)
    def _():
        for c in range(part, chunks):
            select(1, c)
        step_wait()
        dn_start(1)
        run_near(1)
        with jax.named_scope("sentwait"):
            dispatched(1, 1)
            pl.semaphore_signal(
                clear, inc=1, device_id=at(far_gate * n2 + spot), device_id_type=MESH
            )
            pl.semaphore_wait(clear, 1)
        for c in range(chunks):
            combine(2, c)

    with jax.named_scope("farB"):
        run_far(2)

    @pl.when(on_gate)
    def _():
        send_near(0, 1, n2)
        send_near(1, 0, n2)
        for c in range(chunks):
            combine(1, c)

    @pl.when(on_end)
    def _():
        run_relay(2)
        send_near(1, part, n2)
        step_wait()
        dn_start(1)

    with jax.named_scope("dnwait"):
        dn_bytes(1).wait_recv()
        dn_swap(core).start()
        dn_swap(peer).wait_recv()
    with jax.named_scope("densebranch"):
        dense_branch()
    with jax.named_scope("own"):
        own()

    with jax.named_scope("drain"):
        for away in range(2):
            dispatched(0, away)
        for copy in meta_copies():
            copy.wait_send()
        remote(
            dense.at[0], dense.at[0], dense_send, dense_recv.at[0, 0], at(base + outer)
        ).wait_send()
        for group in range(2):
            given_back(group, n2 - 1 + group)
        for group in range(2, n1):
            given_back(group, n2 - 1)
        dn_near(plane).wait_send()
        for step in range(2):
            dn_bytes(step).wait_send()
        dn_swap(core).wait_send()

        @pl.when(on_end)
        def _():
            dn_far(plane).wait_send()
            for group in (0, 1):
                remote(
                    relay.at[group],
                    relay.at[group],
                    relay_send.at[group],
                    relay_recv.at[0],
                    at(base + outer),
                ).wait_send()

        @pl.when(on_gate)
        def _():
            for away in range(2):
                dispatched(2, away)
            dispatched(1, 0)
            dn_cross(plane).wait_send()
            for order in range(2):
                dn_down(order).wait_send()

    with jax.named_scope("finish"):
        for c in range(chunks):
            with jax.named_scope("finwait"):
                fin_copy(1, c).wait_recv()
            span = slice(c * chunk, (c + 1) * chunk)
            out_ref[:, span] = (accs[:, span] + fin[c].astype(F32)).astype(BF16)

    @pl.when(on_gate)
    def _():
        for kind in (1, 2):
            sent = pout.at[kind - 1]
            remote(
                sent, sent, fin_send.at[kind - 1], fin_recv.at[0], at(base + outer)
            ).wait_send()


def gateway_call(sizes, operands):
    n, n1, n2, cap, blocks = sizes
    tokens, dense_in, w_gate = operands[2], operands[5], operands[7]
    rows, width = tokens.shape
    half, depth = w_gate.shape[1], dense_in.shape[1]
    tall, near = blocks * cap, n // 2
    chunk = blocks * LANES
    chunks = width // chunk
    packed = n2 * tall
    vmem = pl.BlockSpec(memory_space=pltpu.VMEM)
    anywhere = pl.BlockSpec(memory_space=pl.ANY)
    dma = pltpu.SemaphoreType.DMA
    return pl.pallas_call(
        functools.partial(gateway_kernel, sizes),
        out_shape=jax.ShapeDtypeStruct((rows, width), BF16),
        in_specs=[vmem] * 7 + [anywhere] * 3,
        out_specs=vmem,
        scratch_shapes=[
            pltpu.VMEM((3, 2, rows), jnp.int32),
            pltpu.VMEM((3, 2, rows), F32),
            pltpu.VMEM((3, chunks, blocks * rows, LANES), BF16),
            pltpu.VMEM((3, near * tall, blocks * rows), BF16),
            pltpu.VMEM((3, 2 * blocks * rows, near * tall), BF16),
            pltpu.VMEM((3, rows, 8), F32),
            pltpu.VMEM((3, near, chunks, tall, LANES), BF16),
            pltpu.VMEM((n1, n2, chunks, tall, LANES), BF16),
            pltpu.VMEM((n2 * cap, width), BF16),
            pltpu.VMEM((2, n2 * cap, half), BF16),
            pltpu.VMEM((packed, packed), BF16),
            pltpu.VMEM((packed, packed), BF16),
            pltpu.VMEM((n1, n2, chunks, tall, LANES), BF16),
            pltpu.VMEM((3, near, chunks, tall, LANES), BF16),
            pltpu.VMEM((2, n2, chunks, tall, LANES), BF16),
            pltpu.VMEM((rows, width), F32),
            pltpu.VMEM((2, chunks, rows, chunk), BF16),
            pltpu.VMEM((chunks, rows, chunk), BF16),
            pltpu.VMEM((2, width, half), BF16),
            pltpu.VMEM((2, width, half), BF16),
            pltpu.VMEM((2, half, width), BF16),
            pltpu.VMEM((2, n1, n2, width // n, depth), BF16),
            dma((3,)),
            dma((3,)),
            dma((3,)),
            dma((2,)),
            dma((2, 2)),
            dma,
            dma((2, chunks)),
            dma((6,)),
            dma((n1 * chunks,)),
            dma((n1,)),
            dma((3 * chunks,)),
            dma((2,)),
            dma((chunks,)),
            dma((8,)),
            dma((8,)),
            dma((2,)),
            dma((2 * chunks,)),
            pltpu.SemaphoreType.REGULAR,
        ],
        compiler_params=pltpu.CompilerParams(
            collective_id=0, has_side_effects=True, vmem_limit_bytes=60 * 1024 * 1024
        ),
    )(*operands)


def shards(
    tokens, norm_gain, routes, route_weights, w_gate, w_up, w_down, dense_in, dense_out, dense_gate
):
    rows, width = tokens.shape
    top_count = routes.shape[1]
    n = lax.axis_size("ep")
    capacity = (4 * rows * top_count + 3 * n - 1) // (3 * n)
    cap = capacity
    blocks = 8 // math.gcd(cap, 8)
    tall, tile = blocks * cap, width // blocks
    n2 = 1
    while n2 * n2 < n:
        n2 *= 2
    n1 = n // n2
    half = w_gate.shape[2]
    depth = dense_in.shape[1]
    if n1 == 4 and n2 == 4 and width % (2 * blocks * LANES) == 0 and width % n == 0:
        return gateway_call(
            (n, n1, n2, cap, blocks),
            (
                routes.T,
                route_weights.T,
                tokens,
                norm_gain.reshape(1, width),
                dense_gate.reshape(1, width),
                dense_in,
                dense_out,
                w_gate[0],
                w_up[0],
                w_down[0],
            ),
        )
    vmem = pl.BlockSpec(memory_space=pltpu.VMEM)
    anywhere = pl.BlockSpec(memory_space=pl.ANY)
    dma = pltpu.SemaphoreType.DMA
    slab = pltpu.VMEM((n, tall, tile), BF16)
    return pl.pallas_call(
        functools.partial(layer_kernel, (n, n1, n2, cap, blocks)),
        out_shape=jax.ShapeDtypeStruct((rows, width), BF16),
        in_specs=[vmem] * 8 + [anywhere] * 3,
        out_specs=vmem,
        scratch_shapes=[
            pltpu.VMEM((rows, width), BF16),
            pltpu.VMEM((n1, n2, blocks * rows), jnp.int32),
            pltpu.VMEM((blocks * rows, tile), BF16),
            pltpu.VMEM((rows, 2), jnp.int32),
            pltpu.VMEM((n2 * cap, width), BF16),
            pltpu.VMEM((n2 * tall, tile), F32),
            pltpu.VMEM((n2 * tall, n2 * tall), BF16),
            pltpu.VMEM((n2 * tall, n2 * tall), BF16),
            slab,
            slab,
            slab,
            slab,
            pltpu.VMEM((2, width, half), BF16),
            pltpu.VMEM((2, width, half), BF16),
            pltpu.VMEM((2, half, width), BF16),
            pltpu.VMEM((2, n2 * cap, half), BF16),
            pltpu.VMEM((2, n1, n2, width // n, depth), BF16),
            pltpu.VMEM((rows, width), F32),
            dma((n,)),
            dma((n,)),
            dma((n,)),
            dma((n,)),
            dma((3,)),
            dma((3,)),
            dma((3,)),
            dma((n1,)),
            dma((n1,)),
            dma((n2,)),
            dma((n2,)),
            dma,
            dma,
        ],
        compiler_params=pltpu.CompilerParams(
            collective_id=0, has_side_effects=True, vmem_limit_bytes=60 * 1024 * 1024
        ),
    )(
        routes.T,
        routes,
        route_weights,
        tokens,
        norm_gain.reshape(1, width),
        dense_gate.reshape(1, width),
        dense_in,
        dense_out,
        w_gate[0],
        w_up[0],
        w_down[0],
    )


def solution(mesh):
    placed = (
        P(("ep", "tp"), None),
        P(),
        P(("ep", "tp"), None),
        P(("ep", "tp"), None),
        P("ep", None, "tp"),
        P("ep", None, "tp"),
        P("ep", "tp", None),
        P("ep", None),
        P("ep", None),
        P(),
    )
    return jax.shard_map(
        shards, mesh=mesh, in_specs=placed, out_specs=P(("ep", "tp"), None), check_vma=False
    )
```

```python
import functools
import math

import jax
import jax.numpy as jnp
from jax import lax
from jax.experimental import pallas as pl
from jax.experimental.pallas import tpu as pltpu
from jax.sharding import PartitionSpec as P

CLAMP_LIMIT = 7.0
SLOPE_ALPHA = 1.702
NORM_EPS = 1e-06
MESH = pl.DeviceIdType.MESH
F32 = jnp.float32
BF16 = jnp.bfloat16


def clamped_unit(gate_pre, up_pre):
    gate_clip = jnp.minimum(gate_pre, CLAMP_LIMIT)
    up_clip = jnp.clip(up_pre, -CLAMP_LIMIT, CLAMP_LIMIT)
    return ((up_clip + 1.0) * gate_clip * jax.nn.sigmoid(SLOPE_ALPHA * gate_clip)).astype(BF16)


def layer_kernel(
    sizes,
    routes_t_ref,
    routes_ref,
    weights_ref,
    tokens_ref,
    gain_ref,
    dgate_ref,
    din_ref,
    dout_ref,
    wg_ref,
    wu_ref,
    wd_ref,
    out_ref,
    normed,
    keys,
    stacked,
    places,
    xs,
    totals,
    unpack_ref,
    pack_ref,
    buf,
    recv,
    outb,
    ret,
    wgs,
    wus,
    wds,
    hid,
    dn,
    acc,
    send1,
    recv1,
    send2,
    recv2,
    w_local,
    w_send,
    w_recv,
    ds1,
    dr1,
    ds2,
    dr2,
    ds3,
    dr3,
):
    n, n1, n2, cap, blocks = sizes
    rows, width = tokens_ref.shape
    half = wg_ref.shape[1]
    tall, tile = blocks * cap, width // blocks
    group_rows, packed_rows = n2 * cap, n2 * blocks * cap
    me = lax.axis_index("ep")
    core = lax.axis_index("tp")
    plane, spot = me // n2, me % n2
    peer = 1 - core

    barrier = pltpu.get_barrier_semaphore()

    def greet(i, carry):
        pl.semaphore_signal(
            barrier, inc=1, device_id={"ep": (me + i) % n}, device_id_type=MESH
        )
        return carry

    lax.fori_loop(1, n, greet, 0)
    pl.semaphore_signal(barrier, inc=1, device_id={"tp": peer}, device_id_type=MESH)

    weight_pairs = ((wg_ref, wgs), (wu_ref, wus), (wd_ref, wds))
    for i, (src, dst) in enumerate(weight_pairs):
        pltpu.make_async_copy(src, dst.at[0], w_local.at[i]).start()

    @pl.when(core == 0)
    def _():
        dn[0, plane, spot] = din_ref[...]

    @pl.when(core == 1)
    def _():
        dn[1, plane, spot] = dout_ref[...]

    widened = tokens_ref[...].astype(F32)
    inv_scale = lax.rsqrt(jnp.mean(widened * widened, axis=1, keepdims=True) + NORM_EPS)
    normed[...] = (widened * inv_scale * gain_ref[...]).astype(BF16)
    for j in range(blocks):
        stacked[j * rows : (j + 1) * rows, :] = normed[:, j * tile : (j + 1) * tile]

    expert_ids = lax.broadcasted_iota(jnp.int32, (n, rows), 0)
    chosen = (routes_t_ref[0:1, :] == expert_ids) | (routes_t_ref[1:2, :] == expert_ids)
    earlier = (
        lax.broadcasted_iota(jnp.int32, (rows, rows), 0)
        < lax.broadcasted_iota(jnp.int32, (rows, rows), 1)
    )
    counted = jnp.dot(
        jnp.where(chosen, 1.0, 0.0).astype(BF16),
        jnp.where(earlier, 1.0, 0.0).astype(BF16),
        preferred_element_type=F32,
    )
    for j in range(blocks):
        found = jnp.where(chosen, counted.astype(jnp.int32) + j * cap, -1)
        for z in range(n1):
            keys[z, :, j * rows : (j + 1) * rows] = found[z * n2 : (z + 1) * n2]
    experts_across = lax.broadcasted_iota(jnp.int32, (rows, n), 1)
    takes = [routes_ref[:, k : k + 1] == experts_across for k in range(2)]
    before = (
        lax.broadcasted_iota(jnp.int32, (rows, rows), 0)
        > lax.broadcasted_iota(jnp.int32, (rows, rows), 1)
    )
    counts = jnp.dot(
        jnp.where(before, 1.0, 0.0).astype(BF16),
        jnp.where(takes[0] | takes[1], 1.0, 0.0).astype(BF16),
        preferred_element_type=F32,
    )
    for k in range(2):
        slot = jnp.sum(jnp.where(takes[k], counts, 0.0), axis=1, keepdims=True)
        places[:, k : k + 1] = routes_ref[:, k : k + 1] * tall + slot.astype(jnp.int32)

    pl.semaphore_wait(barrier, n)

    def weight_copy(i):
        src, dst = weight_pairs[i]
        return pltpu.make_async_remote_copy(
            src_ref=src,
            dst_ref=dst.at[1],
            send_sem=w_send.at[i],
            recv_sem=w_recv.at[i],
            device_id={"tp": peer},
            device_id_type=MESH,
        )

    def dense_copy1(bit, block):
        other = plane + bit - 2 * bit * ((plane // bit) % 2)
        return pltpu.make_async_remote_copy(
            src_ref=dn.at[core, block, spot],
            dst_ref=dn.at[core, block, spot],
            send_sem=ds1.at[block],
            recv_sem=dr1.at[block],
            device_id={"ep": other * n2 + spot},
            device_id_type=MESH,
        )

    bits = [1 << b for b in reversed(range(n1.bit_length() - 1))]

    def dense_held(bit, where):
        return [where % (2 * bit) + m * 2 * bit for m in range(n1 // (2 * bit))]

    def dense_start(bit):
        for block in dense_held(bit, plane):
            dense_copy1(bit, block).start()

    def dense_finish(bit):
        for block in dense_held(bit, plane + bit - 2 * bit * ((plane // bit) % 2)):
            dense_copy1(bit, block).wait_recv()
        for block in dense_held(bit, plane):
            dense_copy1(bit, block).wait_send()

    def dense_copy2(other, slot):
        return pltpu.make_async_remote_copy(
            src_ref=dn.at[core, :, slot],
            dst_ref=dn.at[core, :, slot],
            send_sem=ds2.at[other],
            recv_sem=dr2.at[slot],
            device_id={"ep": plane * n2 + other},
            device_id_type=MESH,
        )

    def dense_copy3(which):
        return pltpu.make_async_remote_copy(
            src_ref=dn.at[which],
            dst_ref=dn.at[which],
            send_sem=ds3,
            recv_sem=dr3,
            device_id={"tp": peer},
            device_id_type=MESH,
        )

    def each(count, act):
        def step(i, carry):
            act(i)
            return carry

        lax.fori_loop(0, count, step, 0)

    dense_start(bits[0])
    for i in range(3):
        weight_copy(i).start()

    def dispatch(dst, slot):
        return pltpu.make_async_remote_copy(
            src_ref=buf.at[dst],
            dst_ref=recv.at[slot],
            send_sem=send1.at[dst],
            recv_sem=recv1.at[slot],
            device_id={"ep": dst},
            device_id_type=MESH,
        )

    def give_back(dst, slot):
        return pltpu.make_async_remote_copy(
            src_ref=outb.at[dst],
            dst_ref=ret.at[slot],
            send_sem=send2.at[dst],
            recv_sem=recv2.at[slot],
            device_id={"ep": dst},
            device_id_type=MESH,
        )

    def partner_plane(x):
        return sum(((plane // b) % 2 + (x // b) % 2) % 2 * b for b in bits)

    def turn(i):
        return partner_plane(i % 2 * (n1 // 2) + i // 2)

    def send_group(i):
        group = partner_plane((i + n1 // 2) % n1)
        first = group * n2
        wanted = keys[group]
        picks = wanted[:, None, :] == lax.broadcasted_iota(
            jnp.int32, (n2, tall, blocks * rows), 1
        )
        picks = jnp.where(picks, 1.0, 0.0).reshape(packed_rows, blocks * rows).astype(BF16)
        found = jnp.dot(picks, stacked[...], preferred_element_type=F32)
        buf[pl.ds(first, n2)] = found.reshape(n2, tall, tile).astype(BF16)

        def start(j):
            dst = first + (spot + 1 + j) % n2

            @pl.when(dst != me)
            def _():
                dispatch(dst, me).start()

            @pl.when(dst == me)
            def _():
                recv[me] = buf[me]

        each(n2, start)

    each(n1, send_group)


    for i, (src, dst) in enumerate(weight_pairs):
        pltpu.make_async_copy(src, dst.at[0], w_local.at[i]).wait()
    for i in range(3):
        weight_copy(i).wait()

    piece = min(256, half)
    upright = lax.broadcasted_iota(jnp.int32, (packed_rows, packed_rows), 0)
    across = lax.broadcasted_iota(jnp.int32, (packed_rows, packed_rows), 1)

    def packed_place(r):
        return (r // cap) % n2 * tall + r // group_rows * cap + r % cap

    unpack = jnp.where(packed_place(upright) == across, 1.0, 0.0).astype(BF16)
    pack = jnp.where(packed_place(across) == upright, 1.0, 0.0).astype(BF16)
    unpack_ref[...] = unpack
    pack_ref[...] = pack

    def run_group(i):
        group = turn(i)
        first = group * n2

        def arrive(j):
            src = first + j

            @pl.when(src != me)
            def _():
                dispatch(src, src).wait_recv()

        each(n2, arrive)
        came = recv[pl.ds(first, n2)].astype(F32).reshape(packed_rows, tile).astype(BF16)
        apart = jnp.dot(unpack_ref[...], came, preferred_element_type=F32)
        for j in range(blocks):
            xs[:, j * tile : (j + 1) * tile] = apart[
                j * group_rows : (j + 1) * group_rows
            ].astype(BF16)
        x = xs[...]
        for part in range(2):
            for low in range(0, half, piece):
                gate_pre = jnp.dot(
                    x, wgs[part, :, low : low + piece], preferred_element_type=F32
                )
                up_pre = jnp.dot(x, wus[part, :, low : low + piece], preferred_element_type=F32)
                hid[part, :, low : low + piece] = clamped_unit(gate_pre, up_pre)
        for j in range(blocks):
            total = jnp.zeros((group_rows, tile), F32)
            for part in range(2):
                partial = jnp.dot(
                    hid[part],
                    wds[part, :, j * tile : (j + 1) * tile],
                    preferred_element_type=F32,
                )
                total = total + partial.astype(BF16).astype(F32)
            totals[j * group_rows : (j + 1) * group_rows, :] = total
        joined = jnp.dot(pack_ref[...], totals[...].astype(BF16), preferred_element_type=F32)
        outb[pl.ds(first, n2)] = joined.reshape(n2, tall, tile).astype(BF16)

        def start(j):
            dst = first + (spot + 1 + j) % n2

            @pl.when(dst != me)
            def _():
                give_back(dst, me).start()

            @pl.when(dst == me)
            def _():
                ret[me] = outb[me]

        each(n2, start)

    def run_turn(i):
        run_group(i)
        for b, bit in enumerate(bits):

            @pl.when(i == b)
            def _():
                dense_finish(bit)
                if b + 1 < len(bits):
                    dense_start(bits[b + 1])
                else:
                    each(n2 - 1, lambda j: dense_copy2((spot + 1 + j) % n2, spot).start())

    each(n1, run_turn)
    each(n2 - 1, lambda i: dense_copy2((spot + 1 + i) % n2, (spot + 1 + i) % n2).wait_recv())
    dense_copy3(core).start()
    dense_copy3(core).wait_send()
    dense_copy3(peer).wait_recv()
    depth = din_ref.shape[1]
    dense_pre = jnp.dot(
        normed[...], dn[0].reshape(width, depth), preferred_element_type=F32
    )
    dense_hidden = jax.nn.silu(dense_pre).astype(BF16)
    step = width // n1
    for z in range(n1):
        branch = lax.dot_general(
            dense_hidden,
            dn[1, z].reshape(step, depth),
            (((1,), (1,)), ((), ())),
            preferred_element_type=F32,
        )
        acc[:, z * step : (z + 1) * step] = (
            jax.nn.sigmoid(dgate_ref[:, z * step : (z + 1) * step]) * branch
        )

    def combine_group(i):
        group = turn(i)
        first = group * n2

        def arrive(j):
            src = first + j

            @pl.when(src != me)
            def _():
                give_back(src, src).wait_recv()

        each(n2, arrive)
        back = ret[pl.ds(first, n2)].astype(F32).reshape(packed_rows, tile).astype(BF16)
        lanes = lax.broadcasted_iota(jnp.int32, (rows, packed_rows), 1) + first * tall
        wanted = jnp.concatenate(
            [
                jnp.where(places[:, k : k + 1] + j * cap == lanes, 1.0, 0.0).astype(BF16)
                for k in range(2)
                for j in range(blocks)
            ],
            axis=0,
        )
        picked = jnp.dot(wanted, back, preferred_element_type=F32)
        for j in range(blocks):
            total = acc[:, j * tile : (j + 1) * tile]
            for k in range(2):
                at = (k * blocks + j) * rows
                total = total + picked[at : at + rows] * weights_ref[:, k : k + 1]
            acc[:, j * tile : (j + 1) * tile] = total

    each(n1, combine_group)
    out_ref[...] = acc[...].astype(BF16)

    def drain(i):
        other = (me + 1 + i) % n
        dispatch(other, me).wait_send()
        give_back(other, me).wait_send()

    each(n - 1, drain)
    each(n2 - 1, lambda i: dense_copy2((spot + 1 + i) % n2, spot).wait_send())


LANES = 128
CHUNKS = 4


def gateway_kernel(
    sizes,
    routes_ref,
    weights_ref,
    tokens_ref,
    gain_ref,
    dgate_ref,
    din_ref,
    dout_ref,
    wg_ref,
    wu_ref,
    wd_ref,
    out_ref,
    tokens_in,
    gain_in,
    dgate_in,
    routes_of,
    weights_of,
    dense,
    picks,
    wanted,
    columns,
    buf,
    recv,
    xs,
    hid,
    outb,
    ret,
    relay,
    accs,
    pout,
    fin,
    through,
    wgs,
    wus,
    wds,
    dn,
    w_local,
    w_send,
    w_recv,
    meta_send,
    meta_recv,
    dense_send,
    dense_recv,
    send1,
    recv1,
    send2,
    recv2,
    fin_send,
    fin_recv,
    dn_send,
    dn_recv,
    relay_send,
    relay_recv,
    through_send,
    through_recv,
    inputs,
):
    n, n1, n2, tall = sizes
    rows, width = tokens_ref.shape
    half = wg_ref.shape[1]
    chunks = CHUNKS
    chunk = width // chunks
    near = n // 2
    group_rows = n2 * tall
    me = lax.axis_index("ep")
    core = lax.axis_index("tp")
    peer = 1 - core
    plane, spot = me // n2, me % n2
    side = plane // 2
    mine = me % near
    base = side * near
    is_gate = (plane + 1) // 2 % 2
    sibling = plane + 1 - 2 * (plane % 2)
    gate_plane = 1 + side
    far_gate = 2 - side
    far_end = 3 - 3 * side
    on_gate = is_gate == 1
    on_end = is_gate == 0

    def at(where):
        return {"ep": where}

    def each(count, act):
        def step(i, carry):
            act(i)
            return carry

        lax.fori_loop(0, count, step, 0)

    def remote(src, dst, send_sem, recv_sem, device):
        return pltpu.make_async_remote_copy(
            src_ref=src,
            dst_ref=dst,
            send_sem=send_sem,
            recv_sem=recv_sem,
            device_id=device,
            device_id_type=MESH,
        )

    barrier = pltpu.get_barrier_semaphore()
    small_pairs = (
        (tokens_ref, tokens_in),
        (gain_ref, gain_in),
        (routes_ref, routes_of.at[0]),
        (weights_ref, weights_of.at[0]),
        (dgate_ref, dgate_in),
    )
    small_copies = [
        pltpu.make_async_copy(src, dst, inputs.at[i])
        for i, (src, dst) in enumerate(small_pairs)
    ]
    for copy in small_copies:
        copy.start()

    def greet(device):
        pl.semaphore_signal(barrier, inc=1, device_id=device, device_id_type=MESH)

    each(near - 1, lambda i: greet(at(base + (mine + 1 + i) % near)))
    greet({"tp": peer})
    greet(at(far_gate * n2 + spot))

    @pl.when(on_gate)
    def _():
        greet(at(far_end * n2 + spot))

    def block_copy(which):
        return pltpu.make_async_copy(
            (din_ref, dout_ref)[which], dn.at[which, plane, spot], inputs.at[5]
        )

    for which in range(2):

        @pl.when(core == which)
        def _():
            block_copy(which).start()

    block_copy(0).wait()
    for copy in small_copies:
        copy.wait()
    weight_pairs = ((wg_ref, wgs), (wu_ref, wus), (wd_ref, wds))
    for i, (src, dst) in enumerate(weight_pairs):
        pltpu.make_async_copy(src, dst.at[0], w_local.at[i]).start()

    with jax.named_scope("norm"):
        widened = tokens_in[...].astype(F32)
        inv_scale = lax.rsqrt(jnp.mean(widened * widened, axis=1, keepdims=True) + NORM_EPS)
        normed = (widened * inv_scale * gain_in[...]).astype(BF16)
        for c in range(chunks):
            dense[0, c] = normed[:, c * chunk : (c + 1) * chunk]

    def prepare(kind):
        experts = lax.broadcasted_iota(jnp.int32, (near, rows), 0) + base
        first, second = routes_of[kind, 0:1, :], routes_of[kind, 1:2, :]
        takes = (first == experts, second == experts)
        chosen = takes[0] | takes[1]
        earlier = (
            lax.broadcasted_iota(jnp.int32, (rows, rows), 0)
            < lax.broadcasted_iota(jnp.int32, (rows, rows), 1)
        )
        counted = jnp.dot(
            jnp.where(chosen, 1.0, 0.0).astype(BF16),
            jnp.where(earlier, 1.0, 0.0).astype(BF16),
            preferred_element_type=F32,
        )
        keys = jnp.where(chosen, counted.astype(jnp.int32), -1)
        hits = keys[:, None, :] == lax.broadcasted_iota(jnp.int32, (near, tall, rows), 1)
        picks[kind] = jnp.where(hits, 1.0, 0.0).reshape(near * tall, rows).astype(BF16)
        local = lax.broadcasted_iota(jnp.int32, (near, rows), 0) * tall
        places = [
            jnp.sum(
                jnp.where(take, counted + local.astype(F32) + n * tall, 0.0),
                axis=0,
                keepdims=True,
            )
            - n * tall
            for take in takes
        ]
        stack = jnp.concatenate(
            places + [weights_of[kind], jnp.zeros((4, rows), F32)], axis=0
        )
        turned = jnp.transpose(stack)
        columns[kind] = turned
        lanes = lax.broadcasted_iota(jnp.int32, (rows, near * tall), 1)
        for k in range(2):
            place = turned[:, k : k + 1].astype(jnp.int32)
            wanted[kind, k * rows : (k + 1) * rows, :] = jnp.where(
                place == lanes, 1.0, 0.0
            ).astype(BF16)

    with jax.named_scope("prepare0"):
        prepare(0)

    def meta_copies():
        slot = 2 - is_gate
        device = at(far_gate * n2 + spot)
        return (
            remote(routes_of.at[0], routes_of.at[slot], meta_send.at[0], meta_recv.at[0, slot - 1], device),
            remote(weights_of.at[0], weights_of.at[slot], meta_send.at[1], meta_recv.at[1, slot - 1], device),
        )

    def meta_wait(slot):
        device = at(far_gate * n2 + spot)
        remote(
            routes_of.at[0], routes_of.at[slot], meta_send.at[0], meta_recv.at[0, slot - 1], device
        ).wait_recv()
        remote(
            weights_of.at[0], weights_of.at[slot], meta_send.at[1], meta_recv.at[1, slot - 1], device
        ).wait_recv()

    def dense_copy(slot, c):
        return remote(
            dense.at[0, c],
            dense.at[slot, c],
            dense_send,
            dense_recv.at[slot - 1, c],
            at(far_gate * n2 + spot),
        )

    def dense_start():
        for c in range(chunks):
            dense_copy(2 - is_gate, c).start()

    def dn_block(which, index, target):
        block = dn.at[core, which, spot]
        return remote(
            block, block, dn_send.at[index], dn_recv.at[index], at(target * n2 + spot)
        )

    def dn_near(which):
        return dn_block(which, 0, sibling)

    def dn_cross(which):
        return dn_block(which, 1, far_gate)

    def dn_far(which):
        return dn_block(which, 2, far_gate)

    def dn_down(order):
        return dn_block(far_end if order else far_gate, 3 + order, sibling)

    first_bit, second_bit = 1 + core, 2 - core
    first_spot = spot + first_bit - 2 * first_bit * (spot // first_bit % 2)
    second_spot = spot + second_bit - 2 * second_bit * (spot // second_bit % 2)

    def dn_step(part, step, block):
        index = 5 + 2 * part + step
        return remote(
            block,
            block,
            dn_send.at[index],
            dn_recv.at[index],
            at(plane * n2 + (second_spot if step else first_spot)),
        )

    def dn_start(part, step):
        for slot in (spot, first_spot)[: 1 + step]:
            if part == 0:
                dn_step(part, step, dn.at[core, plane, slot]).start()
            else:
                dn_step(part, step, dn.at[core, sibling, slot]).start()
                dn_step(part, step, dn.at[core, pl.ds((1 - side) * 2, 2), slot]).start()

    def dn_bytes(part, step):
        slots = pl.ds(0, 2) if step else 0
        return dn_step(part, step, dn.at[core, pl.ds(0, n1 - 1) if part else 0, slots])

    def dn_swap(which):
        last = 9
        return remote(
            dn.at[which], dn.at[which], dn_send.at[last], dn_recv.at[last], {"tp": peer}
        )

    def weight_copy(i):
        src, dst = weight_pairs[i]
        return remote(src, dst.at[1], w_send.at[i], w_recv.at[i], {"tp": peer})

    spots = [(spot + i) % n2 for i in range(n2)]
    inner = plane % 2 * n2
    outer = n2 - inner

    def dispatch(kind, away, i, c):
        expert = (outer if away else inner) + spots[i]
        group = kind + 1 if kind else away
        return remote(
            buf.at[kind, expert] if c is None else buf.at[kind, expert, c],
            recv.at[group, spot] if c is None else recv.at[group, spot, c],
            send1.at[kind * 2 + away],
            recv1.at[group * chunks + (c or 0)],
            at(base + expert),
        )

    def dispatched(kind, away):
        sent = buf.at[kind, pl.ds(0, n2 - 1 + away)]
        remote(sent, sent, send1.at[kind * 2 + away], recv1.at[0], at(base + outer)).wait_send()

    others = [(1, i) for i in range(n2)] + [(0, i) for i in range(1, n2)]

    def select_own():
        everything = jnp.concatenate([dense[0, c] for c in range(chunks)], axis=1)
        found = jnp.dot(picks[0], everything, preferred_element_type=F32).astype(BF16)
        for c in range(chunks):
            buf[0, :, c] = found[:, c * chunk : (c + 1) * chunk].reshape(near, tall, chunk)
        for away, i in others:
            dispatch(0, away, i, None).start()
        recv[0, spot] = buf[0, mine]

    def select(kind, c):
        with jax.named_scope("densewait"):
            dense_copy(kind, c).wait_recv()
        with jax.named_scope("select"):
            found = jnp.dot(picks[kind], dense[kind, c], preferred_element_type=F32)
            buf[kind, :, c] = found.astype(BF16).reshape(near, tall, chunk)
            for away, i in others:
                dispatch(kind, away, i, c).start()
            recv[kind + 1, spot, c] = buf[kind, mine, c]

    def hop(group):
        return (plane, sibling, gate_plane, gate_plane)[group]

    def give_back(group, i, c):
        s = spots[i]
        kind = max(group - 1, 0)
        return remote(
            outb.at[group, s] if c is None else outb.at[group, s, c],
            ret.at[kind, mine] if c is None else ret.at[kind, mine, c],
            send2.at[group],
            recv2.at[kind * chunks + (c or 0)],
            at(hop(group) * n2 + s),
        )

    def given_back(group, count):
        sent = outb.at[group, pl.ds(0, count)]
        remote(sent, sent, send2.at[group], recv2.at[0], at(base + outer)).wait_send()

    def arrived(group, c, count):
        part = recv.at[group, pl.ds(0, count)]
        if c is not None:
            part = recv.at[group, pl.ds(0, count), c]
        remote(
            part, part, send1.at[0], recv1.at[group * chunks + (c or 0)], at(base + outer)
        ).wait_recv()

    def by_role(act):
        @pl.when(on_end)
        def _():
            act(n2)

        @pl.when(on_gate)
        def _():
            act(n2 - 1)

    piece = min(256, half)

    def feed(x):
        for part in range(2):
            for low in range(0, half, piece):
                gate_pre = jnp.dot(
                    x, wgs[part, :, low : low + piece], preferred_element_type=F32
                )
                up_pre = jnp.dot(x, wus[part, :, low : low + piece], preferred_element_type=F32)
                hid[part, :, low : low + piece] = clamped_unit(gate_pre, up_pre)

    def down(c):
        return jnp.dot(
            hid[0], wds[0, :, c * chunk : (c + 1) * chunk], preferred_element_type=F32
        ) + jnp.dot(
            hid[1], wds[1, :, c * chunk : (c + 1) * chunk], preferred_element_type=F32
        )

    def store_out(group, c):
        outb[group, :, c] = down(c).astype(BF16).reshape(n2, tall, chunk)

    def take_in(group, c):
        xs[:, c * chunk : (c + 1) * chunk] = recv[group, :, c].reshape(group_rows, chunk)

    def run_near(group):
        with jax.named_scope("neararrive"):
            arrived(group, None, n2 - 1 + group)
        with jax.named_scope("near"):
            for c in range(chunks):
                take_in(group, c)
            feed(xs[...])
            for c in range(chunks):
                store_out(group, c)
            if group == 0:
                ret[0, mine] = outb[0, spot]

    def send_near(group, low, high):
        for i in range(low, high):
            give_back(group, i, None).start()

    def run_far(group):
        for c in range(chunks):
            with jax.named_scope("arrive"):
                by_role(lambda count: arrived(group, c, count))
            take_in(group, c)
        with jax.named_scope("feed"):
            feed(xs[...])
        for c in range(chunks):
            store_out(group, c)

            @pl.when(on_end)
            def _():
                for i in range(1, n2):
                    pass_on(group, i, c).start()
                relay[group - 2, spot, c] = outb[group, spot, c]

            @pl.when(on_gate)
            def _():
                for i in range(1, n2):
                    give_back(group, i, c).start()
                ret[group - 1, mine, c] = outb[group, spot, c]

    def pass_on(group, i, c):
        s = spots[i]
        return remote(
            outb.at[group, s, c],
            relay.at[group - 2, spot, c],
            send2.at[group],
            relay_recv.at[(group - 2) * chunks + c],
            at(plane * n2 + s),
        )

    def forward(group, c):
        return remote(
            relay.at[group - 2, :, c],
            ret.at[group - 1, pl.ds(inner, n2), c],
            relay_send.at[group - 2],
            recv2.at[(group - 1) * chunks + c],
            at(sibling * n2 + spot),
        )

    def run_relay(group):
        with jax.named_scope("relay"):
            for c in range(chunks):
                part = relay.at[group - 2, pl.ds(0, n2 - 1), c]
                remote(
                    part,
                    part,
                    relay_send.at[0],
                    relay_recv.at[(group - 2) * chunks + c],
                    at(base + outer),
                ).wait_recv()
                forward(group, c).start()

    def returned(kind, c):
        part = ret.at[kind, pl.ds(0, near - 1)]
        if c is not None:
            part = ret.at[kind, pl.ds(0, near - 1), c]
        remote(
            part, part, send2.at[0], recv2.at[kind * chunks + (c or 0)], at(base + outer)
        ).wait_recv()

    def weighed(kind, c):
        back = ret[kind, :, c].reshape(near * tall, chunk)
        picked = jnp.dot(wanted[kind], back, preferred_element_type=F32)
        return (
            picked[:rows] * columns[kind, :, 2:3] + picked[rows:] * columns[kind, :, 3:4]
        )

    def fin_copy(kind, c):
        target = fin.at[c] if kind == 1 else through.at[c]
        landing = fin_recv.at[c] if kind == 1 else through_recv.at[c]
        return remote(
            pout.at[kind - 1, c],
            target,
            fin_send.at[kind - 1],
            landing,
            at(far_gate * n2 + spot),
        )

    def pass_through(c):
        return remote(
            through.at[c], fin.at[c], through_send, fin_recv.at[c], at(sibling * n2 + spot)
        )

    def run_through(c):
        with jax.named_scope("through"):
            fin_copy(2, c).wait_recv()
            pass_through(c).start()

    def combine(kind, c):
        with jax.named_scope("gatherwait"):
            returned(kind, c)
        with jax.named_scope("combine"):
            pout[kind - 1, c] = weighed(kind, c).astype(BF16)
            fin_copy(kind, c).start()

    def dense_branch():
        depth = din_ref.shape[1]
        x = jnp.concatenate(
            [
                dense[0, c]
                for c in range(chunks)
            ],
            axis=1,
        )
        pre = jnp.dot(x, dn[0].reshape(width, depth), preferred_element_type=F32)
        dense_hidden = jax.nn.silu(pre).astype(BF16)
        step = width // n1
        for z in range(n1):
            branch = lax.dot_general(
                dense_hidden,
                dn[1, z].reshape(step, depth),
                (((1,), (1,)), ((), ())),
                preferred_element_type=F32,
            )
            accs[:, z * step : (z + 1) * step] = (
                jax.nn.sigmoid(dgate_in[:, z * step : (z + 1) * step]) * branch
            )

    def own():
        with jax.named_scope("ownwait"):
            returned(0, None)
        for c in range(chunks):
            span = slice(c * chunk, (c + 1) * chunk)
            accs[:, span] = accs[:, span] + weighed(0, c)

    with jax.named_scope("barrier"):
        pl.semaphore_wait(barrier, near + 1 + is_gate)
    for copy in meta_copies():
        copy.start()

    @pl.when(on_gate)
    def _():
        dn_cross(plane).start()

    dense_start()
    dn_near(plane).start()

    @pl.when(on_end)
    def _():
        dn_far(plane).start()

    for i in range(3):
        weight_copy(i).start()
    with jax.named_scope("selectown"):
        select_own()
    dn_start(0, 0)

    def weights_wait():
        with jax.named_scope("weightwait"):
            for i, (src, dst) in enumerate(weight_pairs):
                pltpu.make_async_copy(src, dst.at[0], w_local.at[i]).wait()
            for i in range(3):
                weight_copy(i).wait()

    def prepare_for(kind):
        with jax.named_scope("prepare"):
            meta_wait(kind)
            prepare(kind)

    part = chunks // 2

    def step_wait(index):
        with jax.named_scope("stepwait"):
            dn_bytes(index, 0).wait_recv()

    @pl.when(on_gate)
    def _():
        prepare_for(2)
        select(2, 0)
        step_wait(0)
        dn_start(0, 1)
        for c in range(1, chunks):
            select(2, c)
        prepare_for(1)
        weights_wait()
        run_near(0)
        send_near(0, 1, n2)
        select(1, 0)
        with jax.named_scope("upwait"):
            dn_cross(far_gate).wait_recv()
        dn_down(0).start()

    @pl.when(on_end)
    def _():
        step_wait(0)
        dn_start(0, 1)
        weights_wait()
        run_near(0)
        send_near(0, 1, n2)
        run_near(1)

    with jax.named_scope("farC"):
        run_far(3)

    @pl.when(on_end)
    def _():
        run_relay(3)
        send_near(1, 0, 1)
        with jax.named_scope("upwait"):
            dn_near(sibling).wait_recv()
            for order in range(2):
                dn_down(order).wait_recv()
        dn_start(1, 0)

    @pl.when(on_gate)
    def _():
        select(1, 1)
        with jax.named_scope("upwait"):
            dn_far(far_end).wait_recv()
            dn_near(sibling).wait_recv()
        dn_down(1).start()
        select(1, 2)
        run_near(1)
        select(1, 3)
        dn_start(1, 0)
        for c in range(chunks):
            combine(2, c)
        send_near(1, 0, part)
        run_through(0)

    with jax.named_scope("farB"):
        run_far(2)

    @pl.when(on_gate)
    def _():
        step_wait(1)
        dn_start(1, 1)
        run_through(1)
        combine(1, 0)
        run_through(2)
        send_near(1, part, n2)
        combine(1, 1)
        run_through(3)
        combine(1, 2)
        combine(1, 3)

    @pl.when(on_end)
    def _():
        step_wait(1)
        dn_start(1, 1)
        run_relay(2)
        send_near(1, 1, n2)

    with jax.named_scope("dnwait"):
        for p in range(2):
            dn_bytes(p, 1).wait_recv()
        dn_swap(core).start()
        dn_swap(peer).wait_recv()
    with jax.named_scope("densebranch"):
        dense_branch()
    with jax.named_scope("own"):
        own()

    with jax.named_scope("drain"):
        for away in range(2):
            dispatched(0, away)
        for copy in meta_copies():
            copy.wait_send()
        remote(
            dense.at[0], dense.at[0], dense_send, dense_recv.at[0, 0], at(base + outer)
        ).wait_send()
        for group in range(2):
            given_back(group, n2 - 1 + group)
        for group in range(2, n1):
            given_back(group, n2 - 1)
        dn_near(plane).wait_send()
        for p in range(2):
            for step in range(2):
                dn_bytes(p, step).wait_send()
        dn_swap(core).wait_send()

        @pl.when(on_end)
        def _():
            dn_far(plane).wait_send()
            for group in (0, 1):
                remote(
                    relay.at[group],
                    relay.at[group],
                    relay_send.at[group],
                    relay_recv.at[0],
                    at(base + outer),
                ).wait_send()

        @pl.when(on_gate)
        def _():
            for away in range(2):
                dispatched(2, away)
            for away in range(2):
                dispatched(1, away)
            remote(
                through, through, through_send, through_recv.at[0], at(base + outer)
            ).wait_send()
            dn_cross(plane).wait_send()
            for order in range(2):
                dn_down(order).wait_send()

    with jax.named_scope("finish"):
        for c in range(chunks):
            with jax.named_scope("finwait"):
                fin_copy(1, c).wait_recv()
            span = slice(c * chunk, (c + 1) * chunk)
            out_ref[:, span] = (accs[:, span] + fin[c].astype(F32)).astype(BF16)

    @pl.when(on_gate)
    def _():
        for kind in (1, 2):
            sent = pout.at[kind - 1]
            remote(
                sent, sent, fin_send.at[kind - 1], fin_recv.at[0], at(base + outer)
            ).wait_send()


def gateway_call(sizes, operands):
    n, n1, n2, tall = sizes
    tokens, dense_in, w_gate = operands[2], operands[5], operands[7]
    rows, width = tokens.shape
    half, depth = w_gate.shape[1], dense_in.shape[1]
    near, chunks = n // 2, CHUNKS
    chunk = width // chunks
    vmem = pl.BlockSpec(memory_space=pltpu.VMEM)
    anywhere = pl.BlockSpec(memory_space=pltpu.HBM)
    dma = pltpu.SemaphoreType.DMA
    return pl.pallas_call(
        functools.partial(gateway_kernel, sizes),
        out_shape=jax.ShapeDtypeStruct((rows, width), BF16),
        in_specs=[anywhere] * 10,
        out_specs=vmem,
        scratch_shapes=[
            pltpu.VMEM((rows, width), BF16),
            pltpu.VMEM((1, width), F32),
            pltpu.VMEM((1, width), F32),
            pltpu.VMEM((3, 2, rows), jnp.int32),
            pltpu.VMEM((3, 2, rows), F32),
            pltpu.VMEM((3, chunks, rows, chunk), BF16),
            pltpu.VMEM((3, near * tall, rows), BF16),
            pltpu.VMEM((3, 2 * rows, near * tall), BF16),
            pltpu.VMEM((3, rows, 8), F32),
            pltpu.VMEM((3, near, chunks, tall, chunk), BF16),
            pltpu.VMEM((n1, n2, chunks, tall, chunk), BF16),
            pltpu.VMEM((n2 * tall, width), BF16),
            pltpu.VMEM((2, n2 * tall, half), BF16),
            pltpu.VMEM((n1, n2, chunks, tall, chunk), BF16),
            pltpu.VMEM((3, near, chunks, tall, chunk), BF16),
            pltpu.VMEM((2, n2, chunks, tall, chunk), BF16),
            pltpu.VMEM((rows, width), F32),
            pltpu.VMEM((2, chunks, rows, chunk), BF16),
            pltpu.VMEM((chunks, rows, chunk), BF16),
            pltpu.VMEM((chunks, rows, chunk), BF16),
            pltpu.VMEM((2, width, half), BF16),
            pltpu.VMEM((2, width, half), BF16),
            pltpu.VMEM((2, half, width), BF16),
            pltpu.VMEM((2, n1, n2, width // n, depth), BF16),
            dma((3,)),
            dma((3,)),
            dma((3,)),
            dma((2,)),
            dma((2, 2)),
            dma,
            dma((2, chunks)),
            dma((6,)),
            dma((n1 * chunks,)),
            dma((n1,)),
            dma((3 * chunks,)),
            dma((2,)),
            dma((chunks,)),
            dma((10,)),
            dma((10,)),
            dma((2,)),
            dma((2 * chunks,)),
            dma,
            dma((chunks,)),
            dma((6,)),
        ],
        compiler_params=pltpu.CompilerParams(
            collective_id=0, has_side_effects=True, vmem_limit_bytes=60 * 1024 * 1024
        ),
    )(*operands)


def shards(
    tokens, norm_gain, routes, route_weights, w_gate, w_up, w_down, dense_in, dense_out, dense_gate
):
    rows, width = tokens.shape
    top_count = routes.shape[1]
    n = lax.axis_size("ep")
    capacity = (4 * rows * top_count + 3 * n - 1) // (3 * n)
    cap = capacity
    blocks = 8 // math.gcd(cap, 8)
    tall, tile = blocks * cap, width // blocks
    n2 = 1
    while n2 * n2 < n:
        n2 *= 2
    n1 = n // n2
    half = w_gate.shape[2]
    depth = dense_in.shape[1]
    if n1 == 4 and n2 == 4 and width % (CHUNKS * LANES) == 0 and width % n == 0:
        return gateway_call(
            (n, n1, n2, -(-cap // 8) * 8),
            (
                routes.T,
                route_weights.T,
                tokens,
                norm_gain.reshape(1, width),
                dense_gate.reshape(1, width),
                dense_in,
                dense_out,
                w_gate[0],
                w_up[0],
                w_down[0],
            ),
        )
    vmem = pl.BlockSpec(memory_space=pltpu.VMEM)
    anywhere = pl.BlockSpec(memory_space=pl.ANY)
    dma = pltpu.SemaphoreType.DMA
    slab = pltpu.VMEM((n, tall, tile), BF16)
    return pl.pallas_call(
        functools.partial(layer_kernel, (n, n1, n2, cap, blocks)),
        out_shape=jax.ShapeDtypeStruct((rows, width), BF16),
        in_specs=[vmem] * 8 + [anywhere] * 3,
        out_specs=vmem,
        scratch_shapes=[
            pltpu.VMEM((rows, width), BF16),
            pltpu.VMEM((n1, n2, blocks * rows), jnp.int32),
            pltpu.VMEM((blocks * rows, tile), BF16),
            pltpu.VMEM((rows, 2), jnp.int32),
            pltpu.VMEM((n2 * cap, width), BF16),
            pltpu.VMEM((n2 * tall, tile), F32),
            pltpu.VMEM((n2 * tall, n2 * tall), BF16),
            pltpu.VMEM((n2 * tall, n2 * tall), BF16),
            slab,
            slab,
            slab,
            slab,
            pltpu.VMEM((2, width, half), BF16),
            pltpu.VMEM((2, width, half), BF16),
            pltpu.VMEM((2, half, width), BF16),
            pltpu.VMEM((2, n2 * cap, half), BF16),
            pltpu.VMEM((2, n1, n2, width // n, depth), BF16),
            pltpu.VMEM((rows, width), F32),
            dma((n,)),
            dma((n,)),
            dma((n,)),
            dma((n,)),
            dma((3,)),
            dma((3,)),
            dma((3,)),
            dma((n1,)),
            dma((n1,)),
            dma((n2,)),
            dma((n2,)),
            dma,
            dma,
        ],
        compiler_params=pltpu.CompilerParams(
            collective_id=0, has_side_effects=True, vmem_limit_bytes=60 * 1024 * 1024
        ),
    )(
        routes.T,
        routes,
        route_weights,
        tokens,
        norm_gain.reshape(1, width),
        dense_gate.reshape(1, width),
        dense_in,
        dense_out,
        w_gate[0],
        w_up[0],
        w_down[0],
    )


def solution(mesh):
    placed = (
        P(("ep", "tp"), None),
        P(),
        P(("ep", "tp"), None),
        P(("ep", "tp"), None),
        P("ep", None, "tp"),
        P("ep", None, "tp"),
        P("ep", "tp", None),
        P("ep", None),
        P("ep", None),
        P(),
    )
    return jax.shard_map(
        shards, mesh=mesh, in_specs=placed, out_specs=P(("ep", "tp"), None), check_vma=False
    )
```

```python
import functools
import math

import jax
import jax.numpy as jnp
from jax import lax
from jax.experimental import pallas as pl
from jax.experimental.pallas import tpu as pltpu
from jax.sharding import PartitionSpec as P

CLAMP_LIMIT = 7.0
SLOPE_ALPHA = 1.702
NORM_EPS = 1e-06
MESH = pl.DeviceIdType.MESH
F32 = jnp.float32
BF16 = jnp.bfloat16


def clamped_unit(gate_pre, up_pre):
    gate_clip = jnp.minimum(gate_pre, CLAMP_LIMIT)
    up_clip = jnp.clip(up_pre, -CLAMP_LIMIT, CLAMP_LIMIT)
    return ((up_clip + 1.0) * gate_clip * jax.nn.sigmoid(SLOPE_ALPHA * gate_clip)).astype(BF16)


def layer_kernel(
    sizes,
    routes_t_ref,
    routes_ref,
    weights_ref,
    tokens_ref,
    gain_ref,
    dgate_ref,
    din_ref,
    dout_ref,
    wg_ref,
    wu_ref,
    wd_ref,
    out_ref,
    normed,
    keys,
    stacked,
    places,
    xs,
    totals,
    unpack_ref,
    pack_ref,
    buf,
    recv,
    outb,
    ret,
    wgs,
    wus,
    wds,
    hid,
    dn,
    acc,
    send1,
    recv1,
    send2,
    recv2,
    w_local,
    w_send,
    w_recv,
    ds1,
    dr1,
    ds2,
    dr2,
    ds3,
    dr3,
):
    n, n1, n2, cap, blocks = sizes
    rows, width = tokens_ref.shape
    half = wg_ref.shape[1]
    tall, tile = blocks * cap, width // blocks
    group_rows, packed_rows = n2 * cap, n2 * blocks * cap
    me = lax.axis_index("ep")
    core = lax.axis_index("tp")
    plane, spot = me // n2, me % n2
    peer = 1 - core

    barrier = pltpu.get_barrier_semaphore()

    def greet(i, carry):
        pl.semaphore_signal(
            barrier, inc=1, device_id={"ep": (me + i) % n}, device_id_type=MESH
        )
        return carry

    lax.fori_loop(1, n, greet, 0)
    pl.semaphore_signal(barrier, inc=1, device_id={"tp": peer}, device_id_type=MESH)

    weight_pairs = ((wg_ref, wgs), (wu_ref, wus), (wd_ref, wds))
    for i, (src, dst) in enumerate(weight_pairs):
        pltpu.make_async_copy(src, dst.at[0], w_local.at[i]).start()

    @pl.when(core == 0)
    def _():
        dn[0, plane, spot] = din_ref[...]

    @pl.when(core == 1)
    def _():
        dn[1, plane, spot] = dout_ref[...]

    widened = tokens_ref[...].astype(F32)
    inv_scale = lax.rsqrt(jnp.mean(widened * widened, axis=1, keepdims=True) + NORM_EPS)
    normed[...] = (widened * inv_scale * gain_ref[...]).astype(BF16)
    for j in range(blocks):
        stacked[j * rows : (j + 1) * rows, :] = normed[:, j * tile : (j + 1) * tile]

    expert_ids = lax.broadcasted_iota(jnp.int32, (n, rows), 0)
    chosen = (routes_t_ref[0:1, :] == expert_ids) | (routes_t_ref[1:2, :] == expert_ids)
    earlier = (
        lax.broadcasted_iota(jnp.int32, (rows, rows), 0)
        < lax.broadcasted_iota(jnp.int32, (rows, rows), 1)
    )
    counted = jnp.dot(
        jnp.where(chosen, 1.0, 0.0).astype(BF16),
        jnp.where(earlier, 1.0, 0.0).astype(BF16),
        preferred_element_type=F32,
    )
    for j in range(blocks):
        found = jnp.where(chosen, counted.astype(jnp.int32) + j * cap, -1)
        for z in range(n1):
            keys[z, :, j * rows : (j + 1) * rows] = found[z * n2 : (z + 1) * n2]
    experts_across = lax.broadcasted_iota(jnp.int32, (rows, n), 1)
    takes = [routes_ref[:, k : k + 1] == experts_across for k in range(2)]
    before = (
        lax.broadcasted_iota(jnp.int32, (rows, rows), 0)
        > lax.broadcasted_iota(jnp.int32, (rows, rows), 1)
    )
    counts = jnp.dot(
        jnp.where(before, 1.0, 0.0).astype(BF16),
        jnp.where(takes[0] | takes[1], 1.0, 0.0).astype(BF16),
        preferred_element_type=F32,
    )
    for k in range(2):
        slot = jnp.sum(jnp.where(takes[k], counts, 0.0), axis=1, keepdims=True)
        places[:, k : k + 1] = routes_ref[:, k : k + 1] * tall + slot.astype(jnp.int32)

    pl.semaphore_wait(barrier, n)

    def weight_copy(i):
        src, dst = weight_pairs[i]
        return pltpu.make_async_remote_copy(
            src_ref=src,
            dst_ref=dst.at[1],
            send_sem=w_send.at[i],
            recv_sem=w_recv.at[i],
            device_id={"tp": peer},
            device_id_type=MESH,
        )

    def dense_copy1(bit, block):
        other = plane + bit - 2 * bit * ((plane // bit) % 2)
        return pltpu.make_async_remote_copy(
            src_ref=dn.at[core, block, spot],
            dst_ref=dn.at[core, block, spot],
            send_sem=ds1.at[block],
            recv_sem=dr1.at[block],
            device_id={"ep": other * n2 + spot},
            device_id_type=MESH,
        )

    bits = [1 << b for b in reversed(range(n1.bit_length() - 1))]

    def dense_held(bit, where):
        return [where % (2 * bit) + m * 2 * bit for m in range(n1 // (2 * bit))]

    def dense_start(bit):
        for block in dense_held(bit, plane):
            dense_copy1(bit, block).start()

    def dense_finish(bit):
        for block in dense_held(bit, plane + bit - 2 * bit * ((plane // bit) % 2)):
            dense_copy1(bit, block).wait_recv()
        for block in dense_held(bit, plane):
            dense_copy1(bit, block).wait_send()

    def dense_copy2(other, slot):
        return pltpu.make_async_remote_copy(
            src_ref=dn.at[core, :, slot],
            dst_ref=dn.at[core, :, slot],
            send_sem=ds2.at[other],
            recv_sem=dr2.at[slot],
            device_id={"ep": plane * n2 + other},
            device_id_type=MESH,
        )

    def dense_copy3(which):
        return pltpu.make_async_remote_copy(
            src_ref=dn.at[which],
            dst_ref=dn.at[which],
            send_sem=ds3,
            recv_sem=dr3,
            device_id={"tp": peer},
            device_id_type=MESH,
        )

    def each(count, act):
        def step(i, carry):
            act(i)
            return carry

        lax.fori_loop(0, count, step, 0)

    dense_start(bits[0])
    for i in range(3):
        weight_copy(i).start()

    def dispatch(dst, slot):
        return pltpu.make_async_remote_copy(
            src_ref=buf.at[dst],
            dst_ref=recv.at[slot],
            send_sem=send1.at[dst],
            recv_sem=recv1.at[slot],
            device_id={"ep": dst},
            device_id_type=MESH,
        )

    def give_back(dst, slot):
        return pltpu.make_async_remote_copy(
            src_ref=outb.at[dst],
            dst_ref=ret.at[slot],
            send_sem=send2.at[dst],
            recv_sem=recv2.at[slot],
            device_id={"ep": dst},
            device_id_type=MESH,
        )

    def partner_plane(x):
        return sum(((plane // b) % 2 + (x // b) % 2) % 2 * b for b in bits)

    def turn(i):
        return partner_plane(i % 2 * (n1 // 2) + i // 2)

    def send_group(i):
        group = partner_plane((i + n1 // 2) % n1)
        first = group * n2
        wanted = keys[group]
        picks = wanted[:, None, :] == lax.broadcasted_iota(
            jnp.int32, (n2, tall, blocks * rows), 1
        )
        picks = jnp.where(picks, 1.0, 0.0).reshape(packed_rows, blocks * rows).astype(BF16)
        found = jnp.dot(picks, stacked[...], preferred_element_type=F32)
        buf[pl.ds(first, n2)] = found.reshape(n2, tall, tile).astype(BF16)

        def start(j):
            dst = first + (spot + 1 + j) % n2

            @pl.when(dst != me)
            def _():
                dispatch(dst, me).start()

            @pl.when(dst == me)
            def _():
                recv[me] = buf[me]

        each(n2, start)

    each(n1, send_group)


    for i, (src, dst) in enumerate(weight_pairs):
        pltpu.make_async_copy(src, dst.at[0], w_local.at[i]).wait()
    for i in range(3):
        weight_copy(i).wait()

    piece = min(256, half)
    upright = lax.broadcasted_iota(jnp.int32, (packed_rows, packed_rows), 0)
    across = lax.broadcasted_iota(jnp.int32, (packed_rows, packed_rows), 1)

    def packed_place(r):
        return (r // cap) % n2 * tall + r // group_rows * cap + r % cap

    unpack = jnp.where(packed_place(upright) == across, 1.0, 0.0).astype(BF16)
    pack = jnp.where(packed_place(across) == upright, 1.0, 0.0).astype(BF16)
    unpack_ref[...] = unpack
    pack_ref[...] = pack

    def run_group(i):
        group = turn(i)
        first = group * n2

        def arrive(j):
            src = first + j

            @pl.when(src != me)
            def _():
                dispatch(src, src).wait_recv()

        each(n2, arrive)
        came = recv[pl.ds(first, n2)].astype(F32).reshape(packed_rows, tile).astype(BF16)
        apart = jnp.dot(unpack_ref[...], came, preferred_element_type=F32)
        for j in range(blocks):
            xs[:, j * tile : (j + 1) * tile] = apart[
                j * group_rows : (j + 1) * group_rows
            ].astype(BF16)
        x = xs[...]
        for part in range(2):
            for low in range(0, half, piece):
                gate_pre = jnp.dot(
                    x, wgs[part, :, low : low + piece], preferred_element_type=F32
                )
                up_pre = jnp.dot(x, wus[part, :, low : low + piece], preferred_element_type=F32)
                hid[part, :, low : low + piece] = clamped_unit(gate_pre, up_pre)
        for j in range(blocks):
            total = jnp.zeros((group_rows, tile), F32)
            for part in range(2):
                partial = jnp.dot(
                    hid[part],
                    wds[part, :, j * tile : (j + 1) * tile],
                    preferred_element_type=F32,
                )
                total = total + partial.astype(BF16).astype(F32)
            totals[j * group_rows : (j + 1) * group_rows, :] = total
        joined = jnp.dot(pack_ref[...], totals[...].astype(BF16), preferred_element_type=F32)
        outb[pl.ds(first, n2)] = joined.reshape(n2, tall, tile).astype(BF16)

        def start(j):
            dst = first + (spot + 1 + j) % n2

            @pl.when(dst != me)
            def _():
                give_back(dst, me).start()

            @pl.when(dst == me)
            def _():
                ret[me] = outb[me]

        each(n2, start)

    def run_turn(i):
        run_group(i)
        for b, bit in enumerate(bits):

            @pl.when(i == b)
            def _():
                dense_finish(bit)
                if b + 1 < len(bits):
                    dense_start(bits[b + 1])
                else:
                    each(n2 - 1, lambda j: dense_copy2((spot + 1 + j) % n2, spot).start())

    each(n1, run_turn)
    each(n2 - 1, lambda i: dense_copy2((spot + 1 + i) % n2, (spot + 1 + i) % n2).wait_recv())
    dense_copy3(core).start()
    dense_copy3(core).wait_send()
    dense_copy3(peer).wait_recv()
    depth = din_ref.shape[1]
    dense_pre = jnp.dot(
        normed[...], dn[0].reshape(width, depth), preferred_element_type=F32
    )
    dense_hidden = jax.nn.silu(dense_pre).astype(BF16)
    step = width // n1
    for z in range(n1):
        branch = lax.dot_general(
            dense_hidden,
            dn[1, z].reshape(step, depth),
            (((1,), (1,)), ((), ())),
            preferred_element_type=F32,
        )
        acc[:, z * step : (z + 1) * step] = (
            jax.nn.sigmoid(dgate_ref[:, z * step : (z + 1) * step]) * branch
        )

    def combine_group(i):
        group = turn(i)
        first = group * n2

        def arrive(j):
            src = first + j

            @pl.when(src != me)
            def _():
                give_back(src, src).wait_recv()

        each(n2, arrive)
        back = ret[pl.ds(first, n2)].astype(F32).reshape(packed_rows, tile).astype(BF16)
        lanes = lax.broadcasted_iota(jnp.int32, (rows, packed_rows), 1) + first * tall
        wanted = jnp.concatenate(
            [
                jnp.where(places[:, k : k + 1] + j * cap == lanes, 1.0, 0.0).astype(BF16)
                for k in range(2)
                for j in range(blocks)
            ],
            axis=0,
        )
        picked = jnp.dot(wanted, back, preferred_element_type=F32)
        for j in range(blocks):
            total = acc[:, j * tile : (j + 1) * tile]
            for k in range(2):
                at = (k * blocks + j) * rows
                total = total + picked[at : at + rows] * weights_ref[:, k : k + 1]
            acc[:, j * tile : (j + 1) * tile] = total

    each(n1, combine_group)
    out_ref[...] = acc[...].astype(BF16)

    def drain(i):
        other = (me + 1 + i) % n
        dispatch(other, me).wait_send()
        give_back(other, me).wait_send()

    each(n - 1, drain)
    each(n2 - 1, lambda i: dense_copy2((spot + 1 + i) % n2, spot).wait_send())


LANES = 128
CHUNKS = 4


def gateway_kernel(
    sizes,
    routes_ref,
    weights_ref,
    tokens_ref,
    gain_ref,
    dgate_ref,
    din_ref,
    dout_ref,
    wg_ref,
    wu_ref,
    wd_ref,
    out_ref,
    tokens_in,
    mixed,
    gain_in,
    dgate_in,
    routes_of,
    weights_of,
    dense,
    picks,
    wanted,
    columns,
    buf,
    recv,
    xs,
    hid,
    outb,
    ret,
    relay,
    accs,
    pout,
    fin,
    through,
    wgs,
    wus,
    wds,
    dn,
    w_local,
    w_send,
    w_recv,
    meta_send,
    meta_recv,
    dense_send,
    dense_recv,
    send1,
    recv1,
    send2,
    recv2,
    fin_send,
    fin_recv,
    dn_send,
    dn_recv,
    relay_send,
    relay_recv,
    through_send,
    through_recv,
    inputs,
    out_sem,
):
    n, n1, n2, tall = sizes
    rows, width = tokens_ref.shape
    half = wg_ref.shape[1]
    chunks = CHUNKS
    chunk = width // chunks
    near = n // 2
    group_rows = n2 * tall
    me = lax.axis_index("ep")
    core = lax.axis_index("tp")
    peer = 1 - core
    plane, spot = me // n2, me % n2
    side = plane // 2
    mine = me % near
    base = side * near
    is_gate = (plane + 1) // 2 % 2
    sibling = plane + 1 - 2 * (plane % 2)
    gate_plane = 1 + side
    far_gate = 2 - side
    far_end = 3 - 3 * side
    on_gate = is_gate == 1
    on_end = is_gate == 0

    def at(where):
        return {"ep": where}

    def each(count, act):
        def step(i, carry):
            act(i)
            return carry

        lax.fori_loop(0, count, step, 0)

    def remote(src, dst, send_sem, recv_sem, device):
        return pltpu.make_async_remote_copy(
            src_ref=src,
            dst_ref=dst,
            send_sem=send_sem,
            recv_sem=recv_sem,
            device_id=device,
            device_id_type=MESH,
        )

    barrier = pltpu.get_barrier_semaphore()
    small_pairs = (
        (tokens_ref, tokens_in),
        (gain_ref, gain_in),
        (routes_ref, routes_of.at[0]),
        (weights_ref, weights_of.at[0]),
        (dgate_ref, dgate_in),
    )
    small_copies = [
        pltpu.make_async_copy(src, dst, inputs.at[i])
        for i, (src, dst) in enumerate(small_pairs)
    ]
    for copy in small_copies:
        copy.start()

    def greet(device):
        pl.semaphore_signal(barrier, inc=1, device_id=device, device_id_type=MESH)

    each(near - 1, lambda i: greet(at(base + (mine + 1 + i) % near)))
    greet({"tp": peer})
    greet(at(far_gate * n2 + spot))

    @pl.when(on_gate)
    def _():
        greet(at(far_end * n2 + spot))

    def block_copy(which):
        return pltpu.make_async_copy(
            (din_ref, dout_ref)[which], dn.at[which, plane, spot], inputs.at[5]
        )

    for which in range(2):

        @pl.when(core == which)
        def _():
            block_copy(which).start()

    block_copy(0).wait()
    for copy in small_copies:
        copy.wait()
    weight_pairs = ((wg_ref, wgs), (wu_ref, wus), (wd_ref, wds))
    for i, (src, dst) in enumerate(weight_pairs):
        pltpu.make_async_copy(src, dst.at[0], w_local.at[i]).start()

    with jax.named_scope("norm"):
        widened = tokens_in[...].astype(F32)
        inv_scale = lax.rsqrt(jnp.mean(widened * widened, axis=1, keepdims=True) + NORM_EPS)
        normed = (widened * inv_scale * gain_in[...]).astype(BF16)
        for c in range(chunks):
            dense[0, c] = normed[:, c * chunk : (c + 1) * chunk]

    def prepare(kind):
        experts = lax.broadcasted_iota(jnp.int32, (near, rows), 0) + base
        first, second = routes_of[kind, 0:1, :], routes_of[kind, 1:2, :]
        takes = (first == experts, second == experts)
        chosen = takes[0] | takes[1]
        earlier = (
            lax.broadcasted_iota(jnp.int32, (rows, rows), 0)
            < lax.broadcasted_iota(jnp.int32, (rows, rows), 1)
        )
        counted = jnp.dot(
            jnp.where(chosen, 1.0, 0.0).astype(BF16),
            jnp.where(earlier, 1.0, 0.0).astype(BF16),
            preferred_element_type=F32,
        )
        keys = jnp.where(chosen, counted.astype(jnp.int32), -1)
        hits = keys[:, None, :] == lax.broadcasted_iota(jnp.int32, (near, tall, rows), 1)
        picks[kind] = jnp.where(hits, 1.0, 0.0).reshape(near * tall, rows).astype(BF16)
        local = lax.broadcasted_iota(jnp.int32, (near, rows), 0) * tall
        places = [
            jnp.sum(
                jnp.where(take, counted + local.astype(F32) + n * tall, 0.0),
                axis=0,
                keepdims=True,
            )
            - n * tall
            for take in takes
        ]
        stack = jnp.concatenate(
            places + [weights_of[kind], jnp.zeros((4, rows), F32)], axis=0
        )
        turned = jnp.transpose(stack)
        columns[kind] = turned
        lanes = lax.broadcasted_iota(jnp.int32, (rows, near * tall), 1)
        for k in range(2):
            place = turned[:, k : k + 1].astype(jnp.int32)
            wanted[kind, k * rows : (k + 1) * rows, :] = jnp.where(
                place == lanes, 1.0, 0.0
            ).astype(BF16)

    with jax.named_scope("prepare0"):
        prepare(0)

    def meta_copies():
        slot = 2 - is_gate
        device = at(far_gate * n2 + spot)
        return (
            remote(routes_of.at[0], routes_of.at[slot], meta_send.at[0], meta_recv.at[0, slot - 1], device),
            remote(weights_of.at[0], weights_of.at[slot], meta_send.at[1], meta_recv.at[1, slot - 1], device),
        )

    def meta_wait(slot):
        device = at(far_gate * n2 + spot)
        remote(
            routes_of.at[0], routes_of.at[slot], meta_send.at[0], meta_recv.at[0, slot - 1], device
        ).wait_recv()
        remote(
            weights_of.at[0], weights_of.at[slot], meta_send.at[1], meta_recv.at[1, slot - 1], device
        ).wait_recv()

    def dense_copy(slot, c):
        return remote(
            dense.at[0, c],
            dense.at[slot, c],
            dense_send,
            dense_recv.at[slot - 1, c],
            at(far_gate * n2 + spot),
        )

    def dense_start():
        for c in range(chunks):
            dense_copy(2 - is_gate, c).start()

    def dn_block(which, index, target):
        block = dn.at[core, which, spot]
        return remote(
            block, block, dn_send.at[index], dn_recv.at[index], at(target * n2 + spot)
        )

    def dn_near(which):
        return dn_block(which, 0, sibling)

    def dn_cross(which):
        return dn_block(which, 1, far_gate)

    def dn_far(which):
        return dn_block(which, 2, far_gate)

    def dn_down(order):
        return dn_block(far_end if order else far_gate, 3 + order, sibling)

    first_bit, second_bit = 1 + core, 2 - core
    first_spot = spot + first_bit - 2 * first_bit * (spot // first_bit % 2)
    second_spot = spot + second_bit - 2 * second_bit * (spot // second_bit % 2)

    def dn_step(part, step, block):
        index = 5 + 2 * part + step
        return remote(
            block,
            block,
            dn_send.at[index],
            dn_recv.at[index],
            at(plane * n2 + (second_spot if step else first_spot)),
        )

    def dn_start(part, step):
        for slot in (spot, first_spot)[: 1 + step]:
            if part == 0:
                dn_step(part, step, dn.at[core, plane, slot]).start()
            else:
                dn_step(part, step, dn.at[core, sibling, slot]).start()
                dn_step(part, step, dn.at[core, pl.ds((1 - side) * 2, 2), slot]).start()

    def dn_bytes(part, step):
        slots = pl.ds(0, 2) if step else 0
        return dn_step(part, step, dn.at[core, pl.ds(0, n1 - 1) if part else 0, slots])

    def dn_swap(which):
        last = 9
        return remote(
            dn.at[which], dn.at[which], dn_send.at[last], dn_recv.at[last], {"tp": peer}
        )

    def weight_copy(i):
        src, dst = weight_pairs[i]
        return remote(src, dst.at[1], w_send.at[i], w_recv.at[i], {"tp": peer})

    spots = [(spot + i) % n2 for i in range(n2)]
    inner = plane % 2 * n2
    outer = n2 - inner

    def dispatch(kind, away, i, c):
        expert = (outer if away else inner) + spots[i]
        group = kind + 1 if kind else away
        return remote(
            buf.at[kind, expert] if c is None else buf.at[kind, expert, c],
            recv.at[group, spot] if c is None else recv.at[group, spot, c],
            send1.at[kind * 2 + away],
            recv1.at[group * chunks + (c or 0)],
            at(base + expert),
        )

    def dispatched(kind, away):
        sent = buf.at[kind, pl.ds(0, n2 - 1 + away)]
        remote(sent, sent, send1.at[kind * 2 + away], recv1.at[0], at(base + outer)).wait_send()

    others = [(1, i) for i in range(n2)] + [(0, i) for i in range(1, n2)]

    def select_own():
        everything = jnp.concatenate([dense[0, c] for c in range(chunks)], axis=1)
        found = jnp.dot(picks[0], everything, preferred_element_type=F32).astype(BF16)
        for c in range(chunks):
            buf[0, :, c] = found[:, c * chunk : (c + 1) * chunk].reshape(near, tall, chunk)
        for away, i in others:
            dispatch(0, away, i, None).start()
        recv[0, spot] = buf[0, mine]

    def select(kind, c):
        with jax.named_scope("densewait"):
            dense_copy(kind, c).wait_recv()
        with jax.named_scope("select"):
            found = jnp.dot(picks[kind], dense[kind, c], preferred_element_type=F32)
            buf[kind, :, c] = found.astype(BF16).reshape(near, tall, chunk)
            for away, i in others:
                dispatch(kind, away, i, c).start()
            recv[kind + 1, spot, c] = buf[kind, mine, c]

    def hop(group):
        return (plane, sibling, gate_plane, gate_plane)[group]

    def give_back(group, i, c):
        s = spots[i]
        kind = max(group - 1, 0)
        return remote(
            outb.at[group, s] if c is None else outb.at[group, s, c],
            ret.at[kind, mine] if c is None else ret.at[kind, mine, c],
            send2.at[group],
            recv2.at[kind * chunks + (c or 0)],
            at(hop(group) * n2 + s),
        )

    def given_back(group, count):
        sent = outb.at[group, pl.ds(0, count)]
        remote(sent, sent, send2.at[group], recv2.at[0], at(base + outer)).wait_send()

    def arrived(group, c, count):
        part = recv.at[group, pl.ds(0, count)]
        if c is not None:
            part = recv.at[group, pl.ds(0, count), c]
        remote(
            part, part, send1.at[0], recv1.at[group * chunks + (c or 0)], at(base + outer)
        ).wait_recv()

    def by_role(act):
        @pl.when(on_end)
        def _():
            act(n2)

        @pl.when(on_gate)
        def _():
            act(n2 - 1)

    piece = min(256, half)

    def feed(x):
        for part in range(2):
            for low in range(0, half, piece):
                gate_pre = jnp.dot(
                    x, wgs[part, :, low : low + piece], preferred_element_type=F32
                )
                up_pre = jnp.dot(x, wus[part, :, low : low + piece], preferred_element_type=F32)
                hid[part, :, low : low + piece] = clamped_unit(gate_pre, up_pre)

    def down(c):
        return jnp.dot(
            hid[0], wds[0, :, c * chunk : (c + 1) * chunk], preferred_element_type=F32
        ) + jnp.dot(
            hid[1], wds[1, :, c * chunk : (c + 1) * chunk], preferred_element_type=F32
        )

    def store_out(group, c):
        outb[group, :, c] = down(c).astype(BF16).reshape(n2, tall, chunk)

    def take_in(group, c):
        xs[:, c * chunk : (c + 1) * chunk] = recv[group, :, c].reshape(group_rows, chunk)

    def run_near(group):
        with jax.named_scope("neararrive"):
            arrived(group, None, n2 - 1 + group)
        with jax.named_scope("near"):
            for c in range(chunks):
                take_in(group, c)
            feed(xs[...])
            for c in range(chunks):
                store_out(group, c)
            if group == 0:
                ret[0, mine] = outb[0, spot]

    def send_near(group, low, high):
        for i in range(low, high):
            give_back(group, i, None).start()

    def run_far(group):
        for c in range(chunks):
            with jax.named_scope("arrive"):
                by_role(lambda count: arrived(group, c, count))
            take_in(group, c)
        with jax.named_scope("feed"):
            feed(xs[...])
        for c in range(chunks):
            store_out(group, c)

            @pl.when(on_end)
            def _():
                for i in range(1, n2):
                    pass_on(group, i, c).start()
                relay[group - 2, spot, c] = outb[group, spot, c]

            @pl.when(on_gate)
            def _():
                for i in range(1, n2):
                    give_back(group, i, c).start()
                ret[group - 1, mine, c] = outb[group, spot, c]

    def pass_on(group, i, c):
        s = spots[i]
        return remote(
            outb.at[group, s, c],
            relay.at[group - 2, spot, c],
            send2.at[group],
            relay_recv.at[(group - 2) * chunks + c],
            at(plane * n2 + s),
        )

    def forward(group, c):
        return remote(
            relay.at[group - 2, :, c],
            ret.at[group - 1, pl.ds(inner, n2), c],
            relay_send.at[group - 2],
            recv2.at[(group - 1) * chunks + c],
            at(sibling * n2 + spot),
        )

    def run_relay(group):
        with jax.named_scope("relay"):
            for c in range(chunks):
                part = relay.at[group - 2, pl.ds(0, n2 - 1), c]
                remote(
                    part,
                    part,
                    relay_send.at[0],
                    relay_recv.at[(group - 2) * chunks + c],
                    at(base + outer),
                ).wait_recv()
                forward(group, c).start()

    def returned(kind, c):
        part = ret.at[kind, pl.ds(0, near - 1)]
        if c is not None:
            part = ret.at[kind, pl.ds(0, near - 1), c]
        remote(
            part, part, send2.at[0], recv2.at[kind * chunks + (c or 0)], at(base + outer)
        ).wait_recv()

    def weighed(kind, c):
        back = ret[kind, :, c].reshape(near * tall, chunk)
        picked = jnp.dot(wanted[kind], back, preferred_element_type=F32)
        return (
            picked[:rows] * columns[kind, :, 2:3] + picked[rows:] * columns[kind, :, 3:4]
        )

    def fin_copy(kind, c):
        target = fin.at[c] if kind == 1 else through.at[c]
        landing = fin_recv.at[c] if kind == 1 else through_recv.at[c]
        return remote(
            pout.at[kind - 1, c],
            target,
            fin_send.at[kind - 1],
            landing,
            at(far_gate * n2 + spot),
        )

    def pass_through(c):
        return remote(
            through.at[c], fin.at[c], through_send, fin_recv.at[c], at(sibling * n2 + spot)
        )

    def run_through(c):
        with jax.named_scope("through"):
            fin_copy(2, c).wait_recv()
            pass_through(c).start()

    def combine(kind, c):
        with jax.named_scope("gatherwait"):
            returned(kind, c)
        with jax.named_scope("combine"):
            pout[kind - 1, c] = weighed(kind, c).astype(BF16)
            fin_copy(kind, c).start()

    def dense_branch():
        depth = din_ref.shape[1]
        x = jnp.concatenate(
            [
                dense[0, c]
                for c in range(chunks)
            ],
            axis=1,
        )
        pre = jnp.dot(x, dn[0].reshape(width, depth), preferred_element_type=F32)
        dense_hidden = jax.nn.silu(pre).astype(BF16)
        step = width // n1
        for z in range(n1):
            branch = lax.dot_general(
                dense_hidden,
                dn[1, z].reshape(step, depth),
                (((1,), (1,)), ((), ())),
                preferred_element_type=F32,
            )
            accs[:, z * step : (z + 1) * step] = (
                jax.nn.sigmoid(dgate_in[:, z * step : (z + 1) * step]) * branch
            )

    def own():
        with jax.named_scope("ownwait"):
            returned(0, None)
        for c in range(chunks):
            span = slice(c * chunk, (c + 1) * chunk)
            accs[:, span] = accs[:, span] + weighed(0, c)

    with jax.named_scope("barrier"):
        pl.semaphore_wait(barrier, near + 1 + is_gate)
    for copy in meta_copies():
        copy.start()

    @pl.when(on_gate)
    def _():
        dn_cross(plane).start()

    dense_start()
    dn_near(plane).start()

    @pl.when(on_end)
    def _():
        dn_far(plane).start()

    for i in range(3):
        weight_copy(i).start()
    with jax.named_scope("selectown"):
        select_own()
    dn_start(0, 0)

    def weights_wait():
        with jax.named_scope("weightwait"):
            for i, (src, dst) in enumerate(weight_pairs):
                pltpu.make_async_copy(src, dst.at[0], w_local.at[i]).wait()
            for i in range(3):
                weight_copy(i).wait()

    def prepare_for(kind):
        with jax.named_scope("prepare"):
            meta_wait(kind)
            prepare(kind)

    part = chunks // 2

    def swap_start():
        with jax.named_scope("swapstart"):
            for p in range(2):
                dn_bytes(p, 1).wait_recv()
        dn_swap(core).start()

    def step_wait(index):
        with jax.named_scope("stepwait"):
            dn_bytes(index, 0).wait_recv()

    @pl.when(on_gate)
    def _():
        prepare_for(2)
        select(2, 0)
        step_wait(0)
        dn_start(0, 1)
        for c in range(1, chunks):
            select(2, c)
        prepare_for(1)
        weights_wait()
        run_near(0)
        send_near(0, 1, n2)
        select(1, 0)
        with jax.named_scope("upwait"):
            dn_cross(far_gate).wait_recv()
        dn_down(0).start()

    @pl.when(on_end)
    def _():
        step_wait(0)
        dn_start(0, 1)
        weights_wait()
        run_near(0)
        send_near(0, 1, n2)
        run_near(1)

    with jax.named_scope("farC"):
        run_far(3)

    @pl.when(on_end)
    def _():
        run_relay(3)
        send_near(1, 0, 1)
        with jax.named_scope("upwait"):
            dn_near(sibling).wait_recv()
            for order in range(2):
                dn_down(order).wait_recv()
        dn_start(1, 0)

    @pl.when(on_gate)
    def _():
        select(1, 1)
        with jax.named_scope("upwait"):
            dn_far(far_end).wait_recv()
            dn_near(sibling).wait_recv()
        dn_down(1).start()
        select(1, 2)
        run_near(1)
        select(1, 3)
        send_near(1, 0, 1)
        dn_start(1, 0)
        for c in range(chunks):
            combine(2, c)
        send_near(1, 1, part)
        run_through(0)

    with jax.named_scope("farB"):
        run_far(2)

    @pl.when(on_gate)
    def _():
        step_wait(1)
        dn_start(1, 1)
        run_through(1)
        run_through(2)
        run_through(3)
        send_near(1, part, n2)
        combine(1, 0)
        combine(1, 1)
        combine(1, 2)
        swap_start()
        combine(1, 3)

    @pl.when(on_end)
    def _():
        step_wait(1)
        dn_start(1, 1)
        run_relay(2)
        send_near(1, 1, n2)
        swap_start()

    with jax.named_scope("dnwait"):
        dn_swap(peer).wait_recv()
    with jax.named_scope("densebranch"):
        dense_branch()
    with jax.named_scope("own"):
        own()

    with jax.named_scope("drain"):
        for away in range(2):
            dispatched(0, away)
        for copy in meta_copies():
            copy.wait_send()
        remote(
            dense.at[0], dense.at[0], dense_send, dense_recv.at[0, 0], at(base + outer)
        ).wait_send()
        for group in range(2):
            given_back(group, n2 - 1 + group)
        for group in range(2, n1):
            given_back(group, n2 - 1)
        dn_near(plane).wait_send()
        for p in range(2):
            for step in range(2):
                dn_bytes(p, step).wait_send()
        dn_swap(core).wait_send()

        @pl.when(on_end)
        def _():
            dn_far(plane).wait_send()
            for group in (0, 1):
                remote(
                    relay.at[group],
                    relay.at[group],
                    relay_send.at[group],
                    relay_recv.at[0],
                    at(base + outer),
                ).wait_send()

        @pl.when(on_gate)
        def _():
            for away in range(2):
                dispatched(2, away)
            for away in range(2):
                dispatched(1, away)
            remote(
                through, through, through_send, through_recv.at[0], at(base + outer)
            ).wait_send()
            dn_cross(plane).wait_send()
            for order in range(2):
                dn_down(order).wait_send()

    with jax.named_scope("finish"):
        for c in range(chunks):
            with jax.named_scope("finwait"):
                fin_copy(1, c).wait_recv()
            span = slice(c * chunk, (c + 1) * chunk)
            mixed[:, span] = (accs[:, span] + fin[c].astype(F32)).astype(BF16)
            pltpu.make_async_copy(mixed.at[:, span], out_ref.at[:, span], out_sem).start()

    @pl.when(on_gate)
    def _():
        for kind in (1, 2):
            sent = pout.at[kind - 1]
            remote(
                sent, sent, fin_send.at[kind - 1], fin_recv.at[0], at(base + outer)
            ).wait_send()

    pltpu.make_async_copy(mixed, out_ref, out_sem).wait()


def gateway_call(sizes, operands):
    n, n1, n2, tall = sizes
    tokens, dense_in, w_gate = operands[2], operands[5], operands[7]
    rows, width = tokens.shape
    half, depth = w_gate.shape[1], dense_in.shape[1]
    near, chunks = n // 2, CHUNKS
    chunk = width // chunks
    anywhere = pl.BlockSpec(memory_space=pltpu.HBM)
    dma = pltpu.SemaphoreType.DMA
    return pl.pallas_call(
        functools.partial(gateway_kernel, sizes),
        out_shape=jax.ShapeDtypeStruct((rows, width), BF16),
        in_specs=[anywhere] * 10,
        out_specs=anywhere,
        scratch_shapes=[
            pltpu.VMEM((rows, width), BF16),
            pltpu.VMEM((rows, width), BF16),
            pltpu.VMEM((1, width), F32),
            pltpu.VMEM((1, width), F32),
            pltpu.VMEM((3, 2, rows), jnp.int32),
            pltpu.VMEM((3, 2, rows), F32),
            pltpu.VMEM((3, chunks, rows, chunk), BF16),
            pltpu.VMEM((3, near * tall, rows), BF16),
            pltpu.VMEM((3, 2 * rows, near * tall), BF16),
            pltpu.VMEM((3, rows, 8), F32),
            pltpu.VMEM((3, near, chunks, tall, chunk), BF16),
            pltpu.VMEM((n1, n2, chunks, tall, chunk), BF16),
            pltpu.VMEM((n2 * tall, width), BF16),
            pltpu.VMEM((2, n2 * tall, half), BF16),
            pltpu.VMEM((n1, n2, chunks, tall, chunk), BF16),
            pltpu.VMEM((3, near, chunks, tall, chunk), BF16),
            pltpu.VMEM((2, n2, chunks, tall, chunk), BF16),
            pltpu.VMEM((rows, width), F32),
            pltpu.VMEM((2, chunks, rows, chunk), BF16),
            pltpu.VMEM((chunks, rows, chunk), BF16),
            pltpu.VMEM((chunks, rows, chunk), BF16),
            pltpu.VMEM((2, width, half), BF16),
            pltpu.VMEM((2, width, half), BF16),
            pltpu.VMEM((2, half, width), BF16),
            pltpu.VMEM((2, n1, n2, width // n, depth), BF16),
            dma((3,)),
            dma((3,)),
            dma((3,)),
            dma((2,)),
            dma((2, 2)),
            dma,
            dma((2, chunks)),
            dma((6,)),
            dma((n1 * chunks,)),
            dma((n1,)),
            dma((3 * chunks,)),
            dma((2,)),
            dma((chunks,)),
            dma((10,)),
            dma((10,)),
            dma((2,)),
            dma((2 * chunks,)),
            dma,
            dma((chunks,)),
            dma((6,)),
            dma,
        ],
        compiler_params=pltpu.CompilerParams(
            collective_id=0, has_side_effects=True, vmem_limit_bytes=60 * 1024 * 1024
        ),
    )(*operands)


def shards(
    tokens, norm_gain, routes, route_weights, w_gate, w_up, w_down, dense_in, dense_out, dense_gate
):
    rows, width = tokens.shape
    top_count = routes.shape[1]
    n = lax.axis_size("ep")
    capacity = (4 * rows * top_count + 3 * n - 1) // (3 * n)
    cap = capacity
    blocks = 8 // math.gcd(cap, 8)
    tall, tile = blocks * cap, width // blocks
    n2 = 1
    while n2 * n2 < n:
        n2 *= 2
    n1 = n // n2
    half = w_gate.shape[2]
    depth = dense_in.shape[1]
    if n1 == 4 and n2 == 4 and width % (CHUNKS * LANES) == 0 and width % n == 0:
        return gateway_call(
            (n, n1, n2, -(-cap // 8) * 8),
            (
                routes.T,
                route_weights.T,
                tokens,
                norm_gain.reshape(1, width),
                dense_gate.reshape(1, width),
                dense_in,
                dense_out,
                w_gate[0],
                w_up[0],
                w_down[0],
            ),
        )
    vmem = pl.BlockSpec(memory_space=pltpu.VMEM)
    anywhere = pl.BlockSpec(memory_space=pl.ANY)
    dma = pltpu.SemaphoreType.DMA
    slab = pltpu.VMEM((n, tall, tile), BF16)
    return pl.pallas_call(
        functools.partial(layer_kernel, (n, n1, n2, cap, blocks)),
        out_shape=jax.ShapeDtypeStruct((rows, width), BF16),
        in_specs=[vmem] * 8 + [anywhere] * 3,
        out_specs=vmem,
        scratch_shapes=[
            pltpu.VMEM((rows, width), BF16),
            pltpu.VMEM((n1, n2, blocks * rows), jnp.int32),
            pltpu.VMEM((blocks * rows, tile), BF16),
            pltpu.VMEM((rows, 2), jnp.int32),
            pltpu.VMEM((n2 * cap, width), BF16),
            pltpu.VMEM((n2 * tall, tile), F32),
            pltpu.VMEM((n2 * tall, n2 * tall), BF16),
            pltpu.VMEM((n2 * tall, n2 * tall), BF16),
            slab,
            slab,
            slab,
            slab,
            pltpu.VMEM((2, width, half), BF16),
            pltpu.VMEM((2, width, half), BF16),
            pltpu.VMEM((2, half, width), BF16),
            pltpu.VMEM((2, n2 * cap, half), BF16),
            pltpu.VMEM((2, n1, n2, width // n, depth), BF16),
            pltpu.VMEM((rows, width), F32),
            dma((n,)),
            dma((n,)),
            dma((n,)),
            dma((n,)),
            dma((3,)),
            dma((3,)),
            dma((3,)),
            dma((n1,)),
            dma((n1,)),
            dma((n2,)),
            dma((n2,)),
            dma,
            dma,
        ],
        compiler_params=pltpu.CompilerParams(
            collective_id=0, has_side_effects=True, vmem_limit_bytes=60 * 1024 * 1024
        ),
    )(
        routes.T,
        routes,
        route_weights,
        tokens,
        norm_gain.reshape(1, width),
        dense_gate.reshape(1, width),
        dense_in,
        dense_out,
        w_gate[0],
        w_up[0],
        w_down[0],
    )


def solution(mesh):
    placed = (
        P(("ep", "tp"), None),
        P(),
        P(("ep", "tp"), None),
        P(("ep", "tp"), None),
        P("ep", None, "tp"),
        P("ep", None, "tp"),
        P("ep", "tp", None),
        P("ep", None),
        P("ep", None),
        P(),
    )
    return jax.shard_map(
        shards, mesh=mesh, in_specs=placed, out_specs=P(("ep", "tp"), None), check_vma=False
    )
```

```python
import functools
import math

import jax
import jax.numpy as jnp
from jax import lax
from jax.experimental import pallas as pl
from jax.experimental.pallas import tpu as pltpu
from jax.sharding import PartitionSpec as P

CLAMP_LIMIT = 7.0
SLOPE_ALPHA = 1.702
NORM_EPS = 1e-06
MESH = pl.DeviceIdType.MESH
F32 = jnp.float32
BF16 = jnp.bfloat16


def clamped_unit(gate_pre, up_pre):
    gate_clip = jnp.minimum(gate_pre, CLAMP_LIMIT)
    up_clip = jnp.clip(up_pre, -CLAMP_LIMIT, CLAMP_LIMIT)
    return ((up_clip + 1.0) * gate_clip * jax.nn.sigmoid(SLOPE_ALPHA * gate_clip)).astype(BF16)


def layer_kernel(
    sizes,
    routes_t_ref,
    routes_ref,
    weights_ref,
    tokens_ref,
    gain_ref,
    dgate_ref,
    din_ref,
    dout_ref,
    wg_ref,
    wu_ref,
    wd_ref,
    out_ref,
    normed,
    keys,
    stacked,
    places,
    xs,
    totals,
    unpack_ref,
    pack_ref,
    buf,
    recv,
    outb,
    ret,
    wgs,
    wus,
    wds,
    hid,
    dn,
    acc,
    send1,
    recv1,
    send2,
    recv2,
    w_local,
    w_send,
    w_recv,
    ds1,
    dr1,
    ds2,
    dr2,
    ds3,
    dr3,
):
    n, n1, n2, cap, blocks = sizes
    rows, width = tokens_ref.shape
    half = wg_ref.shape[1]
    tall, tile = blocks * cap, width // blocks
    group_rows, packed_rows = n2 * cap, n2 * blocks * cap
    me = lax.axis_index("ep")
    core = lax.axis_index("tp")
    plane, spot = me // n2, me % n2
    peer = 1 - core

    barrier = pltpu.get_barrier_semaphore()

    def greet(i, carry):
        pl.semaphore_signal(
            barrier, inc=1, device_id={"ep": (me + i) % n}, device_id_type=MESH
        )
        return carry

    lax.fori_loop(1, n, greet, 0)
    pl.semaphore_signal(barrier, inc=1, device_id={"tp": peer}, device_id_type=MESH)

    weight_pairs = ((wg_ref, wgs), (wu_ref, wus), (wd_ref, wds))
    for i, (src, dst) in enumerate(weight_pairs):
        pltpu.make_async_copy(src, dst.at[0], w_local.at[i]).start()

    @pl.when(core == 0)
    def _():
        dn[0, plane, spot] = din_ref[...]

    @pl.when(core == 1)
    def _():
        dn[1, plane, spot] = dout_ref[...]

    widened = tokens_ref[...].astype(F32)
    inv_scale = lax.rsqrt(jnp.mean(widened * widened, axis=1, keepdims=True) + NORM_EPS)
    normed[...] = (widened * inv_scale * gain_ref[...]).astype(BF16)
    for j in range(blocks):
        stacked[j * rows : (j + 1) * rows, :] = normed[:, j * tile : (j + 1) * tile]

    expert_ids = lax.broadcasted_iota(jnp.int32, (n, rows), 0)
    chosen = (routes_t_ref[0:1, :] == expert_ids) | (routes_t_ref[1:2, :] == expert_ids)
    earlier = (
        lax.broadcasted_iota(jnp.int32, (rows, rows), 0)
        < lax.broadcasted_iota(jnp.int32, (rows, rows), 1)
    )
    counted = jnp.dot(
        jnp.where(chosen, 1.0, 0.0).astype(BF16),
        jnp.where(earlier, 1.0, 0.0).astype(BF16),
        preferred_element_type=F32,
    )
    for j in range(blocks):
        found = jnp.where(chosen, counted.astype(jnp.int32) + j * cap, -1)
        for z in range(n1):
            keys[z, :, j * rows : (j + 1) * rows] = found[z * n2 : (z + 1) * n2]
    experts_across = lax.broadcasted_iota(jnp.int32, (rows, n), 1)
    takes = [routes_ref[:, k : k + 1] == experts_across for k in range(2)]
    before = (
        lax.broadcasted_iota(jnp.int32, (rows, rows), 0)
        > lax.broadcasted_iota(jnp.int32, (rows, rows), 1)
    )
    counts = jnp.dot(
        jnp.where(before, 1.0, 0.0).astype(BF16),
        jnp.where(takes[0] | takes[1], 1.0, 0.0).astype(BF16),
        preferred_element_type=F32,
    )
    for k in range(2):
        slot = jnp.sum(jnp.where(takes[k], counts, 0.0), axis=1, keepdims=True)
        places[:, k : k + 1] = routes_ref[:, k : k + 1] * tall + slot.astype(jnp.int32)

    pl.semaphore_wait(barrier, n)

    def weight_copy(i):
        src, dst = weight_pairs[i]
        return pltpu.make_async_remote_copy(
            src_ref=src,
            dst_ref=dst.at[1],
            send_sem=w_send.at[i],
            recv_sem=w_recv.at[i],
            device_id={"tp": peer},
            device_id_type=MESH,
        )

    def dense_copy1(bit, block):
        other = plane + bit - 2 * bit * ((plane // bit) % 2)
        return pltpu.make_async_remote_copy(
            src_ref=dn.at[core, block, spot],
            dst_ref=dn.at[core, block, spot],
            send_sem=ds1.at[block],
            recv_sem=dr1.at[block],
            device_id={"ep": other * n2 + spot},
            device_id_type=MESH,
        )

    bits = [1 << b for b in reversed(range(n1.bit_length() - 1))]

    def dense_held(bit, where):
        return [where % (2 * bit) + m * 2 * bit for m in range(n1 // (2 * bit))]

    def dense_start(bit):
        for block in dense_held(bit, plane):
            dense_copy1(bit, block).start()

    def dense_finish(bit):
        for block in dense_held(bit, plane + bit - 2 * bit * ((plane // bit) % 2)):
            dense_copy1(bit, block).wait_recv()
        for block in dense_held(bit, plane):
            dense_copy1(bit, block).wait_send()

    def dense_copy2(other, slot):
        return pltpu.make_async_remote_copy(
            src_ref=dn.at[core, :, slot],
            dst_ref=dn.at[core, :, slot],
            send_sem=ds2.at[other],
            recv_sem=dr2.at[slot],
            device_id={"ep": plane * n2 + other},
            device_id_type=MESH,
        )

    def dense_copy3(which):
        return pltpu.make_async_remote_copy(
            src_ref=dn.at[which],
            dst_ref=dn.at[which],
            send_sem=ds3,
            recv_sem=dr3,
            device_id={"tp": peer},
            device_id_type=MESH,
        )

    def each(count, act):
        def step(i, carry):
            act(i)
            return carry

        lax.fori_loop(0, count, step, 0)

    dense_start(bits[0])
    for i in range(3):
        weight_copy(i).start()

    def dispatch(dst, slot):
        return pltpu.make_async_remote_copy(
            src_ref=buf.at[dst],
            dst_ref=recv.at[slot],
            send_sem=send1.at[dst],
            recv_sem=recv1.at[slot],
            device_id={"ep": dst},
            device_id_type=MESH,
        )

    def give_back(dst, slot):
        return pltpu.make_async_remote_copy(
            src_ref=outb.at[dst],
            dst_ref=ret.at[slot],
            send_sem=send2.at[dst],
            recv_sem=recv2.at[slot],
            device_id={"ep": dst},
            device_id_type=MESH,
        )

    def partner_plane(x):
        return sum(((plane // b) % 2 + (x // b) % 2) % 2 * b for b in bits)

    def turn(i):
        return partner_plane(i % 2 * (n1 // 2) + i // 2)

    def send_group(i):
        group = partner_plane((i + n1 // 2) % n1)
        first = group * n2
        wanted = keys[group]
        picks = wanted[:, None, :] == lax.broadcasted_iota(
            jnp.int32, (n2, tall, blocks * rows), 1
        )
        picks = jnp.where(picks, 1.0, 0.0).reshape(packed_rows, blocks * rows).astype(BF16)
        found = jnp.dot(picks, stacked[...], preferred_element_type=F32)
        buf[pl.ds(first, n2)] = found.reshape(n2, tall, tile).astype(BF16)

        def start(j):
            dst = first + (spot + 1 + j) % n2

            @pl.when(dst != me)
            def _():
                dispatch(dst, me).start()

            @pl.when(dst == me)
            def _():
                recv[me] = buf[me]

        each(n2, start)

    each(n1, send_group)


    for i, (src, dst) in enumerate(weight_pairs):
        pltpu.make_async_copy(src, dst.at[0], w_local.at[i]).wait()
    for i in range(3):
        weight_copy(i).wait()

    piece = min(256, half)
    upright = lax.broadcasted_iota(jnp.int32, (packed_rows, packed_rows), 0)
    across = lax.broadcasted_iota(jnp.int32, (packed_rows, packed_rows), 1)

    def packed_place(r):
        return (r // cap) % n2 * tall + r // group_rows * cap + r % cap

    unpack = jnp.where(packed_place(upright) == across, 1.0, 0.0).astype(BF16)
    pack = jnp.where(packed_place(across) == upright, 1.0, 0.0).astype(BF16)
    unpack_ref[...] = unpack
    pack_ref[...] = pack

    def run_group(i):
        group = turn(i)
        first = group * n2

        def arrive(j):
            src = first + j

            @pl.when(src != me)
            def _():
                dispatch(src, src).wait_recv()

        each(n2, arrive)
        came = recv[pl.ds(first, n2)].astype(F32).reshape(packed_rows, tile).astype(BF16)
        apart = jnp.dot(unpack_ref[...], came, preferred_element_type=F32)
        for j in range(blocks):
            xs[:, j * tile : (j + 1) * tile] = apart[
                j * group_rows : (j + 1) * group_rows
            ].astype(BF16)
        x = xs[...]
        for part in range(2):
            for low in range(0, half, piece):
                gate_pre = jnp.dot(
                    x, wgs[part, :, low : low + piece], preferred_element_type=F32
                )
                up_pre = jnp.dot(x, wus[part, :, low : low + piece], preferred_element_type=F32)
                hid[part, :, low : low + piece] = clamped_unit(gate_pre, up_pre)
        for j in range(blocks):
            total = jnp.zeros((group_rows, tile), F32)
            for part in range(2):
                partial = jnp.dot(
                    hid[part],
                    wds[part, :, j * tile : (j + 1) * tile],
                    preferred_element_type=F32,
                )
                total = total + partial.astype(BF16).astype(F32)
            totals[j * group_rows : (j + 1) * group_rows, :] = total
        joined = jnp.dot(pack_ref[...], totals[...].astype(BF16), preferred_element_type=F32)
        outb[pl.ds(first, n2)] = joined.reshape(n2, tall, tile).astype(BF16)

        def start(j):
            dst = first + (spot + 1 + j) % n2

            @pl.when(dst != me)
            def _():
                give_back(dst, me).start()

            @pl.when(dst == me)
            def _():
                ret[me] = outb[me]

        each(n2, start)

    def run_turn(i):
        run_group(i)
        for b, bit in enumerate(bits):

            @pl.when(i == b)
            def _():
                dense_finish(bit)
                if b + 1 < len(bits):
                    dense_start(bits[b + 1])
                else:
                    each(n2 - 1, lambda j: dense_copy2((spot + 1 + j) % n2, spot).start())

    each(n1, run_turn)
    each(n2 - 1, lambda i: dense_copy2((spot + 1 + i) % n2, (spot + 1 + i) % n2).wait_recv())
    dense_copy3(core).start()
    dense_copy3(core).wait_send()
    dense_copy3(peer).wait_recv()
    depth = din_ref.shape[1]
    dense_pre = jnp.dot(
        normed[...], dn[0].reshape(width, depth), preferred_element_type=F32
    )
    dense_hidden = jax.nn.silu(dense_pre).astype(BF16)
    step = width // n1
    for z in range(n1):
        branch = lax.dot_general(
            dense_hidden,
            dn[1, z].reshape(step, depth),
            (((1,), (1,)), ((), ())),
            preferred_element_type=F32,
        )
        acc[:, z * step : (z + 1) * step] = (
            jax.nn.sigmoid(dgate_ref[:, z * step : (z + 1) * step]) * branch
        )

    def combine_group(i):
        group = turn(i)
        first = group * n2

        def arrive(j):
            src = first + j

            @pl.when(src != me)
            def _():
                give_back(src, src).wait_recv()

        each(n2, arrive)
        back = ret[pl.ds(first, n2)].astype(F32).reshape(packed_rows, tile).astype(BF16)
        lanes = lax.broadcasted_iota(jnp.int32, (rows, packed_rows), 1) + first * tall
        wanted = jnp.concatenate(
            [
                jnp.where(places[:, k : k + 1] + j * cap == lanes, 1.0, 0.0).astype(BF16)
                for k in range(2)
                for j in range(blocks)
            ],
            axis=0,
        )
        picked = jnp.dot(wanted, back, preferred_element_type=F32)
        for j in range(blocks):
            total = acc[:, j * tile : (j + 1) * tile]
            for k in range(2):
                at = (k * blocks + j) * rows
                total = total + picked[at : at + rows] * weights_ref[:, k : k + 1]
            acc[:, j * tile : (j + 1) * tile] = total

    each(n1, combine_group)
    out_ref[...] = acc[...].astype(BF16)

    def drain(i):
        other = (me + 1 + i) % n
        dispatch(other, me).wait_send()
        give_back(other, me).wait_send()

    each(n - 1, drain)
    each(n2 - 1, lambda i: dense_copy2((spot + 1 + i) % n2, spot).wait_send())


LANES = 128
CHUNKS = 4


def gateway_kernel(
    sizes,
    routes_ref,
    weights_ref,
    tokens_ref,
    gain_ref,
    dgate_ref,
    din_ref,
    dout_ref,
    wg_ref,
    wu_ref,
    wd_ref,
    out_ref,
    tokens_in,
    mixed,
    gain_in,
    dgate_in,
    routes_of,
    weights_of,
    dense,
    picks,
    wanted,
    columns,
    buf,
    recv,
    xs,
    hid,
    outb,
    ret,
    relay,
    accs,
    pout,
    fin,
    through,
    wgs,
    wus,
    wds,
    dn,
    w_local,
    w_send,
    w_recv,
    meta_send,
    meta_recv,
    dense_send,
    dense_recv,
    send1,
    recv1,
    send2,
    recv2,
    fin_send,
    fin_recv,
    dn_send,
    dn_recv,
    relay_send,
    relay_recv,
    through_send,
    through_recv,
    inputs,
    out_sem,
):
    n, n1, n2, tall = sizes
    rows, width = tokens_ref.shape
    half = wg_ref.shape[1]
    chunks = CHUNKS
    chunk = width // chunks
    near = n // 2
    group_rows = n2 * tall
    me = lax.axis_index("ep")
    core = lax.axis_index("tp")
    peer = 1 - core
    plane, spot = me // n2, me % n2
    side = plane // 2
    mine = me % near
    base = side * near
    is_gate = (plane + 1) // 2 % 2
    sibling = plane + 1 - 2 * (plane % 2)
    gate_plane = 1 + side
    far_gate = 2 - side
    far_end = 3 - 3 * side
    on_gate = is_gate == 1
    on_end = is_gate == 0

    def at(where):
        return {"ep": where}

    def each(count, act):
        def step(i, carry):
            act(i)
            return carry

        lax.fori_loop(0, count, step, 0)

    def remote(src, dst, send_sem, recv_sem, device):
        return pltpu.make_async_remote_copy(
            src_ref=src,
            dst_ref=dst,
            send_sem=send_sem,
            recv_sem=recv_sem,
            device_id=device,
            device_id_type=MESH,
        )

    barrier = pltpu.get_barrier_semaphore()
    small_pairs = (
        (tokens_ref, tokens_in),
        (gain_ref, gain_in),
        (routes_ref, routes_of.at[0]),
        (weights_ref, weights_of.at[0]),
        (dgate_ref, dgate_in),
    )
    small_copies = [
        pltpu.make_async_copy(src, dst, inputs.at[i])
        for i, (src, dst) in enumerate(small_pairs)
    ]
    for copy in small_copies:
        copy.start()

    def greet(device):
        pl.semaphore_signal(barrier, inc=1, device_id=device, device_id_type=MESH)

    each(near - 1, lambda i: greet(at(base + (mine + 1 + i) % near)))
    greet({"tp": peer})
    greet(at(far_gate * n2 + spot))

    @pl.when(on_gate)
    def _():
        greet(at(far_end * n2 + spot))

    def block_copy(which):
        return pltpu.make_async_copy(
            (din_ref, dout_ref)[which], dn.at[which, plane, spot], inputs.at[5]
        )

    for which in range(2):

        @pl.when(core == which)
        def _():
            block_copy(which).start()

    block_copy(0).wait()
    for copy in small_copies:
        copy.wait()
    weight_pairs = ((wg_ref, wgs), (wu_ref, wus), (wd_ref, wds))
    for i, (src, dst) in enumerate(weight_pairs):
        pltpu.make_async_copy(src, dst.at[0], w_local.at[i]).start()

    with jax.named_scope("norm"):
        widened = tokens_in[...].astype(F32)
        inv_scale = lax.rsqrt(jnp.mean(widened * widened, axis=1, keepdims=True) + NORM_EPS)
        normed = (widened * inv_scale * gain_in[...]).astype(BF16)
        for c in range(chunks):
            dense[0, c] = normed[:, c * chunk : (c + 1) * chunk]

    def prepare(kind):
        experts = lax.broadcasted_iota(jnp.int32, (near, rows), 0) + base
        first, second = routes_of[kind, 0:1, :], routes_of[kind, 1:2, :]
        takes = (first == experts, second == experts)
        chosen = takes[0] | takes[1]
        earlier = (
            lax.broadcasted_iota(jnp.int32, (rows, rows), 0)
            < lax.broadcasted_iota(jnp.int32, (rows, rows), 1)
        )
        counted = jnp.dot(
            jnp.where(chosen, 1.0, 0.0).astype(BF16),
            jnp.where(earlier, 1.0, 0.0).astype(BF16),
            preferred_element_type=F32,
        )
        keys = jnp.where(chosen, counted.astype(jnp.int32), -1)
        hits = keys[:, None, :] == lax.broadcasted_iota(jnp.int32, (near, tall, rows), 1)
        picks[kind] = jnp.where(hits, 1.0, 0.0).reshape(near * tall, rows).astype(BF16)
        local = lax.broadcasted_iota(jnp.int32, (near, rows), 0) * tall
        places = [
            jnp.sum(
                jnp.where(take, counted + local.astype(F32) + n * tall, 0.0),
                axis=0,
                keepdims=True,
            )
            - n * tall
            for take in takes
        ]
        stack = jnp.concatenate(
            places + [weights_of[kind], jnp.zeros((4, rows), F32)], axis=0
        )
        turned = jnp.transpose(stack)
        columns[kind] = turned
        lanes = lax.broadcasted_iota(jnp.int32, (rows, near * tall), 1)
        for k in range(2):
            place = turned[:, k : k + 1].astype(jnp.int32)
            wanted[kind, k * rows : (k + 1) * rows, :] = jnp.where(
                place == lanes, 1.0, 0.0
            ).astype(BF16)

    with jax.named_scope("prepare0"):
        prepare(0)

    def meta_copies():
        slot = 2 - is_gate
        device = at(far_gate * n2 + spot)
        return (
            remote(routes_of.at[0], routes_of.at[slot], meta_send.at[0], meta_recv.at[0, slot - 1], device),
            remote(weights_of.at[0], weights_of.at[slot], meta_send.at[1], meta_recv.at[1, slot - 1], device),
        )

    def meta_wait(slot):
        device = at(far_gate * n2 + spot)
        remote(
            routes_of.at[0], routes_of.at[slot], meta_send.at[0], meta_recv.at[0, slot - 1], device
        ).wait_recv()
        remote(
            weights_of.at[0], weights_of.at[slot], meta_send.at[1], meta_recv.at[1, slot - 1], device
        ).wait_recv()

    def dense_copy(slot, c):
        return remote(
            dense.at[0, c],
            dense.at[slot, c],
            dense_send,
            dense_recv.at[slot - 1, c],
            at(far_gate * n2 + spot),
        )

    def dense_start():
        for c in range(chunks):
            dense_copy(2 - is_gate, c).start()

    def dn_block(which, index, target):
        block = dn.at[core, which, spot]
        return remote(
            block, block, dn_send.at[index], dn_recv.at[index], at(target * n2 + spot)
        )

    def dn_near(which):
        return dn_block(which, 0, sibling)

    def dn_cross(which):
        return dn_block(which, 1, far_gate)

    def dn_far(which):
        return dn_block(which, 2, far_gate)

    def dn_down(order):
        return dn_block(far_end if order else far_gate, 3 + order, sibling)

    first_bit, second_bit = 1 + core, 2 - core
    first_spot = spot + first_bit - 2 * first_bit * (spot // first_bit % 2)
    second_spot = spot + second_bit - 2 * second_bit * (spot // second_bit % 2)

    def dn_step(part, step, block):
        index = 5 + 2 * part + step
        return remote(
            block,
            block,
            dn_send.at[index],
            dn_recv.at[index],
            at(plane * n2 + (second_spot if step else first_spot)),
        )

    def dn_start(part, step):
        for slot in (spot, first_spot)[: 1 + step]:
            if part == 0:
                dn_step(part, step, dn.at[core, plane, slot]).start()
            else:
                dn_step(part, step, dn.at[core, sibling, slot]).start()
                dn_step(part, step, dn.at[core, pl.ds((1 - side) * 2, 2), slot]).start()

    def dn_bytes(part, step):
        slots = pl.ds(0, 2) if step else 0
        return dn_step(part, step, dn.at[core, pl.ds(0, n1 - 1) if part else 0, slots])

    def dn_swap(which):
        last = 9
        return remote(
            dn.at[which], dn.at[which], dn_send.at[last], dn_recv.at[last], {"tp": peer}
        )

    def weight_copy(i):
        src, dst = weight_pairs[i]
        return remote(src, dst.at[1], w_send.at[i], w_recv.at[i], {"tp": peer})

    spots = [(spot + i) % n2 for i in range(n2)]
    inner = plane % 2 * n2
    outer = n2 - inner

    def dispatch(kind, away, i, c):
        expert = (outer if away else inner) + spots[i]
        group = kind + 1 if kind else away
        return remote(
            buf.at[kind, expert] if c is None else buf.at[kind, expert, c],
            recv.at[group, spot] if c is None else recv.at[group, spot, c],
            send1.at[kind * 2 + away],
            recv1.at[group * chunks + (c or 0)],
            at(base + expert),
        )

    def dispatched(kind, away):
        sent = buf.at[kind, pl.ds(0, n2 - 1 + away)]
        remote(sent, sent, send1.at[kind * 2 + away], recv1.at[0], at(base + outer)).wait_send()

    others = [(1, i) for i in range(n2)] + [(0, i) for i in range(1, n2)]

    def select_own():
        everything = jnp.concatenate([dense[0, c] for c in range(chunks)], axis=1)
        found = jnp.dot(picks[0], everything, preferred_element_type=F32).astype(BF16)
        for c in range(chunks):
            buf[0, :, c] = found[:, c * chunk : (c + 1) * chunk].reshape(near, tall, chunk)
        for away, i in others:
            dispatch(0, away, i, None).start()
        recv[0, spot] = buf[0, mine]

    def select(kind, c):
        with jax.named_scope("densewait"):
            dense_copy(kind, c).wait_recv()
        with jax.named_scope("select"):
            found = jnp.dot(picks[kind], dense[kind, c], preferred_element_type=F32)
            buf[kind, :, c] = found.astype(BF16).reshape(near, tall, chunk)
            for away, i in others:
                dispatch(kind, away, i, c).start()
            recv[kind + 1, spot, c] = buf[kind, mine, c]

    def hop(group):
        return (plane, sibling, gate_plane, gate_plane)[group]

    def give_back(group, i, c):
        s = spots[i]
        kind = max(group - 1, 0)
        return remote(
            outb.at[group, s] if c is None else outb.at[group, s, c],
            ret.at[kind, mine] if c is None else ret.at[kind, mine, c],
            send2.at[group],
            recv2.at[kind * chunks + (c or 0)],
            at(hop(group) * n2 + s),
        )

    def given_back(group, count):
        sent = outb.at[group, pl.ds(0, count)]
        remote(sent, sent, send2.at[group], recv2.at[0], at(base + outer)).wait_send()

    def arrived(group, c, count):
        part = recv.at[group, pl.ds(0, count)]
        if c is not None:
            part = recv.at[group, pl.ds(0, count), c]
        remote(
            part, part, send1.at[0], recv1.at[group * chunks + (c or 0)], at(base + outer)
        ).wait_recv()

    def by_role(act):
        @pl.when(on_end)
        def _():
            act(n2)

        @pl.when(on_gate)
        def _():
            act(n2 - 1)

    piece = min(256, half)

    def feed(x):
        for part in range(2):
            for low in range(0, half, piece):
                gate_pre = jnp.dot(
                    x, wgs[part, :, low : low + piece], preferred_element_type=F32
                )
                up_pre = jnp.dot(x, wus[part, :, low : low + piece], preferred_element_type=F32)
                hid[part, :, low : low + piece] = clamped_unit(gate_pre, up_pre)

    def down(c):
        return jnp.dot(
            hid[0], wds[0, :, c * chunk : (c + 1) * chunk], preferred_element_type=F32
        ) + jnp.dot(
            hid[1], wds[1, :, c * chunk : (c + 1) * chunk], preferred_element_type=F32
        )

    def store_out(group, c):
        outb[group, :, c] = down(c).astype(BF16).reshape(n2, tall, chunk)

    def take_in(group, c):
        xs[:, c * chunk : (c + 1) * chunk] = recv[group, :, c].reshape(group_rows, chunk)

    def run_near(group):
        with jax.named_scope("neararrive"):
            arrived(group, None, n2 - 1 + group)
        with jax.named_scope("near"):
            for c in range(chunks):
                take_in(group, c)
            feed(xs[...])
            for c in range(chunks):
                store_out(group, c)
            if group == 0:
                ret[0, mine] = outb[0, spot]

    def send_near(group, low, high):
        for i in range(low, high):
            give_back(group, i, None).start()

    def run_far(group):
        for c in range(chunks):
            with jax.named_scope("arrive"):
                by_role(lambda count: arrived(group, c, count))
            take_in(group, c)
        with jax.named_scope("feed"):
            feed(xs[...])
        for c in range(chunks):
            store_out(group, c)

            @pl.when(on_end)
            def _():
                for i in range(1, n2):
                    pass_on(group, i, c).start()
                relay[group - 2, spot, c] = outb[group, spot, c]

            @pl.when(on_gate)
            def _():
                for i in range(1, n2):
                    give_back(group, i, c).start()
                ret[group - 1, mine, c] = outb[group, spot, c]

    def pass_on(group, i, c):
        s = spots[i]
        return remote(
            outb.at[group, s, c],
            relay.at[group - 2, spot, c],
            send2.at[group],
            relay_recv.at[(group - 2) * chunks + c],
            at(plane * n2 + s),
        )

    def forward(group, c):
        return remote(
            relay.at[group - 2, :, c],
            ret.at[group - 1, pl.ds(inner, n2), c],
            relay_send.at[group - 2],
            recv2.at[(group - 1) * chunks + c],
            at(sibling * n2 + spot),
        )

    def run_relay(group):
        with jax.named_scope("relay"):
            for c in range(chunks):
                part = relay.at[group - 2, pl.ds(0, n2 - 1), c]
                remote(
                    part,
                    part,
                    relay_send.at[0],
                    relay_recv.at[(group - 2) * chunks + c],
                    at(base + outer),
                ).wait_recv()
                forward(group, c).start()

    def returned(kind, c):
        part = ret.at[kind, pl.ds(0, near - 1)]
        if c is not None:
            part = ret.at[kind, pl.ds(0, near - 1), c]
        remote(
            part, part, send2.at[0], recv2.at[kind * chunks + (c or 0)], at(base + outer)
        ).wait_recv()

    def weighed(kind, c):
        back = ret[kind, :, c].reshape(near * tall, chunk)
        picked = jnp.dot(wanted[kind], back, preferred_element_type=F32)
        return (
            picked[:rows] * columns[kind, :, 2:3] + picked[rows:] * columns[kind, :, 3:4]
        )

    def fin_copy(kind, c):
        target = fin.at[c] if kind == 1 else through.at[c]
        landing = fin_recv.at[c] if kind == 1 else through_recv.at[c]
        return remote(
            pout.at[kind - 1, c],
            target,
            fin_send.at[kind - 1],
            landing,
            at(far_gate * n2 + spot),
        )

    def pass_through(c):
        return remote(
            through.at[c], fin.at[c], through_send, fin_recv.at[c], at(sibling * n2 + spot)
        )

    def run_through(c):
        with jax.named_scope("through"):
            fin_copy(2, c).wait_recv()
            pass_through(c).start()

    def combine(kind, c):
        with jax.named_scope("gatherwait"):
            returned(kind, c)
        with jax.named_scope("combine"):
            pout[kind - 1, c] = weighed(kind, c).astype(BF16)
            fin_copy(kind, c).start()

    def dense_branch():
        depth = din_ref.shape[1]
        x = jnp.concatenate(
            [
                dense[0, c]
                for c in range(chunks)
            ],
            axis=1,
        )
        pre = jnp.dot(x, dn[0].reshape(width, depth), preferred_element_type=F32)
        dense_hidden = jax.nn.silu(pre).astype(BF16)
        step = width // n1
        for z in range(n1):
            branch = lax.dot_general(
                dense_hidden,
                dn[1, z].reshape(step, depth),
                (((1,), (1,)), ((), ())),
                preferred_element_type=F32,
            )
            accs[:, z * step : (z + 1) * step] = (
                jax.nn.sigmoid(dgate_in[:, z * step : (z + 1) * step]) * branch
            )

    with jax.named_scope("barrier"):
        pl.semaphore_wait(barrier, near + 1 + is_gate)
    for copy in meta_copies():
        copy.start()

    @pl.when(on_gate)
    def _():
        dn_cross(plane).start()

    dense_start()
    dn_near(plane).start()

    @pl.when(on_end)
    def _():
        dn_far(plane).start()

    for i in range(3):
        weight_copy(i).start()
    with jax.named_scope("selectown"):
        select_own()
    dn_start(0, 0)

    def weights_wait():
        with jax.named_scope("weightwait"):
            for i, (src, dst) in enumerate(weight_pairs):
                pltpu.make_async_copy(src, dst.at[0], w_local.at[i]).wait()
            for i in range(3):
                weight_copy(i).wait()

    def prepare_for(kind):
        with jax.named_scope("prepare"):
            meta_wait(kind)
            prepare(kind)

    part = chunks // 2

    def swap_start():
        with jax.named_scope("swapstart"):
            for p in range(2):
                dn_bytes(p, 1).wait_recv()
        dn_swap(core).start()

    def step_wait(index):
        with jax.named_scope("stepwait"):
            dn_bytes(index, 0).wait_recv()

    @pl.when(on_gate)
    def _():
        prepare_for(2)
        select(2, 0)
        step_wait(0)
        dn_start(0, 1)
        for c in range(1, chunks):
            select(2, c)
        prepare_for(1)
        weights_wait()
        run_near(0)
        send_near(0, 1, n2)
        select(1, 0)
        with jax.named_scope("upwait"):
            dn_cross(far_gate).wait_recv()
        dn_down(0).start()

    @pl.when(on_end)
    def _():
        step_wait(0)
        dn_start(0, 1)
        weights_wait()
        run_near(0)
        send_near(0, 1, n2)
        run_near(1)

    with jax.named_scope("farC"):
        run_far(3)

    @pl.when(on_end)
    def _():
        run_relay(3)
        send_near(1, 0, 1)
        with jax.named_scope("upwait"):
            dn_near(sibling).wait_recv()
            for order in range(2):
                dn_down(order).wait_recv()
        dn_start(1, 0)

    @pl.when(on_gate)
    def _():
        select(1, 1)
        with jax.named_scope("upwait"):
            dn_far(far_end).wait_recv()
            dn_near(sibling).wait_recv()
        dn_down(1).start()
        select(1, 2)
        run_near(1)
        select(1, 3)
        send_near(1, 0, 1)
        dn_start(1, 0)
        for c in range(chunks):
            combine(2, c)
        send_near(1, 1, part)
        run_through(0)

    with jax.named_scope("farB"):
        run_far(2)

    @pl.when(on_gate)
    def _():
        step_wait(1)
        dn_start(1, 1)
        run_through(1)
        run_through(2)
        run_through(3)
        send_near(1, part, n2)
        combine(1, 0)
        combine(1, 1)
        combine(1, 2)
        swap_start()
        combine(1, 3)

    @pl.when(on_end)
    def _():
        step_wait(1)
        dn_start(1, 1)
        run_relay(2)
        send_near(1, 1, n2)
        swap_start()

    with jax.named_scope("dnwait"):
        dn_swap(peer).wait_recv()
    with jax.named_scope("densebranch"):
        dense_branch()
    with jax.named_scope("ownwait"):
        returned(0, None)

    with jax.named_scope("finish"):
        for c in range(chunks):
            with jax.named_scope("finwait"):
                fin_copy(1, c).wait_recv()
            span = slice(c * chunk, (c + 1) * chunk)
            mixed[:, span] = (
                accs[:, span] + weighed(0, c) + fin[c].astype(F32)
            ).astype(BF16)
            pltpu.make_async_copy(mixed.at[:, span], out_ref.at[:, span], out_sem).start()

    with jax.named_scope("drain"):
        for away in range(2):
            dispatched(0, away)
        for copy in meta_copies():
            copy.wait_send()
        remote(
            dense.at[0], dense.at[0], dense_send, dense_recv.at[0, 0], at(base + outer)
        ).wait_send()
        for group in range(2):
            given_back(group, n2 - 1 + group)
        for group in range(2, n1):
            given_back(group, n2 - 1)
        dn_near(plane).wait_send()
        for p in range(2):
            for step in range(2):
                dn_bytes(p, step).wait_send()
        dn_swap(core).wait_send()

        @pl.when(on_end)
        def _():
            dn_far(plane).wait_send()
            for group in (0, 1):
                remote(
                    relay.at[group],
                    relay.at[group],
                    relay_send.at[group],
                    relay_recv.at[0],
                    at(base + outer),
                ).wait_send()

        @pl.when(on_gate)
        def _():
            for away in range(2):
                dispatched(2, away)
            for away in range(2):
                dispatched(1, away)
            remote(
                through, through, through_send, through_recv.at[0], at(base + outer)
            ).wait_send()
            dn_cross(plane).wait_send()
            for order in range(2):
                dn_down(order).wait_send()

    @pl.when(on_gate)
    def _():
        for kind in (1, 2):
            sent = pout.at[kind - 1]
            remote(
                sent, sent, fin_send.at[kind - 1], fin_recv.at[0], at(base + outer)
            ).wait_send()

    pltpu.make_async_copy(mixed, out_ref, out_sem).wait()


def gateway_call(sizes, operands):
    n, n1, n2, tall = sizes
    tokens, dense_in, w_gate = operands[2], operands[5], operands[7]
    rows, width = tokens.shape
    half, depth = w_gate.shape[1], dense_in.shape[1]
    near, chunks = n // 2, CHUNKS
    chunk = width // chunks
    anywhere = pl.BlockSpec(memory_space=pltpu.HBM)
    dma = pltpu.SemaphoreType.DMA
    return pl.pallas_call(
        functools.partial(gateway_kernel, sizes),
        out_shape=jax.ShapeDtypeStruct((rows, width), BF16),
        in_specs=[anywhere] * 10,
        out_specs=anywhere,
        scratch_shapes=[
            pltpu.VMEM((rows, width), BF16),
            pltpu.VMEM((rows, width), BF16),
            pltpu.VMEM((1, width), F32),
            pltpu.VMEM((1, width), F32),
            pltpu.VMEM((3, 2, rows), jnp.int32),
            pltpu.VMEM((3, 2, rows), F32),
            pltpu.VMEM((3, chunks, rows, chunk), BF16),
            pltpu.VMEM((3, near * tall, rows), BF16),
            pltpu.VMEM((3, 2 * rows, near * tall), BF16),
            pltpu.VMEM((3, rows, 8), F32),
            pltpu.VMEM((3, near, chunks, tall, chunk), BF16),
            pltpu.VMEM((n1, n2, chunks, tall, chunk), BF16),
            pltpu.VMEM((n2 * tall, width), BF16),
            pltpu.VMEM((2, n2 * tall, half), BF16),
            pltpu.VMEM((n1, n2, chunks, tall, chunk), BF16),
            pltpu.VMEM((3, near, chunks, tall, chunk), BF16),
            pltpu.VMEM((2, n2, chunks, tall, chunk), BF16),
            pltpu.VMEM((rows, width), F32),
            pltpu.VMEM((2, chunks, rows, chunk), BF16),
            pltpu.VMEM((chunks, rows, chunk), BF16),
            pltpu.VMEM((chunks, rows, chunk), BF16),
            pltpu.VMEM((2, width, half), BF16),
            pltpu.VMEM((2, width, half), BF16),
            pltpu.VMEM((2, half, width), BF16),
            pltpu.VMEM((2, n1, n2, width // n, depth), BF16),
            dma((3,)),
            dma((3,)),
            dma((3,)),
            dma((2,)),
            dma((2, 2)),
            dma,
            dma((2, chunks)),
            dma((6,)),
            dma((n1 * chunks,)),
            dma((n1,)),
            dma((3 * chunks,)),
            dma((2,)),
            dma((chunks,)),
            dma((10,)),
            dma((10,)),
            dma((2,)),
            dma((2 * chunks,)),
            dma,
            dma((chunks,)),
            dma((6,)),
            dma,
        ],
        compiler_params=pltpu.CompilerParams(
            collective_id=0, has_side_effects=True, vmem_limit_bytes=60 * 1024 * 1024
        ),
    )(*operands)


def shards(
    tokens, norm_gain, routes, route_weights, w_gate, w_up, w_down, dense_in, dense_out, dense_gate
):
    rows, width = tokens.shape
    top_count = routes.shape[1]
    n = lax.axis_size("ep")
    capacity = (4 * rows * top_count + 3 * n - 1) // (3 * n)
    cap = capacity
    blocks = 8 // math.gcd(cap, 8)
    tall, tile = blocks * cap, width // blocks
    n2 = 1
    while n2 * n2 < n:
        n2 *= 2
    n1 = n // n2
    half = w_gate.shape[2]
    depth = dense_in.shape[1]
    if n1 == 4 and n2 == 4 and width % (CHUNKS * LANES) == 0 and width % n == 0:
        return gateway_call(
            (n, n1, n2, -(-cap // 8) * 8),
            (
                routes.T,
                route_weights.T,
                tokens,
                norm_gain.reshape(1, width),
                dense_gate.reshape(1, width),
                dense_in,
                dense_out,
                w_gate[0],
                w_up[0],
                w_down[0],
            ),
        )
    vmem = pl.BlockSpec(memory_space=pltpu.VMEM)
    anywhere = pl.BlockSpec(memory_space=pl.ANY)
    dma = pltpu.SemaphoreType.DMA
    slab = pltpu.VMEM((n, tall, tile), BF16)
    return pl.pallas_call(
        functools.partial(layer_kernel, (n, n1, n2, cap, blocks)),
        out_shape=jax.ShapeDtypeStruct((rows, width), BF16),
        in_specs=[vmem] * 8 + [anywhere] * 3,
        out_specs=vmem,
        scratch_shapes=[
            pltpu.VMEM((rows, width), BF16),
            pltpu.VMEM((n1, n2, blocks * rows), jnp.int32),
            pltpu.VMEM((blocks * rows, tile), BF16),
            pltpu.VMEM((rows, 2), jnp.int32),
            pltpu.VMEM((n2 * cap, width), BF16),
            pltpu.VMEM((n2 * tall, tile), F32),
            pltpu.VMEM((n2 * tall, n2 * tall), BF16),
            pltpu.VMEM((n2 * tall, n2 * tall), BF16),
            slab,
            slab,
            slab,
            slab,
            pltpu.VMEM((2, width, half), BF16),
            pltpu.VMEM((2, width, half), BF16),
            pltpu.VMEM((2, half, width), BF16),
            pltpu.VMEM((2, n2 * cap, half), BF16),
            pltpu.VMEM((2, n1, n2, width // n, depth), BF16),
            pltpu.VMEM((rows, width), F32),
            dma((n,)),
            dma((n,)),
            dma((n,)),
            dma((n,)),
            dma((3,)),
            dma((3,)),
            dma((3,)),
            dma((n1,)),
            dma((n1,)),
            dma((n2,)),
            dma((n2,)),
            dma,
            dma,
        ],
        compiler_params=pltpu.CompilerParams(
            collective_id=0, has_side_effects=True, vmem_limit_bytes=60 * 1024 * 1024
        ),
    )(
        routes.T,
        routes,
        route_weights,
        tokens,
        norm_gain.reshape(1, width),
        dense_gate.reshape(1, width),
        dense_in,
        dense_out,
        w_gate[0],
        w_up[0],
        w_down[0],
    )


def solution(mesh):
    placed = (
        P(("ep", "tp"), None),
        P(),
        P(("ep", "tp"), None),
        P(("ep", "tp"), None),
        P("ep", None, "tp"),
        P("ep", None, "tp"),
        P("ep", "tp", None),
        P("ep", None),
        P("ep", None),
        P(),
    )
    return jax.shard_map(
        shards, mesh=mesh, in_specs=placed, out_specs=P(("ep", "tp"), None), check_vma=False
    )
```
